128 devices in a mesh: st: 16 (over z, x), tp: 8 (over y, core).
Axes of the slice: x: 4, y: 4, z: 4, core: 2. Of those that a mesh axis runs over, the one named last changes fastest.
Arguments:
- tokens: bfloat16 [32768, 2048], P('st', 'tp'), may hold values from -48 to 48
- store: bfloat16 [512, 64, 2048], P('st'), may hold values from -48 to 48
- passage_holder_index: int32 [256, 2], P('st'), may hold values from 0 to 15, all different within a row; in each aligned block of 16 rows (0 to 15, 16 to 31, ...) at most 4 rows name the same one
- passage_slot: int32 [256, 2], P('st'), may hold values from 0 to 31
- query_weight: bfloat16 [2048, 1024], P(None, 'tp'), may hold values from -0.125 to 0.125
- key_matrix: bfloat16 [2048, 1024], P(None, 'tp'), may hold values from -0.125 to 0.125
- value_weight: bfloat16 [2048, 1024], P(None, 'tp'), may hold values from -0.125 to 0.125
- outer_gate: bfloat16 [2048, 1024], P(None, 'tp'), may hold values from -0.125 to 0.125
- inner_gate: bfloat16 [2048, 1024], P(None, 'tp'), may hold values from -0.125 to 0.125
- conv_input: bfloat16 [2048, 1024], P(None, 'tp'), may hold values from -0.125 to 0.125
- conv_taps: bfloat16 [3, 1024], P(None, 'tp'), may hold values from -3.5 to 3.5
- route_gate_projection: bfloat16 [2048, 2], replicated, may hold values from -0.125 to 0.125
- conv_out: bfloat16 [1024, 2048], P('tp'), may hold values from -0.1875 to 0.1875
- memory_out: bfloat16 [1024, 2048], P('tp'), may hold values from -0.1875 to 0.1875
Outputs:
- mixed: bfloat16 [32768, 2048], P(('st', 'tp'))
The draws below stay inside these ranges and needn't reach their ends.
Inputs may be any that keep to these rules, and one draw needn't show every extreme that they name: `passage_holder_index`: each row names 2 different owners; among the rows of one index of st (16 aligned rows) no owner is named more than 4 times, a bound that some index of st reaches.
All inputs are finite; a program needn't handle non-finite values.
Results may differ from the reference program's by a relative error of at most 0.014.
Values may be sent and summed in bfloat16 or wider, within the bound.
A program may use at most 128 MiB of HBM per device.

```python
import math
import jax
import jax.numpy as jnp
import numpy as np
from jax import lax

D = 2048
HEADS = 8
HEAD_SIZE = 128
FILTER_CHANNELS = 1024
CONV_K = 3
SEQ_LEN = 256
BLOCK = 128
NPB = 2
PLEN = 64
P_DEV = 32
MEM_WIDTH = 1024
NBLK_DEV = 16
CAP = 4
TOKENS = 32768
BLOCKS = 256
PASSAGES = 512
N_ST = 16
N_TP = 8


def draw_tokens(key, part):
    first_key = jax.random.fold_in(jax.random.fold_in(key, 11), 0)
    values = jnp.clip(jax.random.normal(first_key, (TOKENS, D), jnp.float32), -4.0, 4.0)
    return values.astype(jnp.bfloat16)


def draw_store(key, part):
    first_key = jax.random.fold_in(jax.random.fold_in(key, 23), 0)
    values = jnp.clip(jax.random.normal(first_key, (PASSAGES, PLEN, D), jnp.float32), -4.0, 4.0)
    return values.astype(jnp.bfloat16)


def set_ends(values, key, smallest, high):
    shape = values.shape
    spot = [jax.random.randint(jax.random.fold_in(key, axis), (), 0, shape[axis]) for axis in range(len(shape))]
    values = values.at[tuple(spot)].set(smallest)
    longest = shape.index(max(shape))
    spot[longest] = (spot[longest] + 1) % shape[longest]
    return values.at[tuple(spot)].set(high)


def shard_levels(key, dims, pieces, low, largest):
    level = 1.0
    for dim, shards_of in pieces:
        draws = jax.random.uniform(jax.random.fold_in(jax.random.fold_in(key, 6), dim), (shards_of,), jnp.float32, low / len(pieces), largest / len(pieces))
        level = level * jnp.repeat(jnp.exp(draws), dims[dim] // shards_of).reshape((-1,) + (1,) * (len(dims) - 1 - dim))
    return level


def rank_bounds(count, skew):
    weights = [(1 << 20) // math.isqrt(standing ** skew) + 1 for standing in range(1, count + 1)]
    scale = 1 + sum(weights) // (1 << 30)
    return np.cumsum(np.array([max(1, weight // scale) for weight in weights]))


def skewed_ids(own_key, extent, amount, skew):
    listing = rank_bounds(amount, skew)
    pick = jax.random.randint(jax.random.fold_in(own_key, 1), extent, 0, int(listing[amount - 1]))
    standing = jnp.searchsorted(jnp.asarray(listing, jnp.int32), pick, side="right")
    return jax.random.permutation(jax.random.fold_in(own_key, 2), amount)[standing].astype(jnp.int32)


def assign_block(rng, own, number, rows, count, top, limit, lean):
    sequence = jax.random.permutation(rng, count)
    heavy_load, ordinary = shares(count, rows * top, limit, lean, True), shares(count, rows * top, limit, lean, False)
    places = jnp.arange(count)

    def named(tallies, rotation):
        used = int((tallies > 0).sum())
        fixed = max(1, used // 4)
        moved = fixed + (places - fixed + rotation * (used - fixed)) % max(1, count - fixed)
        return jnp.zeros((count,), jnp.int32).at[sequence[jnp.where(places < fixed, places, moved)]].set(jnp.asarray(tallies, jnp.int32))

    tallies = jnp.where(number % 4 == 0, named(heavy_load, number // 4), named(ordinary, number - number // 4 - 1))
    mixed = jax.random.permutation(jax.random.fold_in(own, 3), count)
    donor, sink = mixed[0:count // 2 * 2:2], mixed[1:count // 2 * 2:2]
    slack = jnp.minimum(tallies[donor] - 1, limit - tallies[sink]) // 2
    slack = jnp.where((donor == sequence[0]) | (sink == sequence[0]) | (tallies[sink] == 0), 0, jnp.maximum(slack, 0))
    moved = jax.random.randint(jax.random.fold_in(own, 4), (count // 2,), 0, 1 << 20) % (slack + 1)
    tallies = tallies.at[donor].add(-moved).at[sink].add(moved)
    members = jnp.searchsorted(jnp.cumsum(tallies), jnp.arange(rows * top), side="right").astype(jnp.int32)
    listing = members.reshape(top, rows).T
    listing = listing[jax.random.permutation(jax.random.fold_in(own, 1), rows)]
    rotation = jax.random.randint(jax.random.fold_in(own, 2), (rows, 1), 0, top)
    return jnp.take_along_axis(listing, (jnp.arange(top)[None, :] + rotation) % top, axis=1)


def shares(count, total, limit, slope, full):
    loads = [(1 << 20) // math.isqrt(grade ** slope) + 1 for grade in range(1, count + 1)]
    largest = limit if full else min(limit, max(-(-total // count), total * loads[0] // sum(loads)))
    least = 1 if total - largest >= count - 1 else 0
    counts, rest = [largest] + [least] * (count - 1), total - largest - least * (count - 1)
    while rest > 0:
        candidates = [i for i in range(1, count) if counts[i] < largest] or [i for i in range(1, count) if counts[i] < limit]
        pool, budget = sum([loads[i] for i in candidates]), rest
        for i in candidates:
            more = min(limit - counts[i], max(1, budget * loads[i] // pool), rest)
            counts[i] = counts[i] + more
            rest = rest - more
    return np.array(counts)


def bell_draw(rng, dims, deviation, bound, cuts=(), held_as=jnp.bfloat16):
    entries = jax.random.normal(rng, dims, jnp.float32) * deviation
    if len(cuts) > 0:
        entries = shard_levels(rng, dims, cuts, -0.22, 0.18) * entries
    return jnp.clip(entries, min=-bound, max=bound).astype(held_as)


def setup_inputs(seed: int = 0) -> dict:
    splits = jax.random.split(jax.random.key(seed), 15)
    tokens = draw_tokens(jax.random.fold_in(splits[14], 71), 0)
    store = draw_store(jax.random.fold_in(splits[14], 71), 0)
    passage_holder_index_keys = jax.random.split(jax.random.fold_in(splits[2], 1), BLOCKS // NBLK_DEV)
    passage_holder_index_turns = jax.random.permutation(jax.random.fold_in(splits[2], 3), BLOCKS // NBLK_DEV)
    passage_holder_index = jax.vmap(lambda own, number: assign_block(jax.random.fold_in(splits[2], 2), own, number, NBLK_DEV, N_ST, NPB, CAP, 2))(passage_holder_index_keys, passage_holder_index_turns).reshape((BLOCKS, NPB))
    passage_slot = set_ends(skewed_ids(splits[3], (BLOCKS, NPB), P_DEV, 2), jax.random.fold_in(splits[3], 3), 0, P_DEV - 1).astype(jnp.int32)
    query_weight = bell_draw(splits[4], (D, MEM_WIDTH), D ** -0.5, 0.125, ((1, 8),))
    key_matrix = bell_draw(splits[5], (D, MEM_WIDTH), D ** -0.5, 0.125, ((1, 8),))
    value_weight = bell_draw(splits[6], (D, MEM_WIDTH), D ** -0.5, 0.125, ((1, 8),))
    outer_gate = bell_draw(splits[7], (D, FILTER_CHANNELS), D ** -0.5, 0.125, ((1, 8),))
    inner_gate = bell_draw(splits[8], (D, FILTER_CHANNELS), D ** -0.5, 0.125, ((1, 8),))
    conv_input = bell_draw(splits[9], (D, FILTER_CHANNELS), D ** -0.5, 0.125, ((1, 8),))
    conv_taps = bell_draw(splits[10], (CONV_K, FILTER_CHANNELS), CONV_K ** -0.5, 3.5, ((1, 8),))
    route_gate_projection = bell_draw(splits[11], (D, 2), D ** -0.5, 0.125)
    conv_out = bell_draw(splits[12], (FILTER_CHANNELS, D), FILTER_CHANNELS ** -0.5, 0.1875, ((0, 8),))
    memory_out = bell_draw(splits[13], (MEM_WIDTH, D), MEM_WIDTH ** -0.5, 0.1875, ((0, 8),))
    return {"tokens": tokens, "store": store, "passage_holder_index": passage_holder_index, "passage_slot": passage_slot, "query_weight": query_weight, "key_matrix": key_matrix, "value_weight": value_weight, "outer_gate": outer_gate, "inner_gate": inner_gate, "conv_input": conv_input, "conv_taps": conv_taps, "route_gate_projection": route_gate_projection, "conv_out": conv_out, "memory_out": memory_out}


def reference(tokens, store, passage_holder_index, passage_slot, query_weight, key_matrix, value_weight, outer_gate, inner_gate, conv_input, conv_taps, route_gate_projection, conv_out, memory_out):
    queries = jnp.dot(tokens, query_weight, preferred_element_type=jnp.float32).astype(jnp.bfloat16)
    outer_part = jnp.dot(tokens, outer_gate, preferred_element_type=jnp.float32)
    inner_part = jnp.dot(tokens, inner_gate, preferred_element_type=jnp.float32)
    value_part = jnp.dot(tokens, conv_input, preferred_element_type=jnp.float32)
    branch_mix = jax.nn.sigmoid(jnp.dot(tokens, route_gate_projection, preferred_element_type=jnp.float32))
    mixed_input = (inner_part * value_part).reshape(TOKENS // SEQ_LEN, SEQ_LEN, FILTER_CHANNELS)
    padded_input = jnp.pad(mixed_input, ((0, 0), (CONV_K - 1, 0), (0, 0)))
    tap_values = conv_taps.astype(jnp.float32)
    filtered_signal = tap_values[0] * padded_input[:, 0:SEQ_LEN]
    for offset in range(1, CONV_K):
        filtered_signal = filtered_signal + tap_values[offset] * padded_input[:, offset:offset + SEQ_LEN]
    conv_branch = (outer_part * filtered_signal.reshape(TOKENS, FILTER_CHANNELS)).astype(jnp.bfloat16)

    passage_ids = (passage_holder_index * P_DEV + passage_slot).reshape(-1).astype(jnp.int32)
    memory_rows = store[passage_ids].reshape(-1, D)
    passage_key_rows = jnp.dot(memory_rows, key_matrix, preferred_element_type=jnp.float32).astype(jnp.bfloat16)
    retrieved_content_vectors = jnp.dot(memory_rows, value_weight, preferred_element_type=jnp.float32).astype(jnp.bfloat16)
    passage_key_rows = passage_key_rows.reshape(BLOCKS, NPB * PLEN, HEADS, HEAD_SIZE)
    retrieved_content_vectors = retrieved_content_vectors.reshape(BLOCKS, NPB * PLEN, HEADS, HEAD_SIZE)
    query_block_rows = queries.reshape(BLOCKS, BLOCK, HEADS, HEAD_SIZE)
    scores = jnp.einsum('bqhd,bkhd->bhqk', query_block_rows.astype(jnp.float32), passage_key_rows.astype(jnp.float32)) * (HEAD_SIZE ** -0.5)
    softmax_shares = jax.nn.softmax(scores, axis=-1).astype(jnp.bfloat16)
    memory_branch = jnp.einsum('bhqk,bkhd->bqhd', softmax_shares.astype(jnp.float32), retrieved_content_vectors.astype(jnp.float32))
    memory_branch = memory_branch.reshape(TOKENS, MEM_WIDTH).astype(jnp.bfloat16)

    conv_cols = FILTER_CHANNELS // N_TP
    head_cols = MEM_WIDTH // N_TP
    summed = jnp.zeros((TOKENS, D), jnp.float32)
    for tensor_parallel_team in range(N_TP):
        conv_slice = conv_branch[:, tensor_parallel_team * conv_cols:(tensor_parallel_team + 1) * conv_cols]
        memory_slice = memory_branch[:, tensor_parallel_team * head_cols:(tensor_parallel_team + 1) * head_cols]
        share_term = (branch_mix[:, 0:1] * jnp.dot(conv_slice, conv_out[tensor_parallel_team * conv_cols:(tensor_parallel_team + 1) * conv_cols], preferred_element_type=jnp.float32)
                      + branch_mix[:, 1:2] * jnp.dot(memory_slice, memory_out[tensor_parallel_team * head_cols:(tensor_parallel_team + 1) * head_cols], preferred_element_type=jnp.float32))
        summed = summed + lax.optimization_barrier(share_term.astype(jnp.bfloat16)).astype(jnp.float32)
    return summed.astype(jnp.bfloat16)
```

```python
import jax
import jax.numpy as jnp
from jax import lax
from jax.experimental import pallas as pl
from jax.experimental.pallas import tpu as pltpu
from jax.sharding import PartitionSpec as P

HEAD_SIZE = 128
SEQ = 256
BLOCK = 128
PLEN = 64
CAP = 4
NY = 4
NXZ = 4
NST = 16
NTP = 8
MESH = pl.DeviceIdType.MESH
F32 = jnp.float32
BF16 = jnp.bfloat16


def kernel(
    tokens, store, holder, slot, wq, wo, wi, wv, wk, wval, taps, route, cout, mout,
    out,
    G, ST, WIN, WKV, TB, KS, KR, OV, WV, WS, PV, PS, Q, AS, A, W,
    lsem, stsem, ixr, ixs, kvr, kvs, agr, sib, gsend, arecv, asend,
    wloc, w1, p1, p2, wsib, wsend,
):
    st = lax.axis_index("st")
    tp = lax.axis_index("tp")
    y = lax.div(tp, 2)
    k = lax.rem(tp, 2)
    z = lax.div(st, NXZ)
    x = lax.rem(st, NXZ)
    a = (1 - k) * x + k * z
    b = (1 - k) * z + k * x

    def stidx(aa, bb):
        return (1 - k) * (bb * NXZ + aa) + k * (aa * NXZ + bb)

    def ring(v, d):
        return lax.rem(v + d + 4, 4)

    def dev_y(d):
        return (st, ring(y, d) * 2 + k)

    sibling = (st, y * 2 + (1 - k))

    def rcopy(src, dst, ssem, rsem, dev):
        return pltpu.make_async_remote_copy(
            src_ref=src, dst_ref=dst, send_sem=ssem, recv_sem=rsem,
            device_id=dev, device_id_type=MESH,
        )

    def arrived(ref, sem):
        pltpu.make_async_copy(ref, ref, sem).wait()

    def seq_of(t):
        return lax.rem(t, 4) * 2 + lax.div(t, 4)

    def rows(s, lo=0, n=SEQ):
        return pl.ds(pl.multiple_of(s * SEQ + lo, 64), n)

    loads = []
    for j, w in enumerate((wq, wo, wi, wv)):
        loads.append(pltpu.make_async_copy(w, WIN.at[:, pl.ds(j * 128, 128)], lsem.at[j]))
    for j, w in enumerate((wk, wval)):
        loads.append(pltpu.make_async_copy(w, WKV.at[:, pl.ds(j * 128, 128)], lsem.at[4 + j]))
    own = pltpu.make_async_copy(tokens, G.at[tp], lsem.at[6])
    for c in loads[4:]:
        c.start()

    def store_copy(i):
        r = pl.ds(pl.multiple_of(i * SEQ, SEQ), SEQ)
        return pltpu.make_async_copy(store.at[r, :], ST.at[r, :], stsem.at[i])

    def start_store(i, _):
        store_copy(i).start()
        return 0

    lax.fori_loop(0, 8, start_store, 0)
    for c in loads[:4]:
        c.start()
    own.start()

    def wl(cs, m):
        src = (cout, mout)[m]
        return pltpu.make_async_copy(
            src.at[:, pl.ds(pl.multiple_of(cs * 128, 128), 128)], W.at[cs, k, y, m], wloc.at[0]
        )

    def start_wl(cs, _):
        wl(cs, 0).start()
        wl(cs, 1).start()
        return 0

    lax.fori_loop(0, NST, start_wl, 0)

    bar = pltpu.get_barrier_semaphore()

    def sig_tp(d, _):
        pl.semaphore_signal(bar, inc=1, device_id=(st, lax.rem(tp + d, NTP)), device_id_type=MESH)
        return 0

    def sig_st(d, _):
        pl.semaphore_signal(bar, inc=1, device_id=(lax.rem(st + d, NST), tp), device_id_type=MESH)
        return 0

    lax.fori_loop(1, NTP, sig_tp, 0)
    lax.fori_loop(1, NST, sig_st, 0)

    rowi = lax.broadcasted_iota(jnp.int32, (NST, 128), 0)
    lanei = lax.broadcasted_iota(jnp.int32, (NST, 128), 1)
    count = jnp.zeros((NST, 128), jnp.int32)
    wanted = jnp.zeros((NST, 128), jnp.int32)
    for r in range(32):
        o = holder[r % 2, r // 2]
        v = slot[r % 2, r // 2]
        hit = rowi == o
        PV[r] = jnp.sum(jnp.where(hit, count, 0), axis=0, keepdims=True) + o * CAP
        wanted = jnp.where(hit & (lanei == count), v, wanted)
        count = count + hit.astype(jnp.int32)
    for o in range(NST):
        OV[o] = wanted[o : o + 1]
    pcopy = pltpu.make_async_copy(PV, PS, lsem.at[7])
    pcopy.start()

    pl.semaphore_wait(bar, NTP - 1 + NST - 1)

    def ix_copy(d):
        r = lax.rem(st + d, NST)
        return rcopy(OV.at[r], WV.at[st], ixs, ixr.at[st], (r, tp))

    def ix_start(d, _):
        ix_copy(d).start()
        return 0

    lax.fori_loop(1, NST, ix_start, 0)
    pltpu.make_async_copy(OV.at[st], WV.at[st], ixr.at[st]).start()

    def direct(t):
        s = seq_of(t)
        src = tokens.at[rows(s), :]
        dst = G.at[tp, rows(s), :]
        rcopy(src, dst, gsend, agr.at[t, 0], dev_y(1)).start()
        rcopy(src, dst, gsend, agr.at[t, 1], dev_y(-1)).start()
        rcopy(src, dst, gsend, sib.at[t, 0], sibling).start()

    def gblk(d):
        return ring(y, d) * 2 + k


    direct(0)
    direct(1)

    for c in loads[4:]:
        c.wait()

    def kv_body(i, _):
        store_copy(i).wait()
        r = pl.ds(pl.multiple_of(i * SEQ, SEQ), SEQ)
        kv = jnp.dot(ST[r, :], WKV[...], preferred_element_type=F32).astype(BF16)
        for j in range(4):
            TB[i * 4 + j] = kv[j * PLEN : (j + 1) * PLEN]
        return 0

    lax.fori_loop(0, 8, kv_body, 0)

    arrived(W.at[:, k, y], wloc.at[0])

    def w1_copy(dy):
        blk = W.at[st, k, y]
        return rcopy(blk, blk, wsend, w1.at[dy - 1], (st, lax.rem(y + dy, 4) * 2 + k))

    def w1_start(dy, _):
        w1_copy(dy).start()
        return 0

    lax.fori_loop(1, 4, w1_start, 0)
    rcopy(W.at[:, k, y], W.at[:, k, y], wsend, wsib.at[3], sibling).start()

    def send_kv():
        def w(r, _):
            arrived(WV.at[r], ixr.at[r])
            return 0

        lax.fori_loop(0, NST, w, 0)
        c = pltpu.make_async_copy(WV, WS, lsem.at[8])
        c.start()
        c.wait()

        def go(d, _):
            r = lax.rem(st + d, NST)
            for j in range(CAP):
                KS[r, j] = TB[WS[r, 0, j]]
            rcopy(KS.at[r], KR.at[pl.ds(st * CAP, CAP)], kvs, kvr.at[st], (r, tp)).start()
            return 0

        lax.fori_loop(1, NST, go, 0)
        for j in range(CAP):
            KS[st, j] = TB[WS[st, 0, j]]
        pltpu.make_async_copy(KS.at[st], KR.at[pl.ds(st * CAP, CAP)], kvr.at[st]).start()

    def dev_a(d):
        return (stidx(ring(a, d), b), tp)

    def dev_b(d):
        return (stidx(a, ring(b, d)), tp)

    def yo(dy):
        return lax.rem(y + dy, 4)

    def plane1():
        def go(dy, _):
            arrived(W.at[st, k, yo(4 - dy)], w1.at[dy - 1])
            return 0

        lax.fori_loop(1, 4, go, 0)

        def go2(j, _):
            da = lax.div(j, 3) + 1
            dy = lax.rem(j, 3) + 1
            blk = W.at[st, k, yo(dy)]
            rcopy(blk, blk, wsend, p1.at[j], (stidx(lax.rem(a + da, 4), b), tp)).start()
            return 0

        lax.fori_loop(0, 9, go2, 0)

    def plane2():
        def go(j, _):
            da = lax.div(j, 3) + 1
            dy = lax.rem(j, 3) + 1
            arrived(W.at[stidx(lax.rem(a + 4 - da, 4), b), k, yo(dy)], p1.at[j])
            return 0

        lax.fori_loop(0, 9, go, 0)

        def go2(j, _):
            blk = W.at[stidx(lax.div(j, 3), b), k, yo(lax.rem(j, 3) + 1)]
            rcopy(blk, blk, wsend, p2.at[0, j], dev_b(1)).start()
            rcopy(blk, blk, wsend, p2.at[1, j], dev_b(-1)).start()
            return 0

        lax.fori_loop(0, 12, go2, 0)

    def plane3():
        def blk(j, d):
            return W.at[stidx(lax.div(j, 3), ring(b, d)), k, yo(lax.rem(j, 3) + 1)]

        def go(j, _):
            arrived(blk(j, -1), p2.at[0, j])
            arrived(blk(j, 1), p2.at[1, j])
            return 0

        lax.fori_loop(0, 12, go, 0)

        def up(j, _):
            rcopy(blk(j, -1), blk(j, -1), wsend, p2.at[2, j], dev_b(1)).start()
            return 0

        def down(j, _):
            rcopy(blk(j, 1), blk(j, 1), wsend, p2.at[2, j], dev_b(-1)).start()
            return 0

        lax.fori_loop(0, 6, up, 0)
        lax.fori_loop(6, 12, down, 0)

    def plane4():
        def go(j, _):
            arrived(W.at[stidx(lax.div(j, 3), ring(b, 2)), k, yo(lax.rem(j, 3) + 1)], p2.at[2, j])
            return 0

        lax.fori_loop(0, 12, go, 0)

        def go2(dy, _):
            blk = W.at[:, k, yo(dy)]
            rcopy(blk, blk, wsend, wsib.at[dy - 1], sibling).start()
            return 0

        lax.fori_loop(1, 4, go2, 0)

    def send_branch(m, s):
        @pl.when(s != tp)
        def _():
            rcopy(AS.at[m, s], A.at[m, tp], asend, arecv.at[m, tp], (st, s)).start()

        @pl.when(s == tp)
        def _():
            pltpu.make_async_copy(AS.at[m, s], A.at[m, tp], arecv.at[m, tp]).start()

    for c in loads[:4]:
        c.wait()
    own.wait()
    rowf = lax.broadcasted_iota(jnp.int32, (SEQ, 128), 0)

    def gathered(s):
        r = rows(s)
        return jnp.concatenate([G[j, r, :] for j in range(NTP)], axis=1)

    def project(t):
        s = seq_of(t)

        def w(d):
            return G.at[ring(y, d) * 2 + (1 - k), rows(s), :]

        arrived(w(0), sib.at[t, 0])
        arrived(w(-1), sib.at[t, 1])
        arrived(w(1), sib.at[t, 2])
        arrived(w(2), sib.at[t, 3])
        p = jnp.dot(gathered(s), WIN[...], preferred_element_type=F32)
        Q[rows(s), :] = p[:, 0:128].astype(BF16)
        mixed = p[:, 256:384] * p[:, 384:512]
        tv = taps[...].astype(F32)
        m1 = jnp.where(rowf >= 1, pltpu.roll(mixed, 1, 0), 0.0)
        m2 = jnp.where(rowf >= 2, pltpu.roll(mixed, 2, 0), 0.0)
        filt = tv[0:1] * m2 + tv[1:2] * m1 + tv[2:3] * mixed
        AS[0, s] = (p[:, 128:256] * filt).astype(BF16)
        send_branch(0, s)

    HALF = SEQ // 2

    def step(t, _):
        @pl.when(t < 8)
        def _():
            s = seq_of(t)
            g = G.at[gblk(-1), rows(s), :]
            arrived(g, agr.at[t, 0])
            h = G.at[gblk(-1), rows(s, 0, HALF), :]
            rcopy(h, h, gsend, agr.at[t, 2], dev_y(1)).start()
            rcopy(g, g, gsend, sib.at[t, 1], sibling).start()
            g2 = G.at[gblk(1), rows(s), :]
            arrived(g2, agr.at[t, 1])
            h2 = G.at[gblk(1), rows(s, HALF, HALF), :]
            rcopy(h2, h2, gsend, agr.at[t, 3], dev_y(-1)).start()
            rcopy(g2, g2, gsend, sib.at[t, 2], sibling).start()

        @pl.when(t < 6)
        def _():
            direct(t + 2)

        @pl.when(t == 0)
        def _():
            send_kv()

        @pl.when(t == 1)
        def _():
            plane1()

        @pl.when(t == 3)
        def _():
            plane2()

        @pl.when(t == 6)
        def _():
            plane3()

        @pl.when((t >= 1) & (t < 9))
        def _():
            u = t - 1
            s = seq_of(u)
            arrived(G.at[gblk(2), rows(s, 0, HALF), :], agr.at[u, 2])
            arrived(G.at[gblk(2), rows(s, HALF, HALF), :], agr.at[u, 3])
            g = G.at[gblk(2), rows(s), :]
            rcopy(g, g, gsend, sib.at[u, 3], sibling).start()

        @pl.when(t >= 2)
        def _():
            project(t - 2)

        return 0

    lax.fori_loop(0, 10, step, 0)
    plane4()

    def wkv(r, _):
        arrived(KR.at[pl.ds(r * CAP, CAP)], kvr.at[r])
        return 0

    lax.fori_loop(0, NST, wkv, 0)
    pcopy.wait()

    def attend(t, _):
        s = seq_of(t)
        for h in range(2):
            n = (s * 2 + h) * 2
            kv = jnp.concatenate([KR[PS[n, 0, 0]], KR[PS[n + 1, 0, 0]]], axis=0)
            q = Q[rows(s, h * BLOCK, BLOCK), :]
            sc = lax.dot_general(
                q, kv[:, :128], (((1,), (1,)), ((), ())), preferred_element_type=F32
            ) * (HEAD_SIZE ** -0.5)
            e = jnp.exp(sc - jnp.max(sc, axis=1, keepdims=True))
            wt = (e / jnp.sum(e, axis=1, keepdims=True)).astype(BF16)
            o = jnp.dot(wt, kv[:, 128:], preferred_element_type=F32)
            AS[1, s, pl.ds(h * BLOCK, BLOCK), :] = o.astype(BF16)
        send_branch(1, s)
        return 0

    lax.fori_loop(0, 8, attend, 0)

    logits = lax.dot_general(
        gathered(tp), route[...], (((1,), (1,)), ((), ())), preferred_element_type=F32
    )
    mix = jax.nn.sigmoid(logits)
    mix0 = mix[:, 0:1]
    mix1 = mix[:, 1:2]

    def wa(j, _):
        arrived(A.at[0, j], arecv.at[0, j])
        arrived(A.at[1, j], arecv.at[1, j])
        return 0

    lax.fori_loop(0, NTP, wa, 0)

    def wws(dy, _):
        arrived(W.at[:, 1 - k, yo(dy)], wsib.at[lax.rem(dy + 3, 4)])
        return 0

    lax.fori_loop(0, 4, wws, 0)

    order = [(kk, yy) for kk in range(2) for yy in range(4)]

    def outp(c, _):
        acc = []
        for m in range(2):
            lhs = jnp.concatenate([A[m, yy * 2 + kk] for kk, yy in order], axis=1)
            rhs = jnp.concatenate(
                [
                    jnp.concatenate([W[c * 2 + h, kk, yy, m] for kk, yy in order], axis=0)
                    for h in range(2)
                ],
                axis=1,
            )
            acc.append(jnp.dot(lhs, rhs, preferred_element_type=F32))
        out[:, pl.ds(pl.multiple_of(c * 256, 256), 256)] = (mix0 * acc[0] + mix1 * acc[1]).astype(BF16)
        return 0

    lax.fori_loop(0, 8, outp, 0)

    arrived(OV.at[pl.ds(0, NST - 1)], ixs)
    arrived(KS.at[pl.ds(0, NST - 1)], kvs)
    arrived(G.at[pl.ds(0, 7)], gsend)
    arrived(AS.at[:, pl.ds(0, 7)], asend)
    arrived(W.at[pl.ds(0, 14)], wsend)


def local(
    tokens, store, holder, slot, wq, wk, wval, wo, wi, wv, taps, route, cout, mout
):
    anyspec = pl.BlockSpec(memory_space=pl.ANY)
    vmem = pl.BlockSpec(memory_space=pltpu.VMEM)
    smem = pl.BlockSpec(memory_space=pltpu.SMEM)
    dma = pltpu.SemaphoreType.DMA
    V = pltpu.VMEM
    return pl.pallas_call(
        kernel,
        out_shape=jax.ShapeDtypeStruct((SEQ, cout.shape[1]), BF16),
        in_specs=[anyspec, anyspec, smem, smem] + [anyspec] * 6 + [vmem, vmem, anyspec, anyspec],
        out_specs=vmem,
        scratch_shapes=[
            V((8, 2048, 256), BF16),
            V((2048, 2048), BF16),
            V((2048, 512), BF16),
            V((2048, 256), BF16),
            V((32, PLEN, 256), BF16),
            V((NST, CAP, PLEN, 256), BF16),
            V((NST * CAP, PLEN, 256), BF16),
            V((NST, 1, 128), jnp.int32),
            V((NST, 1, 128), jnp.int32),
            pltpu.SMEM((NST, 1, 128), jnp.int32),
            V((32, 1, 128), jnp.int32),
            pltpu.SMEM((32, 1, 128), jnp.int32),
            V((2048, 128), BF16),
            V((2, 8, SEQ, 128), BF16),
            V((2, 8, SEQ, 128), BF16),
            V((NST, 2, 4, 2, 128, 128), BF16),
            dma((9,)), dma((8,)), dma((NST,)), dma, dma((NST,)), dma,
            dma((8, 4)), dma((8, 4)), dma, dma((2, 8)), dma,
            dma((1,)), dma((3,)), dma((9,)), dma((3, 12)), dma((4,)), dma,
        ],
        compiler_params=pltpu.CompilerParams(
            collective_id=0, has_side_effects=True, vmem_limit_bytes=60 * 1024 * 1024
        ),
    )(
        tokens, store.reshape(-1, store.shape[-1]), holder.T, slot.T,
        wq, wo, wi, wv, wk, wval, taps, route.T, cout, mout,
    )


def solution(mesh):
    return jax.shard_map(
        local,
        mesh=mesh,
        in_specs=(
            P("st", "tp"), P("st", None, None), P("st", None), P("st", None),
            P(None, "tp"), P(None, "tp"), P(None, "tp"), P(None, "tp"), P(None, "tp"),
            P(None, "tp"), P(None, "tp"), P(), P("tp", None), P("tp", None),
        ),
        out_specs=P(("st", "tp"), None),
        check_vma=False,
    )
```

```python
import jax
import jax.numpy as jnp
from jax import lax
from jax.experimental import pallas as pl
from jax.experimental.pallas import tpu as pltpu
from jax.sharding import PartitionSpec as P

HEAD_SIZE = 128
SEQ = 256
BLOCK = 128
PLEN = 64
CAP = 4
NY = 4
NXZ = 4
NST = 16
NTP = 8
MESH = pl.DeviceIdType.MESH
F32 = jnp.float32
BF16 = jnp.bfloat16


def kernel(
    tokens, store, holder_h, slot_h, wq, wo, wi, wv, wk, wval, taps_h, route_h, cout, mout,
    out,
    holder, slot, taps, route, G, ST, WIN, WKV, TB, KS, KR, OV, WV, WS, PV, PS, Q, AS, A, W,
    lsem, stsem, ixr, ixs, kvr, kvs, agr, sib, gsend, arecv, asend,
    wloc, w1, p1, p2, wsib, wsown, wsend,
):
    st = lax.axis_index("st")
    tp = lax.axis_index("tp")
    y = lax.div(tp, 2)
    k = lax.rem(tp, 2)
    z = lax.div(st, NXZ)
    x = lax.rem(st, NXZ)
    a = (1 - k) * x + k * z
    b = (1 - k) * z + k * x

    def stidx(aa, bb):
        return (1 - k) * (bb * NXZ + aa) + k * (aa * NXZ + bb)

    def ring(v, d):
        return lax.rem(v + d + 4, 4)

    def dev_y(d):
        return (st, ring(y, d) * 2 + k)

    sibling = (st, y * 2 + (1 - k))

    def rcopy(src, dst, ssem, rsem, dev):
        return pltpu.make_async_remote_copy(
            src_ref=src, dst_ref=dst, send_sem=ssem, recv_sem=rsem,
            device_id=dev, device_id_type=MESH,
        )

    def arrived(ref, sem):
        pltpu.make_async_copy(ref, ref, sem).wait()

    def seq_of(t):
        return lax.rem(t, 4) * 2 + lax.div(t, 4)

    def rows(s, lo=0, n=SEQ):
        return pl.ds(pl.multiple_of(s * SEQ + lo, 64), n)

    bar = pltpu.get_barrier_semaphore()

    def sig_tp(d, _):
        pl.semaphore_signal(bar, inc=1, device_id=(st, lax.rem(tp + d, NTP)), device_id_type=MESH)
        return 0

    def sig_st(d, _):
        pl.semaphore_signal(bar, inc=1, device_id=(lax.rem(st + d, NST), tp), device_id_type=MESH)
        return 0

    lax.fori_loop(1, NTP, sig_tp, 0)
    lax.fori_loop(1, NST, sig_st, 0)

    loads = []
    for j, w in enumerate((wq, wo, wi, wv)):
        loads.append(pltpu.make_async_copy(w, WIN.at[:, pl.ds(j * 128, 128)], lsem.at[j]))
    for j, w in enumerate((wk, wval)):
        loads.append(pltpu.make_async_copy(w, WKV.at[:, pl.ds(j * 128, 128)], lsem.at[4 + j]))
    own = pltpu.make_async_copy(tokens, G.at[tp], lsem.at[6])
    small = [
        pltpu.make_async_copy(p, q, lsem.at[9 + j])
        for j, (p, q) in enumerate(((holder_h, holder), (slot_h, slot), (taps_h, taps), (route_h, route)))
    ]
    for c in small + loads[4:]:
        c.start()

    def store_copy(i):
        r = pl.ds(pl.multiple_of(i * SEQ, SEQ), SEQ)
        return pltpu.make_async_copy(store.at[r, :], ST.at[r, :], stsem.at[i])

    def start_store(i, _):
        store_copy(i).start()
        return 0

    lax.fori_loop(0, 8, start_store, 0)
    for c in loads[:4]:
        c.start()
    own.start()

    def wcol(m, cs):
        return (cout, mout)[m].at[:, pl.ds(pl.multiple_of(cs * 128, 128), 128)]

    def start_wl(cs, _):
        for m in range(2):
            pltpu.make_async_copy(wcol(m, cs), W.at[cs, k, y, m], wloc.at[0]).start()
        return 0

    lax.fori_loop(0, NST, start_wl, 0)
    for c in small[:2]:
        c.wait()

    rowi = lax.broadcasted_iota(jnp.int32, (NST, 128), 0)
    lanei = lax.broadcasted_iota(jnp.int32, (NST, 128), 1)
    count = jnp.zeros((NST, 128), jnp.int32)
    wanted = jnp.zeros((NST, 128), jnp.int32)
    for r in range(32):
        o = holder[r % 2, r // 2]
        v = slot[r % 2, r // 2]
        hit = rowi == o
        PV[r] = jnp.sum(jnp.where(hit, count, 0), axis=0, keepdims=True) + o * CAP
        wanted = jnp.where(hit & (lanei == count), v, wanted)
        count = count + hit.astype(jnp.int32)
    for o in range(NST):
        OV[o] = wanted[o : o + 1]
    pcopy = pltpu.make_async_copy(PV, PS, lsem.at[7])
    pcopy.start()

    pl.semaphore_wait(bar, NTP - 1 + NST - 1)

    def ix_copy(d):
        r = lax.rem(st + d, NST)
        return rcopy(OV.at[r], WV.at[st], ixs, ixr.at[st], (r, tp))

    def ix_start(d, _):
        ix_copy(d).start()
        return 0

    lax.fori_loop(1, NST, ix_start, 0)
    pltpu.make_async_copy(OV.at[st], WV.at[st], ixr.at[st]).start()

    def direct(t):
        s = seq_of(t)
        src = tokens.at[rows(s), :]
        dst = G.at[tp, rows(s), :]
        rcopy(src, dst, gsend, agr.at[t, 0], dev_y(1)).start()
        rcopy(src, dst, gsend, agr.at[t, 1], dev_y(-1)).start()
        rcopy(src, dst, gsend, sib.at[t, 0], sibling).start()

    def gblk(d):
        return ring(y, d) * 2 + k


    direct(0)

    def w1_start(dy, _):
        for m in range(2):
            rcopy(
                wcol(m, st), W.at[st, k, y, m], wsend, w1.at[(dy - 1) * 2 + m],
                (st, lax.rem(y + dy, 4) * 2 + k),
            ).start()
        return 0

    lax.fori_loop(1, 4, w1_start, 0)
    direct(1)

    for c in loads[4:]:
        c.wait()

    def kv_body(i, _):
        store_copy(i).wait()
        r = pl.ds(pl.multiple_of(i * SEQ, SEQ), SEQ)
        kv = jnp.dot(ST[r, :], WKV[...], preferred_element_type=F32).astype(BF16)
        for j in range(4):
            TB[i * 4 + j] = kv[j * PLEN : (j + 1) * PLEN]
        return 0

    lax.fori_loop(0, 8, kv_body, 0)

    def send_kv():
        def w(r, _):
            arrived(WV.at[r], ixr.at[r])
            return 0

        lax.fori_loop(0, NST, w, 0)
        c = pltpu.make_async_copy(WV, WS, lsem.at[8])
        c.start()
        c.wait()

        def go(d, _):
            r = lax.rem(st + d, NST)
            for j in range(CAP):
                KS[r, j] = TB[WS[r, 0, j]]
            rcopy(KS.at[r], KR.at[pl.ds(st * CAP, CAP)], kvs, kvr.at[st], (r, tp)).start()
            return 0

        lax.fori_loop(1, NST, go, 0)
        for j in range(CAP):
            KS[st, j] = TB[WS[st, 0, j]]
        pltpu.make_async_copy(KS.at[st], KR.at[pl.ds(st * CAP, CAP)], kvr.at[st]).start()

    def dev_a(d):
        return (stidx(ring(a, d), b), tp)

    def dev_b(d):
        return (stidx(a, ring(b, d)), tp)

    def yo(dy):
        return lax.rem(y + dy, 4)

    def plane1():
        def go(dy, _):
            for m in range(2):
                arrived(W.at[st, k, yo(4 - dy), m], w1.at[(dy - 1) * 2 + m])
            return 0

        lax.fori_loop(1, 4, go, 0)

        def go2(j, _):
            da = lax.div(j, 3) + 1
            dy = lax.rem(j, 3) + 1
            blk = W.at[st, k, yo(dy)]
            rcopy(blk, blk, wsend, p1.at[j], (stidx(lax.rem(a + da, 4), b), tp)).start()
            return 0

        lax.fori_loop(0, 9, go2, 0)

    def plane2():
        def go(j, _):
            da = lax.div(j, 3) + 1
            dy = lax.rem(j, 3) + 1
            arrived(W.at[stidx(lax.rem(a + 4 - da, 4), b), k, yo(dy)], p1.at[j])
            return 0

        lax.fori_loop(0, 9, go, 0)

        def go2(j, _):
            blk = W.at[stidx(lax.div(j, 3), b), k, yo(lax.rem(j, 3) + 1)]
            rcopy(blk, blk, wsend, p2.at[0, j], dev_b(1)).start()
            rcopy(blk, blk, wsend, p2.at[1, j], dev_b(-1)).start()
            return 0

        lax.fori_loop(0, 12, go2, 0)

    def wblk(j, d):
        return W.at[stidx(lax.div(j, 3), ring(b, d)), k, yo(lax.rem(j, 3) + 1)]

    def wpass(lo, hi, d, sem, dev):
        def go(j, _):
            g = wblk(j, d)
            rcopy(g, g, wsend, sem.at[j], dev).start()
            return 0

        lax.fori_loop(lo, hi, go, 0)

    def plane3():
        def go(j, _):
            arrived(wblk(j, -1), p2.at[0, j])
            arrived(wblk(j, 1), p2.at[1, j])
            return 0

        lax.fori_loop(0, 12, go, 0)
        wpass(0, 6, -1, p2.at[2], dev_b(1))
        wpass(6, 12, 1, p2.at[2], dev_b(-1))
        wpass(0, 12, 0, wsib.at[0], sibling)
        wpass(0, 12, 1, wsib.at[1], sibling)
        wpass(0, 12, -1, wsib.at[3], sibling)

    def plane4():
        def go(j, _):
            arrived(wblk(j, 2), p2.at[2, j])
            return 0

        lax.fori_loop(0, 12, go, 0)
        wpass(0, 12, 2, wsib.at[2], sibling)

    def send_branch(m, s):
        @pl.when(s != tp)
        def _():
            rcopy(AS.at[m, s], A.at[m, tp], asend, arecv.at[m, tp], (st, s)).start()

        @pl.when(s == tp)
        def _():
            pltpu.make_async_copy(AS.at[m, s], A.at[m, tp], arecv.at[m, tp]).start()

    for c in loads[:4] + small[2:]:
        c.wait()
    own.wait()
    arrived(W.at[:, k, y], wloc.at[0])
    rcopy(W.at[:, k, y], W.at[:, k, y], wsend, wsown.at[0], sibling).start()
    rowf = lax.broadcasted_iota(jnp.int32, (SEQ, 128), 0)

    def gathered(s):
        r = rows(s)
        return jnp.concatenate([G[j, r, :] for j in range(NTP)], axis=1)

    def project(t):
        s = seq_of(t)

        def w(d):
            return G.at[ring(y, d) * 2 + (1 - k), rows(s), :]

        arrived(w(0), sib.at[t, 0])
        arrived(w(-1), sib.at[t, 1])
        arrived(w(1), sib.at[t, 2])
        arrived(w(2), sib.at[t, 3])
        p = jnp.dot(gathered(s), WIN[...], preferred_element_type=F32)
        Q[rows(s), :] = p[:, 0:128].astype(BF16)
        mixed = p[:, 256:384] * p[:, 384:512]
        tv = taps[...].astype(F32)
        m1 = jnp.where(rowf >= 1, pltpu.roll(mixed, 1, 0), 0.0)
        m2 = jnp.where(rowf >= 2, pltpu.roll(mixed, 2, 0), 0.0)
        filt = tv[0:1] * m2 + tv[1:2] * m1 + tv[2:3] * mixed
        AS[0, s] = (p[:, 128:256] * filt).astype(BF16)
        send_branch(0, s)

    def wkv(r, _):
        arrived(KR.at[pl.ds(r * CAP, CAP)], kvr.at[r])
        return 0

    def attend(ts):
        parts = [(seq_of(t), h) for t in ts for h in range(2)]
        kvs_, sc = [], []
        for s, h in parts:
            n = (s * 2 + h) * 2
            kv = jnp.concatenate([KR[PS[n, 0, 0]], KR[PS[n + 1, 0, 0]]], axis=0)
            q = Q[rows(s, h * BLOCK, BLOCK), :]
            kvs_.append(kv)
            sc.append(
                lax.dot_general(
                    q, kv[:, :128], (((1,), (1,)), ((), ())), preferred_element_type=F32
                ) * (HEAD_SIZE ** -0.5)
            )
        e = [jnp.exp(v - jnp.max(v, axis=1, keepdims=True)) for v in sc]
        wt = [(v / jnp.sum(v, axis=1, keepdims=True)).astype(BF16) for v in e]
        for (s, h), kv, v in zip(parts, kvs_, wt):
            o = jnp.dot(v, kv[:, 128:], preferred_element_type=F32)
            AS[1, s, pl.ds(h * BLOCK, BLOCK), :] = o.astype(BF16)
        for t in ts:
            send_branch(1, seq_of(t))

    def attend2(i, _):
        attend([2 * i, 2 * i + 1])
        return 0

    HALF = SEQ // 2

    def step(t, _):
        @pl.when(t < 8)
        def _():
            s = seq_of(t)
            g = G.at[gblk(-1), rows(s), :]
            arrived(g, agr.at[t, 0])
            h = G.at[gblk(-1), rows(s, 0, HALF), :]
            rcopy(h, h, gsend, agr.at[t, 2], dev_y(1)).start()
            rcopy(g, g, gsend, sib.at[t, 1], sibling).start()
            g2 = G.at[gblk(1), rows(s), :]
            arrived(g2, agr.at[t, 1])
            h2 = G.at[gblk(1), rows(s, HALF, HALF), :]
            rcopy(h2, h2, gsend, agr.at[t, 3], dev_y(-1)).start()
            rcopy(g2, g2, gsend, sib.at[t, 2], sibling).start()

        @pl.when(t < 6)
        def _():
            direct(t + 2)

        @pl.when(t == 0)
        def _():
            plane1()
            send_kv()

        @pl.when(t == 2)
        def _():
            plane2()

        @pl.when((t >= 1) & (t < 9))
        def _():
            u = t - 1
            s = seq_of(u)
            arrived(G.at[gblk(2), rows(s, 0, HALF), :], agr.at[u, 2])
            arrived(G.at[gblk(2), rows(s, HALF, HALF), :], agr.at[u, 3])
            g = G.at[gblk(2), rows(s), :]
            rcopy(g, g, gsend, sib.at[u, 3], sibling).start()

        @pl.when(t >= 2)
        def _():
            project(t - 2)

        @pl.when(t == 6)
        def _():
            lax.fori_loop(0, NST, wkv, 0)
            pcopy.wait()

        @pl.when((t == 6) | (t == 7))
        def _():
            lax.fori_loop((t - 6) * 2, t - 4, attend2, 0)

        @pl.when(t >= 8)
        def _():
            attend([t - 2])

        @pl.when(t == 8)
        def _():
            plane3()

        return 0

    lax.fori_loop(0, 10, step, 0)
    plane4()

    logits = lax.dot_general(
        gathered(tp), route[...], (((1,), (1,)), ((), ())), preferred_element_type=F32
    )
    mix = jax.nn.sigmoid(logits)
    mix0 = mix[:, 0:1]
    mix1 = mix[:, 1:2]

    def wa(j, _):
        arrived(A.at[0, j], arecv.at[0, j])
        arrived(A.at[1, j], arecv.at[1, j])
        return 0

    lax.fori_loop(0, NTP, wa, 0)

    def wws(j, _):
        for d in range(4):
            bs = lax.rem((1 - k) * x + k * z + d, 4)
            i = lax.div(j, 3)
            blk = (1 - k) * (i * NXZ + bs) + k * (bs * NXZ + i)
            arrived(W.at[blk, 1 - k, yo(lax.rem(j, 3) + 1)], wsib.at[d, j])
        return 0

    arrived(W.at[:, 1 - k, y], wsown.at[0])
    lax.fori_loop(0, 12, wws, 0)

    order = [(kk, yy) for kk in range(2) for yy in range(4)]

    def outp(c, _):
        acc = []
        for m in range(2):
            lhs = jnp.concatenate([A[m, yy * 2 + kk] for kk, yy in order], axis=1)
            rhs = jnp.concatenate(
                [
                    jnp.concatenate([W[c * 2 + h, kk, yy, m] for kk, yy in order], axis=0)
                    for h in range(2)
                ],
                axis=1,
            )
            acc.append(jnp.dot(lhs, rhs, preferred_element_type=F32))
        out[:, pl.ds(pl.multiple_of(c * 256, 256), 256)] = (mix0 * acc[0] + mix1 * acc[1]).astype(BF16)
        return 0

    lax.fori_loop(0, 8, outp, 0)

    arrived(OV.at[pl.ds(0, NST - 1)], ixs)
    arrived(KS.at[pl.ds(0, NST - 1)], kvs)
    arrived(G.at[pl.ds(0, 7)], gsend)
    arrived(AS.at[:, pl.ds(0, 7)], asend)
    arrived(W.at[pl.ds(0, 14)], wsend)


def local(
    tokens, store, holder, slot, wq, wk, wval, wo, wi, wv, taps, route, cout, mout
):
    hbm = pl.BlockSpec(memory_space=pltpu.HBM)
    vmem = pl.BlockSpec(memory_space=pltpu.VMEM)
    dma = pltpu.SemaphoreType.DMA
    V = pltpu.VMEM
    return pl.pallas_call(
        kernel,
        out_shape=jax.ShapeDtypeStruct((SEQ, cout.shape[1]), BF16),
        in_specs=[hbm] * 14,
        out_specs=vmem,
        scratch_shapes=[
            pltpu.SMEM((2, 16), jnp.int32),
            pltpu.SMEM((2, 16), jnp.int32),
            V((3, 128), BF16),
            V((2, 2048), BF16),
            V((8, 2048, 256), BF16),
            V((2048, 2048), BF16),
            V((2048, 512), BF16),
            V((2048, 256), BF16),
            V((32, PLEN, 256), BF16),
            V((NST, CAP, PLEN, 256), BF16),
            V((NST * CAP, PLEN, 256), BF16),
            V((NST, 1, 128), jnp.int32),
            V((NST, 1, 128), jnp.int32),
            pltpu.SMEM((NST, 1, 128), jnp.int32),
            V((32, 1, 128), jnp.int32),
            pltpu.SMEM((32, 1, 128), jnp.int32),
            V((2048, 128), BF16),
            V((2, 8, SEQ, 128), BF16),
            V((2, 8, SEQ, 128), BF16),
            V((NST, 2, 4, 2, 128, 128), BF16),
            dma((13,)), dma((8,)), dma((NST,)), dma, dma((NST,)), dma,
            dma((8, 4)), dma((8, 4)), dma, dma((2, 8)), dma,
            dma((1,)), dma((6,)), dma((9,)), dma((3, 12)), dma((4, 12)), dma((1,)), dma,
        ],
        compiler_params=pltpu.CompilerParams(
            collective_id=0, has_side_effects=True, vmem_limit_bytes=44 * 1024 * 1024
        ),
    )(
        *(
            pltpu.with_memory_space_constraint(v, pltpu.HBM)
            for v in (
                tokens, store.reshape(-1, store.shape[-1]), holder.T, slot.T,
                wq, wo, wi, wv, wk, wval, taps, route.T, cout, mout,
            )
        )
    )


def solution(mesh):
    return jax.shard_map(
        local,
        mesh=mesh,
        in_specs=(
            P("st", "tp"), P("st", None, None), P("st", None), P("st", None),
            P(None, "tp"), P(None, "tp"), P(None, "tp"), P(None, "tp"), P(None, "tp"),
            P(None, "tp"), P(None, "tp"), P(), P("tp", None), P("tp", None),
        ),
        out_specs=P(("st", "tp"), None),
        check_vma=False,
    )
```

```python
import jax
import jax.numpy as jnp
from jax import lax
from jax.experimental import pallas as pl
from jax.experimental.pallas import tpu as pltpu
from jax.sharding import PartitionSpec as P

HEAD_SIZE = 128
SEQ = 256
BLOCK = 128
PLEN = 64
CAP = 4
NY = 4
NXZ = 4
NST = 16
NTP = 8
MESH = pl.DeviceIdType.MESH
F32 = jnp.float32
BF16 = jnp.bfloat16


def kernel(
    tokens, store, holder_h, slot_h, wq, wo, wi, wv, wk, wval, taps_h, route_h, cout, mout,
    out,
    OB, holder, slot, taps, route, G, ST, WIN, WKV, TB, KS, KR, OV, WV, WS, PV, PS, Q, AS, A, W,
    lsem, stsem, ixr, ixs, kvr, kvs, agr, sib, gsend, arecv, asend,
    wloc, w1, p1, p2, wsib, wsown, wsend, osem,
):
    st = lax.axis_index("st")
    tp = lax.axis_index("tp")
    y = lax.div(tp, 2)
    k = lax.rem(tp, 2)
    z = lax.div(st, NXZ)
    x = lax.rem(st, NXZ)
    a = (1 - k) * x + k * z
    b = (1 - k) * z + k * x

    def stidx(aa, bb):
        return (1 - k) * (bb * NXZ + aa) + k * (aa * NXZ + bb)

    def ring(v, d):
        return lax.rem(v + d + 4, 4)

    def dev_y(d):
        return (st, ring(y, d) * 2 + k)

    sibling = (st, y * 2 + (1 - k))

    def rcopy(src, dst, ssem, rsem, dev):
        return pltpu.make_async_remote_copy(
            src_ref=src, dst_ref=dst, send_sem=ssem, recv_sem=rsem,
            device_id=dev, device_id_type=MESH,
        )

    def arrived(ref, sem):
        pltpu.make_async_copy(ref, ref, sem).wait()

    def seq_of(t):
        return lax.rem(t, 4) * 2 + lax.div(t, 4)

    def rows(s, lo=0, n=SEQ):
        return pl.ds(pl.multiple_of(s * SEQ + lo, 64), n)

    bar = pltpu.get_barrier_semaphore()

    def sig_tp(d, _):
        pl.semaphore_signal(bar, inc=1, device_id=(st, lax.rem(tp + d, NTP)), device_id_type=MESH)
        return 0

    def sig_st(d, _):
        pl.semaphore_signal(bar, inc=1, device_id=(lax.rem(st + d, NST), tp), device_id_type=MESH)
        return 0

    lax.fori_loop(1, NTP, sig_tp, 0)
    lax.fori_loop(1, NST, sig_st, 0)

    loads = []
    for j, w in enumerate((wq, wo, wi, wv)):
        loads.append(pltpu.make_async_copy(w, WIN.at[:, pl.ds(j * 128, 128)], lsem.at[0]))
    for j, w in enumerate((wk, wval)):
        loads.append(pltpu.make_async_copy(w, WKV.at[:, pl.ds(j * 128, 128)], lsem.at[1]))
    own = pltpu.make_async_copy(tokens, G.at[tp], lsem.at[2])
    small = [
        pltpu.make_async_copy(p, q, lsem.at[3 + j])
        for j, (p, q) in enumerate(((holder_h, holder), (slot_h, slot), (taps_h, taps), (route_h, route)))
    ]
    for c in small + loads[4:]:
        c.start()

    def store_copy(i):
        r = pl.ds(pl.multiple_of(i * SEQ, SEQ), SEQ)
        return pltpu.make_async_copy(store.at[r, :], ST.at[r, :], stsem.at[i])

    def start_store(i, _):
        store_copy(i).start()
        return 0

    lax.fori_loop(0, 8, start_store, 0)
    for c in loads[:4]:
        c.start()
    own.start()

    def wcol(m, cs):
        return (cout, mout)[m].at[:, pl.ds(pl.multiple_of(cs * 128, 128), 128)]

    def start_wl(cs, _):
        for m in range(2):
            pltpu.make_async_copy(wcol(m, cs), W.at[cs, k, y, m], wloc).start()
        return 0

    lax.fori_loop(0, NST, start_wl, 0)
    for c in small[:2]:
        c.wait()

    rowi = lax.broadcasted_iota(jnp.int32, (NST, 128), 0)
    lanei = lax.broadcasted_iota(jnp.int32, (NST, 128), 1)
    count = jnp.zeros((NST, 128), jnp.int32)
    wanted = jnp.zeros((NST, 128), jnp.int32)
    for r in range(32):
        o = holder[r % 2, r // 2]
        v = slot[r % 2, r // 2]
        hit = rowi == o
        PV[r] = jnp.sum(jnp.where(hit, count, 0), axis=0, keepdims=True) + o * CAP
        wanted = jnp.where(hit & (lanei == count), v, wanted)
        count = count + hit.astype(jnp.int32)
    for o in range(NST):
        OV[o] = wanted[o : o + 1]
    pcopy = pltpu.make_async_copy(PV, PS, lsem.at[7])
    pcopy.start()

    pl.semaphore_wait(bar, NTP - 1 + NST - 1)

    def ix_copy(d):
        r = lax.rem(st + d, NST)
        return rcopy(OV.at[r], WV.at[st], ixs, ixr, (r, tp))

    def ix_start(d, _):
        ix_copy(d).start()
        return 0

    lax.fori_loop(1, NST, ix_start, 0)
    pltpu.make_async_copy(OV.at[st], WV.at[st], ixr).start()

    def direct(t):
        s = seq_of(t)
        src = tokens.at[rows(s), :]
        dst = G.at[tp, rows(s), :]
        rcopy(src, dst, gsend, agr.at[t, 0], dev_y(1)).start()
        rcopy(src, dst, gsend, agr.at[t, 1], dev_y(-1)).start()
        rcopy(src, dst, gsend, sib.at[t], sibling).start()

    def gblk(d):
        return ring(y, d) * 2 + k


    def w1_start(dy, _):
        for m in range(2):
            rcopy(
                wcol(m, st), W.at[st, k, y, m], wsend, w1,
                (st, lax.rem(y + dy, 4) * 2 + k),
            ).start()
        return 0

    lax.fori_loop(1, 4, w1_start, 0)
    direct(0)
    direct(1)

    arrived(WKV, lsem.at[1])

    def kv_body(i, _):
        store_copy(i).wait()
        r = pl.ds(pl.multiple_of(i * SEQ, SEQ), SEQ)
        kv = jnp.dot(ST[r, :], WKV[...], preferred_element_type=F32).astype(BF16)
        for j in range(4):
            TB[i * 4 + j] = kv[j * PLEN : (j + 1) * PLEN]
        return 0

    lax.fori_loop(0, 8, kv_body, 0)

    def send_kv():
        arrived(WV, ixr)
        c = pltpu.make_async_copy(WV, WS, lsem.at[3])
        c.start()
        c.wait()
        lax.fori_loop(1, NST, kv_out, 0)
        for j in range(CAP):
            KS[st, j] = TB[WS[st, 0, j]]
        pltpu.make_async_copy(KS.at[st], KR.at[pl.ds(st * CAP, CAP)], kvr).start()

    def kv_out(d, _):
        r = lax.rem(st + d, NST)
        for j in range(CAP):
            KS[r, j] = TB[WS[r, 0, j]]
        rcopy(KS.at[r], KR.at[pl.ds(st * CAP, CAP)], kvs, kvr, (r, tp)).start()
        return 0

    def dev_a(d):
        return (stidx(ring(a, d), b), tp)

    def dev_b(d):
        return (stidx(a, ring(b, d)), tp)

    def yo(dy):
        return lax.rem(y + dy, 4)

    def plane1():
        arrived(W.at[pl.ds(0, 3), 0, 0], w1)

        def go2(j, _):
            da = lax.div(j, 3) + 1
            dy = lax.rem(j, 3) + 1
            blk = W.at[st, k, yo(dy)]
            rcopy(blk, blk, wsend, p1, (stidx(lax.rem(a + da, 4), b), tp)).start()
            return 0

        lax.fori_loop(0, 9, go2, 0)

    def wblk(j, d):
        return W.at[stidx(lax.div(j, 3), ring(b, d)), k, yo(lax.rem(j, 3) + 1)]

    def wpass(d, sem, dev):
        def go(j, _):
            g = wblk(j, d)
            rcopy(g, g, wsend, sem, dev).start()
            return 0

        lax.fori_loop(0, 12, go, 0)

    TWELVE = W.at[pl.ds(0, 3), 0]

    def plane2():
        arrived(W.at[pl.ds(0, 9), 0, 0], p1)

        def go(j, _):
            g = wblk(j, 0)
            rcopy(g, g, wsend, p2.at[0], dev_b(1)).start()
            rcopy(g, g, wsend, p2.at[1], dev_b(-1)).start()
            return 0

        lax.fori_loop(0, 12, go, 0)
        wpass(0, p2.at[2], dev_b(2))
        wpass(0, wsib.at[0], sibling)

    def plane3():
        arrived(TWELVE, p2.at[0])
        wpass(-1, wsib.at[1], sibling)
        arrived(TWELVE, p2.at[1])
        wpass(1, wsib.at[2], sibling)

    def plane4():
        arrived(TWELVE, p2.at[2])
        wpass(2, wsib.at[3], sibling)

    plane1()
    send_kv()

    def send_branch(m, s):
        @pl.when(s != tp)
        def _():
            rcopy(AS.at[m, s], A.at[m, tp], asend, arecv, (st, s)).start()

        @pl.when(s == tp)
        def _():
            pltpu.make_async_copy(AS.at[m, s], A.at[m, tp], arecv).start()

    arrived(WIN, lsem.at[0])
    for c in small[2:]:
        c.wait()
    own.wait()
    arrived(W.at[:, k, y], wloc)
    rcopy(W.at[:, k, y], W.at[:, k, y], wsend, wsown, sibling).start()
    rowf = lax.broadcasted_iota(jnp.int32, (SEQ, 128), 0)

    def gathered(s):
        r = rows(s)
        return jnp.concatenate([G[j, r, :] for j in range(NTP)], axis=1)

    def project(t):
        s = seq_of(t)

        arrived(G.at[pl.ds(0, 4), rows(s), :], sib.at[t])
        p = jnp.dot(gathered(s), WIN[...], preferred_element_type=F32)
        Q[rows(s), :] = p[:, 0:128].astype(BF16)
        mixed = p[:, 256:384] * p[:, 384:512]
        tv = taps[...].astype(F32)
        m1 = jnp.where(rowf >= 1, pltpu.roll(mixed, 1, 0), 0.0)
        m2 = jnp.where(rowf >= 2, pltpu.roll(mixed, 2, 0), 0.0)
        filt = tv[0:1] * m2 + tv[1:2] * m1 + tv[2:3] * mixed
        AS[0, s] = (p[:, 128:256] * filt).astype(BF16)
        send_branch(0, s)

    def attend(ts):
        parts = [(seq_of(t), h) for t in ts for h in range(2)]
        kvs_, sc = [], []
        for s, h in parts:
            n = (s * 2 + h) * 2
            kv = jnp.concatenate([KR[PS[n, 0, 0]], KR[PS[n + 1, 0, 0]]], axis=0)
            q = Q[rows(s, h * BLOCK, BLOCK), :]
            kvs_.append(kv)
            sc.append(
                lax.dot_general(
                    q, kv[:, :128], (((1,), (1,)), ((), ())), preferred_element_type=F32
                ) * (HEAD_SIZE ** -0.5)
            )
        e = [jnp.exp(v - jnp.max(v, axis=1, keepdims=True)) for v in sc]
        wt = [(v / jnp.sum(v, axis=1, keepdims=True)).astype(BF16) for v in e]
        for (s, h), kv, v in zip(parts, kvs_, wt):
            o = jnp.dot(v, kv[:, 128:], preferred_element_type=F32)
            AS[1, s, pl.ds(h * BLOCK, BLOCK), :] = o.astype(BF16)
        for t in ts:
            send_branch(1, seq_of(t))

    def attend2(i, _):
        attend([2 * i, 2 * i + 1])
        return 0

    HALF = SEQ // 2

    def step(t, _):
        @pl.when(t < 8)
        def _():
            s = seq_of(t)
            g = G.at[gblk(-1), rows(s), :]
            arrived(g, agr.at[t, 0])
            h = G.at[gblk(-1), rows(s, 0, HALF), :]
            rcopy(h, h, gsend, agr.at[t, 2], dev_y(1)).start()
            rcopy(g, g, gsend, sib.at[t], sibling).start()
            g2 = G.at[gblk(1), rows(s), :]
            arrived(g2, agr.at[t, 1])
            h2 = G.at[gblk(1), rows(s, HALF, HALF), :]
            rcopy(h2, h2, gsend, agr.at[t, 2], dev_y(-1)).start()
            rcopy(g2, g2, gsend, sib.at[t], sibling).start()

        @pl.when(t < 6)
        def _():
            direct(t + 2)

        @pl.when(t == 3)
        def _():
            plane2()

        @pl.when((t >= 1) & (t < 9))
        def _():
            u = t - 1
            s = seq_of(u)
            arrived(G.at[gblk(2), rows(s), :], agr.at[u, 2])
            g = G.at[gblk(2), rows(s), :]
            rcopy(g, g, gsend, sib.at[u], sibling).start()

        @pl.when(t == 8)
        def _():
            attend2(2, 0)

        @pl.when(t >= 2)
        def _():
            project(t - 2)

        @pl.when(t == 7)
        def _():
            arrived(KR, kvr)
            pcopy.wait()

        @pl.when(t == 7)
        def _():
            lax.fori_loop(0, 2, attend2, 0)

        @pl.when(t >= 8)
        def _():
            attend([t - 2])

        @pl.when(t == 8)
        def _():
            plane3()


        return 0

    lax.fori_loop(0, 10, step, 0)
    plane4()

    logits = lax.dot_general(
        gathered(tp), route[...], (((1,), (1,)), ((), ())), preferred_element_type=F32
    )
    mix = jax.nn.sigmoid(logits)
    mix0 = mix[:, 0:1]
    mix1 = mix[:, 1:2]

    arrived(A, arecv)

    arrived(W.at[:, 1 - k, y], wsown)
    for d in range(4):
        arrived(TWELVE, wsib.at[d])

    order = [(kk, yy) for kk in range(2) for yy in range(4)]

    def outp(c, _):
        acc = []
        for m in range(2):
            lhs = jnp.concatenate([A[m, yy * 2 + kk] for kk, yy in order], axis=1)
            rhs = jnp.concatenate(
                [
                    jnp.concatenate([W[c * 2 + h, kk, yy, m] for kk, yy in order], axis=0)
                    for h in range(2)
                ],
                axis=1,
            )
            acc.append(jnp.dot(lhs, rhs, preferred_element_type=F32))
        OB[c] = (mix0 * acc[0] + mix1 * acc[1]).astype(BF16)
        put(c).start()
        return 0

    def put(c):
        return pltpu.make_async_copy(
            OB.at[c], out.at[:, pl.ds(pl.multiple_of(c * 256, 256), 256)], osem
        )

    lax.fori_loop(0, 8, outp, 0)

    arrived(OB, osem)
    arrived(OV.at[pl.ds(0, NST - 1)], ixs)
    arrived(KS.at[pl.ds(0, NST - 1)], kvs)
    arrived(G.at[pl.ds(0, 7)], gsend)
    arrived(AS.at[:, pl.ds(0, 7)], asend)
    arrived(W.at[pl.ds(0, 14)], wsend)


def local(
    tokens, store, holder, slot, wq, wk, wval, wo, wi, wv, taps, route, cout, mout
):
    hbm = pl.BlockSpec(memory_space=pltpu.HBM)
    dma = pltpu.SemaphoreType.DMA
    V = pltpu.VMEM
    return pl.pallas_call(
        kernel,
        out_shape=jax.ShapeDtypeStruct((SEQ, cout.shape[1]), BF16),
        in_specs=[hbm] * 14,
        out_specs=pl.BlockSpec(memory_space=pl.ANY),
        scratch_shapes=[
            V((8, SEQ, 256), BF16),
            pltpu.SMEM((2, 16), jnp.int32),
            pltpu.SMEM((2, 16), jnp.int32),
            V((3, 128), BF16),
            V((2, 2048), BF16),
            V((8, 2048, 256), BF16),
            V((2048, 2048), BF16),
            V((2048, 512), BF16),
            V((2048, 256), BF16),
            V((32, PLEN, 256), BF16),
            V((NST, CAP, PLEN, 256), BF16),
            V((NST * CAP, PLEN, 256), BF16),
            V((NST, 1, 128), jnp.int32),
            V((NST, 1, 128), jnp.int32),
            pltpu.SMEM((NST, 1, 128), jnp.int32),
            V((32, 1, 128), jnp.int32),
            pltpu.SMEM((32, 1, 128), jnp.int32),
            V((2048, 128), BF16),
            V((2, 8, SEQ, 128), BF16),
            V((2, 8, SEQ, 128), BF16),
            V((NST, 2, 4, 2, 128, 128), BF16),
            dma((8,)), dma((8,)), dma, dma, dma, dma,
            dma((8, 3)), dma((8,)), dma, dma, dma,
            dma, dma, dma, dma((3,)), dma((4,)), dma, dma, dma,
        ],
        compiler_params=pltpu.CompilerParams(
            collective_id=0, has_side_effects=True, vmem_limit_bytes=44 * 1024 * 1024
        ),
    )(
        *(
            pltpu.with_memory_space_constraint(v, pltpu.HBM)
            for v in (
                tokens, store.reshape(-1, store.shape[-1]), holder.T, slot.T,
                wq, wo, wi, wv, wk, wval, taps, route.T, cout, mout,
            )
        )
    )


def solution(mesh):
    return jax.shard_map(
        local,
        mesh=mesh,
        in_specs=(
            P("st", "tp"), P("st", None, None), P("st", None), P("st", None),
            P(None, "tp"), P(None, "tp"), P(None, "tp"), P(None, "tp"), P(None, "tp"),
            P(None, "tp"), P(None, "tp"), P(), P("tp", None), P("tp", None),
        ),
        out_specs=P(("st", "tp"), None),
        check_vma=False,
    )
```

```python
import jax
import jax.numpy as jnp
from jax import lax
from jax.experimental import pallas as pl
from jax.experimental.pallas import tpu as pltpu
from jax.sharding import PartitionSpec as P

HEAD_SIZE = 128
SEQ = 256
BLOCK = 128
PLEN = 64
CAP = 4
NY = 4
NXZ = 4
NST = 16
NTP = 8
STEP = 32
MESH = pl.DeviceIdType.MESH
F32 = jnp.float32
BF16 = jnp.bfloat16


def kernel(
    tokens, store, holder_h, slot_h, wq, wo, wi, wv, wk, wval, taps_h, route_h, cout, mout,
    out,
    AC, PM, OB, holder, slot, taps, route, G, ST, WIN, WKV, TB, KS, KR, OV, WV, WS, PV, PS, Q, AS, A, W,
    lsem, stsem, ixr, ixs, kvr, kvs, agr, sib, gsend, arecv, asend,
    wloc, w1, p1, p2, wsib, wsown, wsend, osem,
):
    st = lax.axis_index("st")
    tp = lax.axis_index("tp")
    y = lax.div(tp, 2)
    k = lax.rem(tp, 2)
    z = lax.div(st, NXZ)
    x = lax.rem(st, NXZ)
    a = (1 - k) * x + k * z
    b = (1 - k) * z + k * x

    def stidx(aa, bb):
        return (1 - k) * (bb * NXZ + aa) + k * (aa * NXZ + bb)

    def ring(v, d):
        return lax.rem(v + d + 4, 4)

    def dev_y(d):
        return (st, ring(y, d) * 2 + k)

    sibling = (st, y * 2 + (1 - k))

    def rcopy(src, dst, ssem, rsem, dev):
        return pltpu.make_async_remote_copy(
            src_ref=src, dst_ref=dst, send_sem=ssem, recv_sem=rsem,
            device_id=dev, device_id_type=MESH,
        )

    def arrived(ref, sem):
        pltpu.make_async_copy(ref, ref, sem).wait()

    def rows(t):
        return pl.ds(pl.multiple_of(t * STEP, STEP), STEP)

    bar = pltpu.get_barrier_semaphore()

    def sig_tp(d, _):
        pl.semaphore_signal(bar, inc=1, device_id=(st, lax.rem(tp + d, NTP)), device_id_type=MESH)
        return 0

    def sig_st(d, _):
        pl.semaphore_signal(bar, inc=1, device_id=(lax.rem(st + d, NST), tp), device_id_type=MESH)
        return 0

    lax.fori_loop(1, NTP, sig_tp, 0)
    lax.fori_loop(1, NST, sig_st, 0)

    loads = []
    for j, w in enumerate((wq, wo, wi, wv)):
        loads.append(pltpu.make_async_copy(w, WIN.at[:, pl.ds(j * 128, 128)], lsem.at[0]))
    for j, w in enumerate((wk, wval)):
        loads.append(pltpu.make_async_copy(w, WKV.at[:, pl.ds(j * 128, 128)], lsem.at[1]))
    own = pltpu.make_async_copy(tokens, G.at[tp], lsem.at[2])
    small = [
        pltpu.make_async_copy(p, q, lsem.at[3 + j])
        for j, (p, q) in enumerate(((holder_h, holder), (slot_h, slot), (taps_h, taps), (route_h, route)))
    ]
    for c in small + loads[4:]:
        c.start()

    def store_copy(i):
        r = pl.ds(pl.multiple_of(i * SEQ, SEQ), SEQ)
        return pltpu.make_async_copy(store.at[r, :], ST.at[r, :], stsem.at[i])

    def start_store(i, _):
        store_copy(i).start()
        return 0

    lax.fori_loop(0, 8, start_store, 0)
    for c in loads[:4]:
        c.start()
    own.start()

    def wcol(m, cs):
        return (cout, mout)[m].at[:, pl.ds(pl.multiple_of(cs * 128, 128), 128)]

    def start_wl(cs, _):
        for m in range(2):
            pltpu.make_async_copy(wcol(m, cs), W.at[cs, k, y, m], wloc).start()
        return 0

    lax.fori_loop(0, NST, start_wl, 0)
    for c in small[:2]:
        c.wait()

    rowi = lax.broadcasted_iota(jnp.int32, (NST, 128), 0)
    lanei = lax.broadcasted_iota(jnp.int32, (NST, 128), 1)
    count = jnp.zeros((NST, 128), jnp.int32)
    wanted = jnp.zeros((NST, 128), jnp.int32)
    for r in range(32):
        o = holder[r % 2, r // 2]
        v = slot[r % 2, r // 2]
        hit = rowi == o
        PV[r] = jnp.sum(jnp.where(hit, count, 0), axis=0, keepdims=True) + o * CAP
        wanted = jnp.where(hit & (lanei == count), v, wanted)
        count = count + hit.astype(jnp.int32)
    for o in range(NST):
        OV[o] = wanted[o : o + 1]
    pcopy = pltpu.make_async_copy(PV, PS, lsem.at[7])
    pcopy.start()

    pl.semaphore_wait(bar, NTP - 1 + NST - 1)

    def ix_copy(d):
        r = lax.rem(st + d, NST)
        return rcopy(OV.at[r], WV.at[st], ixs, ixr, (r, tp))

    def ix_start(d, _):
        ix_copy(d).start()
        return 0

    lax.fori_loop(1, NST, ix_start, 0)
    pltpu.make_async_copy(OV.at[st], WV.at[st], ixr).start()

    def direct(t):
        src = tokens.at[:, rows(t), :]
        dst = G.at[tp, :, rows(t), :]
        rcopy(src, dst, gsend, agr.at[t, 0], dev_y(1)).start()
        rcopy(src, dst, gsend, agr.at[t, 1], dev_y(-1)).start()
        rcopy(src, dst, gsend, sib.at[t], sibling).start()

    def gblk(d):
        return ring(y, d) * 2 + k


    def w1_start(dy, _):
        for m in range(2):
            rcopy(
                wcol(m, st), W.at[st, k, y, m], wsend, w1,
                (st, lax.rem(y + dy, 4) * 2 + k),
            ).start()
        return 0

    lax.fori_loop(1, 4, w1_start, 0)
    direct(0)
    direct(1)

    arrived(WKV, lsem.at[1])

    def kv_body(i, _):
        store_copy(i).wait()
        r = pl.ds(pl.multiple_of(i * SEQ, SEQ), SEQ)
        kv = jnp.dot(ST[r, :], WKV[...], preferred_element_type=F32).astype(BF16)
        for j in range(4):
            TB[i * 4 + j] = kv[j * PLEN : (j + 1) * PLEN]
        return 0

    lax.fori_loop(0, 6, kv_body, 0)

    def send_kv():
        arrived(WV, ixr)
        c = pltpu.make_async_copy(WV, WS, lsem.at[3])
        c.start()
        c.wait()
        lax.fori_loop(1, NST, kv_out, 0)
        for j in range(CAP):
            KS[st, j] = TB[WS[st, 0, j]]
        pltpu.make_async_copy(KS.at[st], KR.at[pl.ds(st * CAP, CAP)], kvr).start()

    def kv_out(d, _):
        r = lax.rem(st + d, NST)
        for j in range(CAP):
            KS[r, j] = TB[WS[r, 0, j]]
        rcopy(KS.at[r], KR.at[pl.ds(st * CAP, CAP)], kvs, kvr, (r, tp)).start()
        return 0

    def dev_a(d):
        return (stidx(ring(a, d), b), tp)

    def dev_b(d):
        return (stidx(a, ring(b, d)), tp)

    def yo(dy):
        return lax.rem(y + dy, 4)

    def plane1():
        arrived(W.at[pl.ds(0, 3), 0, 0], w1)

        def go2(j, _):
            da = lax.div(j, 3) + 1
            dy = lax.rem(j, 3) + 1
            blk = W.at[st, k, yo(dy)]
            rcopy(blk, blk, wsend, p1, (stidx(lax.rem(a + da, 4), b), tp)).start()
            return 0

        lax.fori_loop(0, 9, go2, 0)

    def wblk(j, d):
        return W.at[stidx(lax.div(j, 3), ring(b, d)), k, yo(lax.rem(j, 3) + 1)]

    def wpass(lo, hi, d, sem, dev):
        def go(j, _):
            g = wblk(j, d)
            rcopy(g, g, wsend, sem, dev).start()
            return 0

        lax.fori_loop(lo, hi, go, 0)

    TWELVE = W.at[pl.ds(0, 3), 0]

    def plane2():
        arrived(W.at[pl.ds(0, 9), 0, 0], p1)

        def go(j, _):
            g = wblk(j, 0)
            rcopy(g, g, wsend, p2.at[0], dev_b(1)).start()
            rcopy(g, g, wsend, p2.at[1], dev_b(-1)).start()
            return 0

        lax.fori_loop(0, 12, go, 0)
        wpass(0, 12, 0, wsib.at[0], sibling)

    def plane3():
        arrived(TWELVE, p2.at[0])
        arrived(TWELVE, p2.at[1])
        wpass(0, 6, -1, p2.at[2], dev_b(1))
        wpass(6, 12, 1, p2.at[2], dev_b(-1))
        wpass(0, 12, -1, wsib.at[1], sibling)
        wpass(0, 12, 1, wsib.at[2], sibling)

    def plane4():
        arrived(TWELVE, p2.at[2])
        wpass(0, 12, 2, wsib.at[3], sibling)

    plane1()
    lax.fori_loop(6, 8, kv_body, 0)
    send_kv()

    def send_branch(m, lo, n):
        r = pl.ds(pl.multiple_of(lo, STEP), n)

        def go(d, _):
            s = lax.rem(tp + d, NTP)
            rcopy(AS.at[m, s, r, :], A.at[m, tp, r, :], asend, arecv.at[m], (st, s)).start()
            return 0

        lax.fori_loop(1, NTP, go, 0)
        pltpu.make_async_copy(AS.at[m, tp, r, :], A.at[m, tp, r, :], arecv.at[m]).start()

    arrived(WIN, lsem.at[0])
    for c in small[2:]:
        c.wait()
    own.wait()
    arrived(W.at[:, k, y], wloc)
    rcopy(W.at[:, k, y], W.at[:, k, y], wsend, wsown, sibling).start()
    PM[...] = jnp.zeros_like(PM)
    place = lax.rem(lax.broadcasted_iota(jnp.int32, (SEQ, 128), 0), STEP)

    def project(t):
        arrived(G.at[pl.ds(0, 4), :, rows(t), :], sib.at[t])
        rws = jnp.concatenate([G[j, :, rows(t), :].reshape(SEQ, 256) for j in range(NTP)], axis=1)
        p = jnp.dot(rws, WIN[...], preferred_element_type=F32)
        Q[:, rows(t), :] = p[:, 0:128].astype(BF16).reshape(NTP, STEP, 128)
        mixed = p[:, 256:384] * p[:, 384:512]
        prev = PM[...]
        PM[...] = mixed
        tv = taps[...].astype(F32)
        m1 = jnp.where(place >= 1, pltpu.roll(mixed, 1, 0), pltpu.roll(prev, SEQ + 1 - STEP, 0))
        m2 = jnp.where(place >= 2, pltpu.roll(mixed, 2, 0), pltpu.roll(prev, SEQ + 2 - STEP, 0))
        filt = tv[0:1] * m2 + tv[1:2] * m1 + tv[2:3] * mixed
        AS[0, :, rows(t), :] = (p[:, 128:256] * filt).astype(BF16).reshape(NTP, STEP, 128)
        send_branch(0, t * STEP, STEP)

    def attend(seqs, lo, n):
        kvs_, sc = [], []
        for s in seqs:
            i = (s * 2 + lo // BLOCK) * 2
            kv = jnp.concatenate([KR[PS[i, 0, 0]], KR[PS[i + 1, 0, 0]]], axis=0)
            kvs_.append(kv)
            sc.append(
                lax.dot_general(
                    Q[s, lo : lo + n, :], kv[:, :128], (((1,), (1,)), ((), ())), preferred_element_type=F32
                ) * (HEAD_SIZE ** -0.5)
            )
        e = [jnp.exp(v - jnp.max(v, axis=1, keepdims=True)) for v in sc]
        wt = [(v / jnp.sum(v, axis=1, keepdims=True)).astype(BF16) for v in e]
        for s, kv, v in zip(seqs, kvs_, wt):
            o = jnp.dot(v, kv[:, 128:], preferred_element_type=F32)
            AS[1, s, lo : lo + n, :] = o.astype(BF16)

    def attend4(i, _):
        attend([i * 4 + j for j in range(4)], 0, BLOCK)
        return 0

    def step(t, _):
        @pl.when(t < 8)
        def _():
            r = rows(t)
            g = G.at[gblk(-1), :, r, :]
            arrived(g, agr.at[t, 0])
            h = G.at[gblk(-1), pl.ds(0, 4), r, :]
            rcopy(h, h, gsend, agr.at[t, 2], dev_y(1)).start()
            rcopy(g, g, gsend, sib.at[t], sibling).start()
            g2 = G.at[gblk(1), :, r, :]
            arrived(g2, agr.at[t, 1])
            h2 = G.at[gblk(1), pl.ds(4, 4), r, :]
            rcopy(h2, h2, gsend, agr.at[t, 2], dev_y(-1)).start()
            rcopy(g2, g2, gsend, sib.at[t], sibling).start()

        @pl.when(t < 6)
        def _():
            direct(t + 2)

        @pl.when(t == 3)
        def _():
            plane2()

        @pl.when((t >= 1) & (t < 9))
        def _():
            u = t - 1
            g = G.at[gblk(2), :, rows(u), :]
            arrived(g, agr.at[u, 2])
            rcopy(g, g, gsend, sib.at[u], sibling).start()

        @pl.when(t == 8)
        def _():
            attend(range(NTP), BLOCK, 64)
            send_branch(1, BLOCK, 64)

        @pl.when(t >= 2)
        def _():
            project(t - 2)

        @pl.when(t == 7)
        def _():
            arrived(KR, kvr)
            pcopy.wait()
            lax.fori_loop(0, 2, attend4, 0)
            send_branch(1, 0, BLOCK)
            plane3()

        return 0

    lax.fori_loop(0, 10, step, 0)
    attend(range(NTP), BLOCK + 64, 64)
    send_branch(1, BLOCK + 64, 64)
    plane4()
    rws = jnp.concatenate([G[j, tp] for j in range(NTP)], axis=1)
    logits = lax.dot_general(rws, route[...], (((1,), (1,)), ((), ())), preferred_element_type=F32)
    mix = jax.nn.sigmoid(logits)
    mix0 = mix[:, 0:1]
    mix1 = mix[:, 1:2]

    arrived(A.at[0], arecv.at[0])
    arrived(W.at[:, 1 - k, y], wsown)
    for d in range(4):
        arrived(TWELVE, wsib.at[d])

    order = [(kk, yy) for kk in range(2) for yy in range(4)]

    def branch(c, m):
        lhs = jnp.concatenate([A[m, yy * 2 + kk] for kk, yy in order], axis=1)
        rhs = jnp.concatenate(
            [
                jnp.concatenate([W[c * 2 + h, kk, yy, m] for kk, yy in order], axis=0)
                for h in range(2)
            ],
            axis=1,
        )
        return jnp.dot(lhs, rhs, preferred_element_type=F32)

    def outc(c, _):
        AC[c] = mix0 * branch(c, 0)
        return 0

    def outp(c, _):
        OB[c] = (AC[c] + mix1 * branch(c, 1)).astype(BF16)
        put(c).start()
        return 0

    def put(c):
        return pltpu.make_async_copy(
            OB.at[c], out.at[:, pl.ds(pl.multiple_of(c * 256, 256), 256)], osem
        )

    lax.fori_loop(0, 8, outc, 0)
    arrived(A.at[1], arecv.at[1])
    lax.fori_loop(0, 8, outp, 0)

    arrived(OB, osem)
    arrived(OV.at[pl.ds(0, NST - 1)], ixs)
    arrived(KS.at[pl.ds(0, NST - 1)], kvs)
    arrived(G.at[pl.ds(0, 7)], gsend)
    arrived(AS.at[:, pl.ds(0, 7)], asend)
    arrived(W.at[pl.ds(0, 14)], wsend)


def local(
    tokens, store, holder, slot, wq, wk, wval, wo, wi, wv, taps, route, cout, mout
):
    hbm = pl.BlockSpec(memory_space=pltpu.HBM)
    dma = pltpu.SemaphoreType.DMA
    V = pltpu.VMEM
    return pl.pallas_call(
        kernel,
        out_shape=jax.ShapeDtypeStruct((SEQ, cout.shape[1]), BF16),
        in_specs=[hbm] * 14,
        out_specs=pl.BlockSpec(memory_space=pl.ANY),
        scratch_shapes=[
            V((8, SEQ, 256), F32),
            V((SEQ, 128), F32),
            V((8, SEQ, 256), BF16),
            pltpu.SMEM((2, 16), jnp.int32),
            pltpu.SMEM((2, 16), jnp.int32),
            V((3, 128), BF16),
            V((2, 2048), BF16),
            V((8, NTP, SEQ, 256), BF16),
            V((2048, 2048), BF16),
            V((2048, 512), BF16),
            V((2048, 256), BF16),
            V((32, PLEN, 256), BF16),
            V((NST, CAP, PLEN, 256), BF16),
            V((NST * CAP, PLEN, 256), BF16),
            V((NST, 1, 128), jnp.int32),
            V((NST, 1, 128), jnp.int32),
            pltpu.SMEM((NST, 1, 128), jnp.int32),
            V((32, 1, 128), jnp.int32),
            pltpu.SMEM((32, 1, 128), jnp.int32),
            V((NTP, SEQ, 128), BF16),
            V((2, 8, SEQ, 128), BF16),
            V((2, 8, SEQ, 128), BF16),
            V((NST, 2, 4, 2, 128, 128), BF16),
            dma((8,)), dma((8,)), dma, dma, dma, dma,
            dma((8, 3)), dma((8,)), dma, dma((2,)), dma,
            dma, dma, dma, dma((3,)), dma((4,)), dma, dma, dma,
        ],
        compiler_params=pltpu.CompilerParams(
            collective_id=0, has_side_effects=True, vmem_limit_bytes=44 * 1024 * 1024
        ),
    )(
        *(
            pltpu.with_memory_space_constraint(v, pltpu.HBM)
            for v in (
                tokens.reshape(NTP, SEQ, tokens.shape[1]), store.reshape(-1, store.shape[-1]), holder.T, slot.T,
                wq, wo, wi, wv, wk, wval, taps, route.T, cout, mout,
            )
        )
    )


def solution(mesh):
    return jax.shard_map(
        local,
        mesh=mesh,
        in_specs=(
            P("st", "tp"), P("st", None, None), P("st", None), P("st", None),
            P(None, "tp"), P(None, "tp"), P(None, "tp"), P(None, "tp"), P(None, "tp"),
            P(None, "tp"), P(None, "tp"), P(), P("tp", None), P("tp", None),
        ),
        out_specs=P(("st", "tp"), None),
        check_vma=False,
    )
```

```python
import jax
import jax.numpy as jnp
from jax import lax
from jax.experimental import pallas as pl
from jax.experimental.pallas import tpu as pltpu
from jax.sharding import PartitionSpec as P

HEAD_SIZE = 128
SEQ = 256
BLOCK = 128
PLEN = 64
CAP = 4
NY = 4
NXZ = 4
NST = 16
NTP = 8
STEP = 32
WIDE = 512
RELAYED = 8
MESH = pl.DeviceIdType.MESH
F32 = jnp.float32
BF16 = jnp.bfloat16


def kernel(
    tokens, store, holder_h, slot_h, wq, wo, wi, wv, wk, wval, taps_h, route_h, cout, mout,
    out,
    PM, OB, holder, slot, taps, route, G, ST, WIN, WKV, TB, KS, KR, OV, WV, WS, PV, PS, Q, AS, A, W,
    lsem, stsem, ixr, ixs, kvr, kvs, agr, sib, gsend, arecv, asend,
    wloc, w1, p1, p2, wsib, wsown, wsend, osem,
):
    st = lax.axis_index("st")
    tp = lax.axis_index("tp")
    y = lax.div(tp, 2)
    k = lax.rem(tp, 2)
    z = lax.div(st, NXZ)
    x = lax.rem(st, NXZ)
    a = (1 - k) * x + k * z
    b = (1 - k) * z + k * x

    def stidx(aa, bb):
        return (1 - k) * (bb * NXZ + aa) + k * (aa * NXZ + bb)

    def ring(v, d):
        return lax.rem(v + d + 4, 4)

    def dev_y(d):
        return (st, ring(y, d) * 2 + k)

    sibling = (st, y * 2 + (1 - k))

    def rcopy(src, dst, ssem, rsem, dev):
        return pltpu.make_async_remote_copy(
            src_ref=src, dst_ref=dst, send_sem=ssem, recv_sem=rsem,
            device_id=dev, device_id_type=MESH,
        )

    def arrived(ref, sem):
        pltpu.make_async_copy(ref, ref, sem).wait()

    def rows(t):
        return pl.ds(pl.multiple_of(t * STEP, STEP), STEP)

    bar = pltpu.get_barrier_semaphore()

    def sig_tp(d, _):
        pl.semaphore_signal(bar, inc=1, device_id=(st, lax.rem(tp + d, NTP)), device_id_type=MESH)
        return 0

    def sig_st(d, _):
        pl.semaphore_signal(bar, inc=1, device_id=(lax.rem(st + d, NST), tp), device_id_type=MESH)
        return 0

    lax.fori_loop(1, NTP, sig_tp, 0)
    lax.fori_loop(1, NST, sig_st, 0)

    loads = []
    for j, w in enumerate((wq, wo, wi, wv)):
        loads.append(pltpu.make_async_copy(w, WIN.at[:, pl.ds(j * 128, 128)], lsem.at[0]))
    for j, w in enumerate((wk, wval)):
        loads.append(pltpu.make_async_copy(w, WKV.at[:, pl.ds(j * 128, 128)], lsem.at[1]))
    own = pltpu.make_async_copy(tokens, G.at[tp], lsem.at[2])
    small = [
        pltpu.make_async_copy(p, q, lsem.at[3 + j])
        for j, (p, q) in enumerate(((holder_h, holder), (slot_h, slot), (taps_h, taps), (route_h, route)))
    ]
    for c in small + loads[4:]:
        c.start()

    def store_copy(i):
        r = pl.ds(pl.multiple_of(i * SEQ, SEQ), SEQ)
        return pltpu.make_async_copy(store.at[r, :], ST.at[r, :], stsem.at[i])

    def start_store(i, _):
        store_copy(i).start()
        return 0

    lax.fori_loop(0, 8, start_store, 0)
    for c in loads[:4]:
        c.start()
    own.start()

    def wcol(m, cs):
        return (cout, mout)[m].at[:, pl.ds(pl.multiple_of(cs * 128, 128), 128)]

    def start_wl(cs, _):
        for m in range(2):
            pltpu.make_async_copy(wcol(m, cs), W.at[cs, k, y, m], wloc).start()
        return 0

    lax.fori_loop(0, NST, start_wl, 0)
    for c in small[:2]:
        c.wait()

    rowi = lax.broadcasted_iota(jnp.int32, (NST, 128), 0)
    lanei = lax.broadcasted_iota(jnp.int32, (NST, 128), 1)
    count = jnp.zeros((NST, 128), jnp.int32)
    wanted = jnp.zeros((NST, 128), jnp.int32)
    for r in range(32):
        o = holder[r % 2, r // 2]
        v = slot[r % 2, r // 2]
        hit = rowi == o
        PV[r] = jnp.sum(jnp.where(hit, count, 0), axis=0, keepdims=True) + o * CAP
        wanted = jnp.where(hit & (lanei == count), v, wanted)
        count = count + hit.astype(jnp.int32)
    for o in range(NST):
        OV[o] = wanted[o : o + 1]
    pcopy = pltpu.make_async_copy(PV, PS, lsem.at[7])
    pcopy.start()

    pl.semaphore_wait(bar, NTP - 1 + NST - 1)

    def ix_copy(d):
        r = lax.rem(st + d, NST)
        return rcopy(OV.at[r], WV.at[st], ixs, ixr, (r, tp))

    def ix_start(d, _):
        ix_copy(d).start()
        return 0

    lax.fori_loop(1, NST, ix_start, 0)
    pltpu.make_async_copy(OV.at[st], WV.at[st], ixr).start()

    def direct(t):
        src = tokens.at[:, rows(t), :]
        dst = G.at[tp, :, rows(t), :]
        rcopy(src, dst, gsend, agr.at[t, 0], dev_y(1)).start()
        rcopy(src, dst, gsend, agr.at[t, 1], dev_y(-1)).start()
        rcopy(src, dst, gsend, sib.at[t], sibling).start()

        @pl.when(t >= RELAYED)
        def _():
            rcopy(src, dst, gsend, agr.at[t, 2], dev_y(2)).start()

    def gblk(d):
        return ring(y, d) * 2 + k


    def w1_start(dy, _):
        for m in range(2):
            rcopy(
                wcol(m, st), W.at[st, k, y, m], wsend, w1,
                (st, lax.rem(y + dy, 4) * 2 + k),
            ).start()
        return 0

    lax.fori_loop(1, 4, w1_start, 0)
    direct(0)
    direct(1)

    arrived(WKV, lsem.at[1])

    def kv_body(i, _):
        store_copy(i).wait()
        r = pl.ds(pl.multiple_of(i * SEQ, SEQ), SEQ)
        kv = jnp.dot(ST[r, :], WKV[...], preferred_element_type=F32).astype(BF16)
        for j in range(4):
            TB[i * 4 + j] = kv[j * PLEN : (j + 1) * PLEN]
        return 0

    lax.fori_loop(0, 6, kv_body, 0)

    def send_kv():
        arrived(WV, ixr)
        c = pltpu.make_async_copy(WV, WS, lsem.at[3])
        c.start()
        c.wait()
        lax.fori_loop(1, NST, kv_out, 0)
        for j in range(CAP):
            KS[st, j] = TB[WS[st, 0, j]]
        pltpu.make_async_copy(KS.at[st], KR.at[pl.ds(st * CAP, CAP)], kvr).start()

    def kv_out(d, _):
        r = lax.rem(st + d, NST)
        for j in range(CAP):
            KS[r, j] = TB[WS[r, 0, j]]
        rcopy(KS.at[r], KR.at[pl.ds(st * CAP, CAP)], kvs, kvr, (r, tp)).start()
        return 0

    def dev_a(d):
        return (stidx(ring(a, d), b), tp)

    def dev_b(d):
        return (stidx(a, ring(b, d)), tp)

    def yo(dy):
        return lax.rem(y + dy, 4)

    def plane1():
        arrived(W.at[pl.ds(0, 3), 0, 0], w1)

        def go2(j, _):
            da = lax.div(j, 3) + 1
            dy = lax.rem(j, 3) + 1
            blk = W.at[st, k, yo(dy)]
            rcopy(blk, blk, wsend, p1, (stidx(lax.rem(a + da, 4), b), tp)).start()
            return 0

        lax.fori_loop(0, 9, go2, 0)

    def wblk(j, d):
        return W.at[stidx(lax.div(j, 3), ring(b, d)), k, yo(lax.rem(j, 3) + 1)]

    def wpass(lo, hi, d, sem, dev):
        def go(j, _):
            g = wblk(j, d)
            rcopy(g, g, wsend, sem, dev).start()
            return 0

        lax.fori_loop(lo, hi, go, 0)

    SIX = W.at[pl.ds(0, 6), 0, 0]
    TWELVE = W.at[pl.ds(0, 3), 0]

    def plane2():
        arrived(W.at[pl.ds(0, 9), 0, 0], p1)
        wpass(0, 6, 0, p2.at[0], dev_b(1))
        wpass(6, 12, 0, p2.at[1], dev_b(-1))
        wpass(0, 12, 0, wsib.at[0], sibling)

    def plane3():
        arrived(SIX, p2.at[0])
        arrived(SIX, p2.at[1])
        wpass(0, 6, -1, p2.at[2], dev_b(1))
        wpass(6, 12, 1, p2.at[2], dev_b(-1))
        wpass(0, 6, -1, wsib.at[1], sibling)
        wpass(6, 12, 1, wsib.at[1], sibling)

    def plane4():
        arrived(TWELVE, p2.at[3])
        wpass(6, 12, -1, wsib.at[2], sibling)
        wpass(0, 6, 1, wsib.at[2], sibling)
        arrived(TWELVE, p2.at[2])
        wpass(0, 12, 2, wsib.at[3], sibling)

    plane1()
    lax.fori_loop(6, 8, kv_body, 0)
    send_kv()

    def send_branch(m, lo, n):
        r = pl.ds(pl.multiple_of(lo, STEP), n)

        def go(d, _):
            s = lax.rem(tp + d, NTP)
            rcopy(AS.at[m, s, r, :], A.at[m, tp, r, :], asend, arecv, (st, s)).start()
            return 0

        lax.fori_loop(1, NTP, go, 0)
        pltpu.make_async_copy(AS.at[m, tp, r, :], A.at[m, tp, r, :], arecv).start()

    arrived(WIN, lsem.at[0])
    for c in small[2:]:
        c.wait()
    own.wait()
    arrived(W.at[:, k, y], wloc)
    rcopy(W.at[:, k, y], W.at[:, k, y], wsend, wsown, sibling).start()
    PM[...] = jnp.zeros_like(PM)
    place = lax.rem(lax.broadcasted_iota(jnp.int32, (SEQ, 128), 0), STEP)

    def project(t):
        arrived(G.at[pl.ds(0, 4), :, rows(t), :], sib.at[t])
        rws = jnp.concatenate([G[j, :, rows(t), :].reshape(SEQ, 256) for j in range(NTP)], axis=1)
        p = jnp.dot(rws, WIN[...], preferred_element_type=F32)
        Q[:, rows(t), :] = p[:, 0:128].astype(BF16).reshape(NTP, STEP, 128)
        mixed = p[:, 256:384] * p[:, 384:512]
        prev = PM[...]
        PM[...] = mixed
        tv = taps[...].astype(F32)
        m1 = jnp.where(place >= 1, pltpu.roll(mixed, 1, 0), pltpu.roll(prev, SEQ + 1 - STEP, 0))
        m2 = jnp.where(place >= 2, pltpu.roll(mixed, 2, 0), pltpu.roll(prev, SEQ + 2 - STEP, 0))
        filt = tv[0:1] * m2 + tv[1:2] * m1 + tv[2:3] * mixed
        AS[0, :, rows(t), :] = (p[:, 128:256] * filt).astype(BF16).reshape(NTP, STEP, 128)
        send_branch(0, t * STEP, STEP)

    def attend(seqs, lo, n):
        kvs_, sc = [], []
        for s in seqs:
            i = (s * 2 + lo // BLOCK) * 2
            kv = jnp.concatenate([KR[PS[i, 0, 0]], KR[PS[i + 1, 0, 0]]], axis=0)
            kvs_.append(kv)
            sc.append(
                lax.dot_general(
                    Q[s, lo : lo + n, :], kv[:, :128], (((1,), (1,)), ((), ())), preferred_element_type=F32
                ) * (HEAD_SIZE ** -0.5)
            )
        e = [jnp.exp(v - jnp.max(v, axis=1, keepdims=True)) for v in sc]
        wt = [(v / jnp.sum(v, axis=1, keepdims=True)).astype(BF16) for v in e]
        for s, kv, v in zip(seqs, kvs_, wt):
            o = jnp.dot(v, kv[:, 128:], preferred_element_type=F32)
            AS[1, s, lo : lo + n, :] = o.astype(BF16)

    def send_memory(i):
        r = pl.ds(0, BLOCK)
        for j in range(4):
            s = i * 4 + j

            @pl.when(s != tp)
            def _():
                rcopy(AS.at[1, s, r, :], A.at[1, tp, r, :], asend, arecv, (st, s)).start()

            @pl.when(s == tp)
            def _():
                pltpu.make_async_copy(AS.at[1, s, r, :], A.at[1, tp, r, :], arecv).start()

    def step(t, _):
        @pl.when(t < 8)
        def _():
            r = rows(t)
            g = G.at[gblk(-1), :, r, :]
            arrived(g, agr.at[t, 0])
            h = G.at[gblk(-1), pl.ds(0, 4), r, :]

            @pl.when(t < RELAYED)
            def _():
                rcopy(h, h, gsend, agr.at[t, 2], dev_y(1)).start()

            rcopy(g, g, gsend, sib.at[t], sibling).start()
            g2 = G.at[gblk(1), :, r, :]
            arrived(g2, agr.at[t, 1])
            h2 = G.at[gblk(1), pl.ds(4, 4), r, :]

            @pl.when(t < RELAYED)
            def _():
                rcopy(h2, h2, gsend, agr.at[t, 2], dev_y(-1)).start()

            rcopy(g2, g2, gsend, sib.at[t], sibling).start()

        @pl.when(t < 6)
        def _():
            direct(t + 2)

        @pl.when(t == 3)
        def _():
            plane2()

        @pl.when(t == 5)
        def _():
            wpass(6, 12, 0, p2.at[3], dev_b(1))
            wpass(0, 6, 0, p2.at[3], dev_b(-1))

        @pl.when(t == 6)
        def _():
            plane3()

        def opposite(u):
            g = G.at[gblk(2), :, rows(u), :]
            arrived(g, agr.at[u, 2])
            rcopy(g, g, gsend, sib.at[u], sibling).start()

        @pl.when((t >= 1) & (t < 9))
        def _():
            opposite(t - 1)

        @pl.when(t == 8)
        def _():
            attend(range(NTP), BLOCK, 64)
            send_branch(1, BLOCK, 64)

        @pl.when(t >= 2)
        def _():
            project(t - 2)

        @pl.when(t == 6)
        def _():
            arrived(KR, kvr)
            pcopy.wait()

        @pl.when((t == 6) | (t == 7))
        def _():
            attend([(t - 6) * 4 + j for j in range(4)], 0, BLOCK)
            send_memory(t - 6)

        return 0

    lax.fori_loop(0, 10, step, 0)
    attend(range(NTP), BLOCK + 64, 64)
    send_branch(1, BLOCK + 64, 64)
    plane4()
    rws = jnp.concatenate([G[j, tp] for j in range(NTP)], axis=1)
    logits = lax.dot_general(rws, route[...], (((1,), (1,)), ((), ())), preferred_element_type=F32)
    mix = jax.nn.sigmoid(logits)

    arrived(W.at[:, 1 - k, y], wsown)
    for d in range(4):
        arrived(TWELVE, wsib.at[d])

    order = [(kk, yy) for kk in range(2) for yy in range(4)]

    def put(c):
        return pltpu.make_async_copy(
            OB.at[c], out.at[:, pl.ds(pl.multiple_of(c * WIDE, WIDE), WIDE)], osem
        )

    def outp(c, _):
        acc = []
        for m in range(2):
            lhs = jnp.concatenate([A[m, yy * 2 + kk] for kk, yy in order], axis=1)
            rhs = jnp.concatenate(
                [
                    jnp.concatenate([W[c * (WIDE // 128) + i, kk, yy, m] for kk, yy in order], axis=0)
                    for i in range(WIDE // 128)
                ],
                axis=1,
            )
            acc.append(jnp.dot(lhs, rhs, preferred_element_type=F32))
        OB[c] = (mix[:, 0:1] * acc[0] + mix[:, 1:2] * acc[1]).astype(BF16)
        put(c).start()
        return 0

    arrived(A, arecv)
    lax.fori_loop(0, 2048 // WIDE, outp, 0)

    arrived(OB, osem)
    arrived(OV.at[pl.ds(0, NST - 1)], ixs)
    arrived(KS.at[pl.ds(0, NST - 1)], kvs)
    arrived(G.at[pl.ds(0, 7)], gsend)
    arrived(AS.at[:, pl.ds(0, 7)], asend)
    arrived(W.at[pl.ds(0, 14)], wsend)


def local(
    tokens, store, holder, slot, wq, wk, wval, wo, wi, wv, taps, route, cout, mout
):
    hbm = pl.BlockSpec(memory_space=pltpu.HBM)
    dma = pltpu.SemaphoreType.DMA
    V = pltpu.VMEM
    return pl.pallas_call(
        kernel,
        out_shape=jax.ShapeDtypeStruct((SEQ, cout.shape[1]), BF16),
        in_specs=[hbm] * 14,
        out_specs=pl.BlockSpec(memory_space=pl.ANY),
        scratch_shapes=[
            V((SEQ, 128), F32),
            V((2048 // WIDE, SEQ, WIDE), BF16),
            pltpu.SMEM((2, 16), jnp.int32),
            pltpu.SMEM((2, 16), jnp.int32),
            V((3, 128), BF16),
            V((2, 2048), BF16),
            V((8, NTP, SEQ, 256), BF16),
            V((2048, 2048), BF16),
            V((2048, 512), BF16),
            V((2048, 256), BF16),
            V((32, PLEN, 256), BF16),
            V((NST, CAP, PLEN, 256), BF16),
            V((NST * CAP, PLEN, 256), BF16),
            V((NST, 1, 128), jnp.int32),
            V((NST, 1, 128), jnp.int32),
            pltpu.SMEM((NST, 1, 128), jnp.int32),
            V((32, 1, 128), jnp.int32),
            pltpu.SMEM((32, 1, 128), jnp.int32),
            V((NTP, SEQ, 128), BF16),
            V((2, 8, SEQ, 128), BF16),
            V((2, 8, SEQ, 128), BF16),
            V((NST, 2, 4, 2, 128, 128), BF16),
            dma((8,)), dma((8,)), dma, dma, dma, dma,
            dma((8, 3)), dma((8,)), dma, dma, dma,
            dma, dma, dma, dma((4,)), dma((4,)), dma, dma, dma,
        ],
        compiler_params=pltpu.CompilerParams(
            collective_id=0, has_side_effects=True, vmem_limit_bytes=44 * 1024 * 1024
        ),
    )(
        *(
            pltpu.with_memory_space_constraint(v, pltpu.HBM)
            for v in (
                tokens.reshape(NTP, SEQ, tokens.shape[1]), store.reshape(-1, store.shape[-1]), holder.T, slot.T,
                wq, wo, wi, wv, wk, wval, taps, route.T, cout, mout,
            )
        )
    )


def solution(mesh):
    return jax.shard_map(
        local,
        mesh=mesh,
        in_specs=(
            P("st", "tp"), P("st", None, None), P("st", None), P("st", None),
            P(None, "tp"), P(None, "tp"), P(None, "tp"), P(None, "tp"), P(None, "tp"),
            P(None, "tp"), P(None, "tp"), P(), P("tp", None), P("tp", None),
        ),
        out_specs=P(("st", "tp"), None),
        check_vma=False,
    )
```

```python
import jax
import jax.numpy as jnp
from jax import lax
from jax.experimental import pallas as pl
from jax.experimental.pallas import tpu as pltpu
from jax.sharding import PartitionSpec as P

HEAD_SIZE = 128
SEQ = 256
BLOCK = 128
PLEN = 64
CAP = 4
NY = 4
NXZ = 4
NST = 16
NTP = 8
STEP = 32
WIDE = 1024
MESH = pl.DeviceIdType.MESH
F32 = jnp.float32
BF16 = jnp.bfloat16


def kernel(
    tokens, store, holder_h, slot_h, wq, wo, wi, wv, wk, wval, taps_h, route_h, cout, mout,
    out,
    PM, OB, holder, slot, taps, route, G, ST, WIN, WKV, TB, KS, KR, OV, WV, WS, PV, PS, Q, AS, A, W,
    lsem, stsem, ixr, ixs, kvr, kvs, agr, sib, gsend, arecv, asend,
    wloc, w1, p1, p2, wsib, wsown, wsend, osem,
):
    st = lax.axis_index("st")
    tp = lax.axis_index("tp")
    y = lax.div(tp, 2)
    k = lax.rem(tp, 2)
    z = lax.div(st, NXZ)
    x = lax.rem(st, NXZ)
    a = (1 - k) * x + k * z
    b = (1 - k) * z + k * x

    def stidx(aa, bb):
        return (1 - k) * (bb * NXZ + aa) + k * (aa * NXZ + bb)

    def ring(v, d):
        return lax.rem(v + d + 4, 4)

    def dev_y(d):
        return (st, ring(y, d) * 2 + k)

    sibling = (st, y * 2 + (1 - k))

    def rcopy(src, dst, ssem, rsem, dev):
        return pltpu.make_async_remote_copy(
            src_ref=src, dst_ref=dst, send_sem=ssem, recv_sem=rsem,
            device_id=dev, device_id_type=MESH,
        )

    def arrived(ref, sem):
        pltpu.make_async_copy(ref, ref, sem).wait()

    def rows(t):
        return pl.ds(pl.multiple_of(t * STEP, STEP), STEP)

    bar = pltpu.get_barrier_semaphore()

    def sig_tp(d, _):
        pl.semaphore_signal(bar, inc=1, device_id=(st, lax.rem(tp + d, NTP)), device_id_type=MESH)
        return 0

    def sig_st(d, _):
        pl.semaphore_signal(bar, inc=1, device_id=(lax.rem(st + d, NST), tp), device_id_type=MESH)
        return 0

    lax.fori_loop(1, NTP, sig_tp, 0)
    lax.fori_loop(1, NST, sig_st, 0)

    loads = []
    for j, w in enumerate((wq, wo, wi, wv)):
        loads.append(pltpu.make_async_copy(w, WIN.at[:, pl.ds(j * 128, 128)], lsem.at[0]))
    for j, w in enumerate((wk, wval)):
        loads.append(pltpu.make_async_copy(w, WKV.at[:, pl.ds(j * 128, 128)], lsem.at[1]))
    own = pltpu.make_async_copy(tokens, G.at[tp], lsem.at[2])
    small = [
        pltpu.make_async_copy(p, q, lsem.at[3 + j])
        for j, (p, q) in enumerate(((holder_h, holder), (slot_h, slot), (taps_h, taps), (route_h, route)))
    ]
    for c in small + loads[4:]:
        c.start()

    def store_copy(i):
        r = pl.ds(pl.multiple_of(i * SEQ, SEQ), SEQ)
        return pltpu.make_async_copy(store.at[r, :], ST.at[r, :], stsem)

    def start_store(i, _):
        store_copy(i).start()
        return 0

    lax.fori_loop(0, 8, start_store, 0)
    for c in loads[:4]:
        c.start()
    own.start()

    def wcol(m, cs):
        return (cout, mout)[m].at[:, pl.ds(pl.multiple_of(cs * 128, 128), 128)]

    def start_wl(cs, _):
        for m in range(2):
            pltpu.make_async_copy(wcol(m, cs), W.at[cs, k, y, m], wloc).start()
        return 0

    lax.fori_loop(0, NST, start_wl, 0)
    for c in small[:2]:
        c.wait()

    rowi = lax.broadcasted_iota(jnp.int32, (NST, 128), 0)
    lanei = lax.broadcasted_iota(jnp.int32, (NST, 128), 1)
    count = jnp.zeros((NST, 128), jnp.int32)
    wanted = jnp.zeros((NST, 128), jnp.int32)
    for r in range(32):
        o = holder[r % 2, r // 2]
        v = slot[r % 2, r // 2]
        hit = rowi == o
        PV[r] = jnp.sum(jnp.where(hit, count, 0), axis=0, keepdims=True) + o * CAP
        wanted = jnp.where(hit & (lanei == count), v, wanted)
        count = count + hit.astype(jnp.int32)
    for o in range(NST):
        OV[o] = wanted[o : o + 1]
    pcopy = pltpu.make_async_copy(PV, PS, lsem.at[7])
    pcopy.start()

    pl.semaphore_wait(bar, NTP - 1 + NST - 1)

    def ix_copy(d):
        r = lax.rem(st + d, NST)
        return rcopy(OV.at[r], WV.at[st], ixs, ixr, (r, tp))

    def ix_start(d, _):
        ix_copy(d).start()
        return 0

    lax.fori_loop(1, NST, ix_start, 0)
    pltpu.make_async_copy(OV.at[st], WV.at[st], ixr).start()

    def direct(t):
        src = tokens.at[:, rows(t), :]
        dst = G.at[tp, :, rows(t), :]
        rcopy(src, dst, gsend, agr.at[t, 0], dev_y(1)).start()
        rcopy(src, dst, gsend, agr.at[t, 1], dev_y(-1)).start()
        rcopy(src, dst, gsend, sib.at[t], sibling).start()

    def gblk(d):
        return ring(y, d) * 2 + k


    def w1_start(dy, _):
        for m in range(2):
            rcopy(
                wcol(m, st), W.at[st, k, y, m], wsend, w1,
                (st, lax.rem(y + dy, 4) * 2 + k),
            ).start()
        return 0

    lax.fori_loop(1, 4, w1_start, 0)
    direct(0)
    direct(1)

    arrived(WKV, lsem.at[1])
    arrived(ST, stsem)

    def kv_body(i, _):
        r = pl.ds(pl.multiple_of(i * SEQ, SEQ), SEQ)
        kv = jnp.dot(ST[r, :], WKV[...], preferred_element_type=F32).astype(BF16)
        for j in range(4):
            TB[i * 4 + j] = kv[j * PLEN : (j + 1) * PLEN]
        return 0

    lax.fori_loop(0, 6, kv_body, 0)

    def send_kv():
        arrived(WV, ixr)
        c = pltpu.make_async_copy(WV, WS, lsem.at[3])
        c.start()
        c.wait()
        lax.fori_loop(1, NST, kv_out, 0)
        for j in range(CAP):
            KS[st, j] = TB[WS[st, 0, j]]
        pltpu.make_async_copy(KS.at[st], KR.at[pl.ds(st * CAP, CAP)], kvr).start()

    def kv_out(d, _):
        r = lax.rem(st + d, NST)
        for j in range(CAP):
            KS[r, j] = TB[WS[r, 0, j]]
        rcopy(KS.at[r], KR.at[pl.ds(st * CAP, CAP)], kvs, kvr, (r, tp)).start()
        return 0

    def dev_a(d):
        return (stidx(ring(a, d), b), tp)

    def dev_b(d):
        return (stidx(a, ring(b, d)), tp)

    def yo(dy):
        return lax.rem(y + dy, 4)

    def plane1():
        arrived(W.at[pl.ds(0, 3), 0, 0], w1)

        def go2(j, _):
            da = lax.div(j, 3) + 1
            dy = lax.rem(j, 3) + 1
            blk = W.at[st, k, yo(dy)]
            rcopy(blk, blk, wsend, p1, (stidx(lax.rem(a + da, 4), b), tp)).start()
            return 0

        lax.fori_loop(0, 9, go2, 0)

    def wblk(j, d):
        return W.at[stidx(lax.div(j, 3), ring(b, d)), k, yo(lax.rem(j, 3) + 1)]

    def wpass(lo, hi, d, sem, dev):
        def go(j, _):
            g = wblk(j, d)
            rcopy(g, g, wsend, sem, dev).start()
            return 0

        lax.fori_loop(lo, hi, go, 0)

    SIX = W.at[pl.ds(0, 6), 0, 0]
    TWELVE = W.at[pl.ds(0, 3), 0]

    def plane2():
        arrived(W.at[pl.ds(0, 9), 0, 0], p1)
        wpass(0, 6, 0, p2.at[0], dev_b(1))
        wpass(6, 12, 0, p2.at[1], dev_b(-1))
        wpass(0, 12, 0, wsib.at[0], sibling)

    def plane3():
        arrived(SIX, p2.at[0])
        arrived(SIX, p2.at[1])
        wpass(0, 6, -1, p2.at[2], dev_b(1))
        wpass(6, 12, 1, p2.at[2], dev_b(-1))
        wpass(0, 6, -1, wsib.at[1], sibling)
        wpass(6, 12, 1, wsib.at[1], sibling)

    def plane4():
        arrived(TWELVE, p2.at[3])
        wpass(6, 12, -1, wsib.at[2], sibling)
        wpass(0, 6, 1, wsib.at[2], sibling)

    def plane5():
        arrived(TWELVE, p2.at[2])
        wpass(0, 12, 2, wsib.at[3], sibling)

    plane1()
    lax.fori_loop(6, 8, kv_body, 0)
    send_kv()

    def send_branch(m, lo, n):
        r = pl.ds(pl.multiple_of(lo, STEP), n)

        def go(d, _):
            s = lax.rem(tp + d, NTP)
            rcopy(AS.at[m, s, r, :], A.at[m, tp, r, :], asend, arecv, (st, s)).start()
            return 0

        lax.fori_loop(1, NTP, go, 0)
        pltpu.make_async_copy(AS.at[m, tp, r, :], A.at[m, tp, r, :], arecv).start()

    arrived(WIN, lsem.at[0])
    for c in small[2:]:
        c.wait()
    own.wait()
    arrived(W.at[:, k, y], wloc)
    rcopy(W.at[:, k, y], W.at[:, k, y], wsend, wsown, sibling).start()
    PM[...] = jnp.zeros_like(PM)
    place = lax.rem(lax.broadcasted_iota(jnp.int32, (SEQ, 128), 0), STEP)

    def project(t):
        arrived(G.at[pl.ds(0, 4), :, rows(t), :], sib.at[t])
        rws = jnp.concatenate([G[j, :, rows(t), :].reshape(SEQ, 256) for j in range(NTP)], axis=1)
        p = jnp.dot(rws, WIN[...], preferred_element_type=F32)
        Q[:, rows(t), :] = p[:, 0:128].astype(BF16).reshape(NTP, STEP, 128)
        mixed = p[:, 256:384] * p[:, 384:512]
        prev = PM[...]
        PM[...] = mixed
        tv = taps[...].astype(F32)
        m1 = jnp.where(place >= 1, pltpu.roll(mixed, 1, 0), pltpu.roll(prev, SEQ + 1 - STEP, 0))
        m2 = jnp.where(place >= 2, pltpu.roll(mixed, 2, 0), pltpu.roll(prev, SEQ + 2 - STEP, 0))
        filt = tv[0:1] * m2 + tv[1:2] * m1 + tv[2:3] * mixed
        AS[0, :, rows(t), :] = (p[:, 128:256] * filt).astype(BF16).reshape(NTP, STEP, 128)
        send_branch(0, t * STEP, STEP)

    def attend(seqs, lo, n):
        blk = lo // BLOCK if isinstance(lo, int) else 0
        r = pl.ds(lo, n)
        kvs_, sc = [], []
        for s in seqs:
            i = (s * 2 + blk) * 2
            kv = jnp.concatenate([KR[PS[i, 0, 0]], KR[PS[i + 1, 0, 0]]], axis=0)
            kvs_.append(kv)
            sc.append(
                lax.dot_general(
                    Q[s, r, :], kv[:, :128], (((1,), (1,)), ((), ())), preferred_element_type=F32
                ) * (HEAD_SIZE ** -0.5)
            )
        e = [jnp.exp(v - jnp.max(v, axis=1, keepdims=True)) for v in sc]
        wt = [(v / jnp.sum(v, axis=1, keepdims=True)).astype(BF16) for v in e]
        for s, kv, v in zip(seqs, kvs_, wt):
            o = jnp.dot(v, kv[:, 128:], preferred_element_type=F32)
            AS[1, s, r, :] = o.astype(BF16)

    def step(t, _):
        @pl.when(t < 8)
        def _():
            r = rows(t)
            g = G.at[gblk(-1), :, r, :]
            arrived(g, agr.at[t, 0])
            h = G.at[gblk(-1), pl.ds(0, 4), r, :]
            rcopy(h, h, gsend, agr.at[t, 2], dev_y(1)).start()
            rcopy(g, g, gsend, sib.at[t], sibling).start()
            g2 = G.at[gblk(1), :, r, :]
            arrived(g2, agr.at[t, 1])
            h2 = G.at[gblk(1), pl.ds(4, 4), r, :]
            rcopy(h2, h2, gsend, agr.at[t, 2], dev_y(-1)).start()
            rcopy(g2, g2, gsend, sib.at[t], sibling).start()

        @pl.when(t < 6)
        def _():
            direct(t + 2)

        @pl.when(t == 3)
        def _():
            plane2()

        @pl.when(t == 5)
        def _():
            wpass(6, 12, 0, p2.at[3], dev_b(1))
            wpass(0, 6, 0, p2.at[3], dev_b(-1))

        @pl.when(t == 7)
        def _():
            plane3()

        def opposite(u):
            g = G.at[gblk(2), :, rows(u), :]
            arrived(g, agr.at[u, 2])
            rcopy(g, g, gsend, sib.at[u], sibling).start()

        @pl.when((t >= 1) & (t < 9))
        def _():
            opposite(t - 1)

        @pl.when(t == 8)
        def _():
            attend(range(NTP), BLOCK, 64)
            send_branch(1, BLOCK, 64)

        @pl.when(t >= 2)
        def _():
            project(t - 2)

        @pl.when(t == 6)
        def _():
            arrived(KR, kvr)
            pcopy.wait()

        @pl.when((t == 6) | (t == 7))
        def _():
            attend(range(NTP), pl.multiple_of((t - 6) * 64, 64), 64)
            send_branch(1, (t - 6) * 64, 64)

        @pl.when(t == 8)
        def _():
            plane4()

        return 0

    lax.fori_loop(0, 10, step, 0)
    attend(range(NTP), BLOCK + 64, 64)
    send_branch(1, BLOCK + 64, 64)
    plane5()
    rws = jnp.concatenate([G[j, tp] for j in range(NTP)], axis=1)
    logits = lax.dot_general(rws, route[...], (((1,), (1,)), ((), ())), preferred_element_type=F32)
    mix = jax.nn.sigmoid(logits)

    arrived(W.at[:, 1 - k, y], wsown)
    for d in range(4):
        arrived(TWELVE, wsib.at[d])

    order = [(kk, yy) for kk in range(2) for yy in range(4)]

    def put(c):
        return pltpu.make_async_copy(
            OB.at[c], out.at[:, pl.ds(pl.multiple_of(c * WIDE, WIDE), WIDE)], osem
        )

    def outp(c, _):
        acc = []
        for m in range(2):
            lhs = jnp.concatenate([A[m, yy * 2 + kk] for kk, yy in order], axis=1)
            rhs = jnp.concatenate(
                [
                    jnp.concatenate([W[c * (WIDE // 128) + i, kk, yy, m] for kk, yy in order], axis=0)
                    for i in range(WIDE // 128)
                ],
                axis=1,
            )
            acc.append(jnp.dot(lhs, rhs, preferred_element_type=F32))
        OB[c] = (mix[:, 0:1] * acc[0] + mix[:, 1:2] * acc[1]).astype(BF16)
        put(c).start()
        return 0

    arrived(A, arecv)
    lax.fori_loop(0, 2048 // WIDE, outp, 0)

    arrived(OB, osem)
    arrived(OV.at[pl.ds(0, NST - 1)], ixs)
    arrived(KS.at[pl.ds(0, NST - 1)], kvs)
    arrived(G.at[pl.ds(0, 7)], gsend)
    arrived(AS.at[:, pl.ds(0, 7)], asend)
    arrived(W.at[pl.ds(0, 14)], wsend)


def local(
    tokens, store, holder, slot, wq, wk, wval, wo, wi, wv, taps, route, cout, mout
):
    hbm = pl.BlockSpec(memory_space=pltpu.HBM)
    dma = pltpu.SemaphoreType.DMA
    V = pltpu.VMEM
    return pl.pallas_call(
        kernel,
        out_shape=jax.ShapeDtypeStruct((SEQ, cout.shape[1]), BF16),
        in_specs=[hbm] * 14,
        out_specs=pl.BlockSpec(memory_space=pl.ANY),
        scratch_shapes=[
            V((SEQ, 128), F32),
            V((2048 // WIDE, SEQ, WIDE), BF16),
            pltpu.SMEM((2, 16), jnp.int32),
            pltpu.SMEM((2, 16), jnp.int32),
            V((3, 128), BF16),
            V((2, 2048), BF16),
            V((8, NTP, SEQ, 256), BF16),
            V((2048, 2048), BF16),
            V((2048, 512), BF16),
            V((2048, 256), BF16),
            V((32, PLEN, 256), BF16),
            V((NST, CAP, PLEN, 256), BF16),
            V((NST * CAP, PLEN, 256), BF16),
            V((NST, 1, 128), jnp.int32),
            V((NST, 1, 128), jnp.int32),
            pltpu.SMEM((NST, 1, 128), jnp.int32),
            V((32, 1, 128), jnp.int32),
            pltpu.SMEM((32, 1, 128), jnp.int32),
            V((NTP, SEQ, 128), BF16),
            V((2, 8, SEQ, 128), BF16),
            V((2, 8, SEQ, 128), BF16),
            V((NST, 2, 4, 2, 128, 128), BF16),
            dma((8,)), dma, dma, dma, dma, dma,
            dma((8, 3)), dma((8,)), dma, dma, dma,
            dma, dma, dma, dma((4,)), dma((4,)), dma, dma, dma,
        ],
        compiler_params=pltpu.CompilerParams(
            collective_id=0, has_side_effects=True, vmem_limit_bytes=44 * 1024 * 1024
        ),
    )(
        *(
            pltpu.with_memory_space_constraint(v, pltpu.HBM)
            for v in (
                tokens.reshape(NTP, SEQ, tokens.shape[1]), store.reshape(-1, store.shape[-1]), holder.T, slot.T,
                wq, wo, wi, wv, wk, wval, taps, route.T, cout, mout,
            )
        )
    )


def solution(mesh):
    return jax.shard_map(
        local,
        mesh=mesh,
        in_specs=(
            P("st", "tp"), P("st", None, None), P("st", None), P("st", None),
            P(None, "tp"), P(None, "tp"), P(None, "tp"), P(None, "tp"), P(None, "tp"),
            P(None, "tp"), P(None, "tp"), P(), P("tp", None), P("tp", None),
        ),
        out_specs=P(("st", "tp"), None),
        check_vma=False,
    )
```

```python
import jax
import jax.numpy as jnp
from jax import lax
from jax.experimental import pallas as pl
from jax.experimental.pallas import tpu as pltpu
from jax.sharding import PartitionSpec as P

HEAD_SIZE = 128
SEQ = 256
BLOCK = 128
PLEN = 64
CAP = 4
NY = 4
NXZ = 4
NST = 16
NTP = 8
STEP = 32
WIDE = 1024
MESH = pl.DeviceIdType.MESH
F32 = jnp.float32
BF16 = jnp.bfloat16


def kernel(
    tokens, store, holder_h, slot_h, wq, wo, wi, wv, wk, wval, taps_h, route_h, cout, mout,
    out,
    PM, OB, holder, slot, taps, route, G, ST, WIN, WKV, TB, KS, KR, OV, WV, WS, PV, PS, Q, AS, A, W,
    lsem, stsem, ixr, ixs, kvr, kvs, agr, sib, gsend, arecv, asend,
    wloc, w1, p1, p2, wsib, wsown, wsend, osem, row_sem, all_sem,
):
    st = lax.axis_index("st")
    tp = lax.axis_index("tp")
    y = lax.div(tp, 2)
    k = lax.rem(tp, 2)
    z = lax.div(st, NXZ)
    x = lax.rem(st, NXZ)
    a = (1 - k) * x + k * z
    b = (1 - k) * z + k * x

    def stidx(aa, bb):
        return (1 - k) * (bb * NXZ + aa) + k * (aa * NXZ + bb)

    def ring(v, d):
        return lax.rem(v + d + 4, 4)

    def dev_y(d):
        return (st, ring(y, d) * 2 + k)

    sibling = (st, y * 2 + (1 - k))

    def rcopy(src, dst, ssem, rsem, dev):
        return pltpu.make_async_remote_copy(
            src_ref=src, dst_ref=dst, send_sem=ssem, recv_sem=rsem,
            device_id=dev, device_id_type=MESH,
        )

    def arrived(ref, sem):
        pltpu.make_async_copy(ref, ref, sem).wait()

    def rows(t):
        return pl.ds(pl.multiple_of(t * STEP, STEP), STEP)

    bar = pltpu.get_barrier_semaphore()

    def signal(sem, dev):
        pl.semaphore_signal(sem, inc=1, device_id=dev, device_id_type=MESH)

    def sig_row(d, _):
        p = lax.rem(y + d, NY) * 2 + 1

        @pl.when(p != tp)
        def _():
            signal(bar, (st, p))

        return 0

    def sig_st(d, _):
        signal(bar, (lax.rem(st + d, NST), y * 2))
        return 0

    lax.fori_loop(0, NY, sig_row, 0)
    lax.fori_loop(1, NST, sig_st, 0)

    loads = []
    for j, w in enumerate((wq, wo, wi, wv)):
        loads.append(pltpu.make_async_copy(w, WIN.at[:, pl.ds(j * 128, 128)], lsem.at[0]))
    for j, w in enumerate((wk, wval)):
        loads.append(pltpu.make_async_copy(w, WKV.at[:, pl.ds(j * 128, 128)], lsem.at[1]))
    own = pltpu.make_async_copy(tokens, G.at[tp], lsem.at[2])
    small = [
        pltpu.make_async_copy(p, q, lsem.at[3 + j])
        for j, (p, q) in enumerate(((holder_h, holder), (slot_h, slot), (taps_h, taps), (route_h, route)))
    ]
    for c in small + loads[4:]:
        c.start()

    def store_copy(i):
        r = pl.ds(pl.multiple_of(i * SEQ, SEQ), SEQ)
        return pltpu.make_async_copy(store.at[r, :], ST.at[r, :], stsem)

    def start_store(i, _):
        store_copy(i).start()
        return 0

    lax.fori_loop(0, 8, start_store, 0)
    for c in loads[:4]:
        c.start()
    own.start()

    def wcol(m, cs):
        return (cout, mout)[m].at[:, pl.ds(pl.multiple_of(cs * 128, 128), 128)]

    def start_wl(cs, _):
        for m in range(2):
            pltpu.make_async_copy(wcol(m, cs), W.at[cs, k, y, m], wloc).start()
        return 0

    lax.fori_loop(0, NST, start_wl, 0)
    for c in small[:2]:
        c.wait()

    rowi = lax.broadcasted_iota(jnp.int32, (NST, 128), 0)
    lanei = lax.broadcasted_iota(jnp.int32, (NST, 128), 1)
    count = jnp.zeros((NST, 128), jnp.int32)
    wanted = jnp.zeros((NST, 128), jnp.int32)
    for r in range(32):
        o = holder[r % 2, r // 2]
        v = slot[r % 2, r // 2]
        hit = rowi == o
        PV[r] = jnp.sum(jnp.where(hit, count, 0), axis=0, keepdims=True) + o * CAP
        wanted = jnp.where(hit & (lanei == count), v, wanted)
        count = count + hit.astype(jnp.int32)
    for o in range(NST):
        OV[o] = wanted[o : o + 1]
    pcopy = pltpu.make_async_copy(PV, PS, lsem.at[7])
    pcopy.start()

    @pl.when(k == 1)
    def _():
        pl.semaphore_wait(bar, NTP - 1)
        signal(row_sem, sibling)

    @pl.when(k == 0)
    def _():
        pl.semaphore_wait(row_sem, 1)

    def direct(t):
        src = tokens.at[:, rows(t), :]
        dst = G.at[tp, :, rows(t), :]
        rcopy(src, dst, gsend, agr.at[t, 0], dev_y(1)).start()
        rcopy(src, dst, gsend, agr.at[t, 1], dev_y(-1)).start()
        rcopy(src, dst, gsend, sib.at[t], sibling).start()

    def gblk(d):
        return ring(y, d) * 2 + k


    def w1_start(dy, _):
        for m in range(2):
            rcopy(
                wcol(m, st), W.at[st, k, y, m], wsend, w1,
                (st, lax.rem(y + dy, 4) * 2 + k),
            ).start()
        return 0

    lax.fori_loop(1, 4, w1_start, 0)
    direct(0)
    direct(1)

    @pl.when(k == 0)
    def _():
        pl.semaphore_wait(bar, 2 * (NST - 1))
        signal(all_sem, sibling)

    @pl.when(k == 1)
    def _():
        pl.semaphore_wait(all_sem, 1)

    def ix_copy(d):
        r = lax.rem(st + d, NST)
        return rcopy(OV.at[r], WV.at[st], ixs, ixr, (r, tp))

    def ix_start(d, _):
        ix_copy(d).start()
        return 0

    lax.fori_loop(1, NST, ix_start, 0)
    pltpu.make_async_copy(OV.at[st], WV.at[st], ixr).start()

    arrived(WKV, lsem.at[1])
    arrived(ST, stsem)

    def kv_body(i, _):
        r = pl.ds(pl.multiple_of(i * SEQ, SEQ), SEQ)
        kv = jnp.dot(ST[r, :], WKV[...], preferred_element_type=F32).astype(BF16)
        for j in range(4):
            TB[i * 4 + j] = kv[j * PLEN : (j + 1) * PLEN]
        return 0

    lax.fori_loop(0, 3, kv_body, 0)
    direct(2)
    lax.fori_loop(3, 6, kv_body, 0)

    def send_kv():
        arrived(WV, ixr)
        c = pltpu.make_async_copy(WV, WS, lsem.at[3])
        c.start()
        c.wait()
        lax.fori_loop(1, 4, kv_out, 0)
        for j in range(CAP):
            KS[st, j] = TB[WS[st, 0, j]]
        pltpu.make_async_copy(KS.at[st], KR.at[pl.ds(st * CAP, CAP)], kvr).start()

    def kv_out(d, _):
        r = lax.rem(st + d, NST)
        for j in range(CAP):
            KS[r, j] = TB[WS[r, 0, j]]
        rcopy(KS.at[r], KR.at[pl.ds(st * CAP, CAP)], kvs, kvr, (r, tp)).start()
        return 0

    def dev_a(d):
        return (stidx(ring(a, d), b), tp)

    def dev_b(d):
        return (stidx(a, ring(b, d)), tp)

    def yo(dy):
        return lax.rem(y + dy, 4)

    def plane1():
        arrived(W.at[pl.ds(0, 3), 0, 0], w1)

        def go2(j, _):
            da = lax.div(j, 3) + 1
            dy = lax.rem(j, 3) + 1
            blk = W.at[st, k, yo(dy)]
            rcopy(blk, blk, wsend, p1, (stidx(lax.rem(a + da, 4), b), tp)).start()
            return 0

        lax.fori_loop(0, 9, go2, 0)

    def wblk(j, d):
        return W.at[stidx(lax.div(j, 3), ring(b, d)), k, yo(lax.rem(j, 3) + 1)]

    def wpass(lo, hi, d, sem, dev):
        def go(j, _):
            g = wblk(j, d)
            rcopy(g, g, wsend, sem, dev).start()
            return 0

        lax.fori_loop(lo, hi, go, 0)

    SIX = W.at[pl.ds(0, 6), 0, 0]
    TWELVE = W.at[pl.ds(0, 3), 0]

    def plane2():
        arrived(W.at[pl.ds(0, 9), 0, 0], p1)
        wpass(0, 6, 0, p2.at[0], dev_b(1))
        wpass(6, 12, 0, p2.at[1], dev_b(-1))
        wpass(0, 12, 0, wsib.at[0], sibling)

    def plane3():
        arrived(SIX, p2.at[0])
        arrived(SIX, p2.at[1])
        wpass(0, 6, -1, p2.at[2], dev_b(1))
        wpass(6, 12, 1, p2.at[2], dev_b(-1))
        wpass(0, 6, -1, wsib.at[1], sibling)
        wpass(6, 12, 1, wsib.at[1], sibling)

    def plane4():
        arrived(TWELVE, p2.at[3])
        wpass(6, 12, -1, wsib.at[2], sibling)
        wpass(0, 6, 1, wsib.at[2], sibling)

    def plane5():
        arrived(TWELVE, p2.at[2])
        wpass(0, 12, 2, wsib.at[3], sibling)

    plane1()
    lax.fori_loop(6, 8, kv_body, 0)
    send_kv()

    def send_branch(m, lo, n):
        r = pl.ds(pl.multiple_of(lo, STEP), n)

        def go(d, _):
            s = lax.rem(tp + d, NTP)
            rcopy(AS.at[m, s, r, :], A.at[m, tp, r, :], asend, arecv, (st, s)).start()
            return 0

        lax.fori_loop(1, NTP, go, 0)
        pltpu.make_async_copy(AS.at[m, tp, r, :], A.at[m, tp, r, :], arecv).start()

    arrived(WIN, lsem.at[0])
    for c in small[2:]:
        c.wait()
    own.wait()
    arrived(W.at[:, k, y], wloc)
    rcopy(W.at[:, k, y], W.at[:, k, y], wsend, wsown, sibling).start()
    PM[...] = jnp.zeros_like(PM)
    place = lax.rem(lax.broadcasted_iota(jnp.int32, (SEQ, 128), 0), STEP)

    def project(t):
        arrived(G.at[pl.ds(0, 4), :, rows(t), :], sib.at[t])
        rws = jnp.concatenate([G[j, :, rows(t), :].reshape(SEQ, 256) for j in range(NTP)], axis=1)
        p = jnp.dot(rws, WIN[...], preferred_element_type=F32)
        Q[:, rows(t), :] = p[:, 0:128].astype(BF16).reshape(NTP, STEP, 128)
        mixed = p[:, 256:384] * p[:, 384:512]
        prev = PM[...]
        PM[...] = mixed
        tv = taps[...].astype(F32)
        m1 = jnp.where(place >= 1, pltpu.roll(mixed, 1, 0), pltpu.roll(prev, SEQ + 1 - STEP, 0))
        m2 = jnp.where(place >= 2, pltpu.roll(mixed, 2, 0), pltpu.roll(prev, SEQ + 2 - STEP, 0))
        filt = tv[0:1] * m2 + tv[1:2] * m1 + tv[2:3] * mixed
        AS[0, :, rows(t), :] = (p[:, 128:256] * filt).astype(BF16).reshape(NTP, STEP, 128)
        send_branch(0, t * STEP, STEP)

    def attend(seqs, lo, n):
        blk = lo // BLOCK if isinstance(lo, int) else 0
        r = pl.ds(lo, n)
        kvs_, sc = [], []
        for s in seqs:
            i = (s * 2 + blk) * 2
            kv = jnp.concatenate([KR[PS[i, 0, 0]], KR[PS[i + 1, 0, 0]]], axis=0)
            kvs_.append(kv)
            sc.append(
                lax.dot_general(
                    Q[s, r, :], kv[:, :128], (((1,), (1,)), ((), ())), preferred_element_type=F32
                ) * (HEAD_SIZE ** -0.5)
            )
        e = [jnp.exp(v - jnp.max(v, axis=1, keepdims=True)) for v in sc]
        wt = [(v / jnp.sum(v, axis=1, keepdims=True)).astype(BF16) for v in e]
        for s, kv, v in zip(seqs, kvs_, wt):
            o = jnp.dot(v, kv[:, 128:], preferred_element_type=F32)
            AS[1, s, r, :] = o.astype(BF16)

    def step(t, _):
        @pl.when(t < 8)
        def _():
            r = rows(t)
            g = G.at[gblk(-1), :, r, :]
            arrived(g, agr.at[t, 0])
            h = G.at[gblk(-1), pl.ds(0, 4), r, :]
            rcopy(h, h, gsend, agr.at[t, 2], dev_y(1)).start()
            rcopy(g, g, gsend, sib.at[t], sibling).start()
            g2 = G.at[gblk(1), :, r, :]
            arrived(g2, agr.at[t, 1])
            h2 = G.at[gblk(1), pl.ds(4, 4), r, :]
            rcopy(h2, h2, gsend, agr.at[t, 2], dev_y(-1)).start()
            rcopy(g2, g2, gsend, sib.at[t], sibling).start()

        @pl.when((t >= 1) & (t < 6))
        def _():
            direct(t + 2)

        @pl.when(t <= 1)
        def _():
            lax.fori_loop(4 + 6 * t, 10 + 6 * t, kv_out, 0)

        @pl.when(t == 4)
        def _():
            plane2()

        @pl.when(t == 5)
        def _():
            wpass(6, 12, 0, p2.at[3], dev_b(1))
            wpass(0, 6, 0, p2.at[3], dev_b(-1))

        @pl.when(t == 7)
        def _():
            plane3()

        def opposite(u):
            g = G.at[gblk(2), :, rows(u), :]
            arrived(g, agr.at[u, 2])
            rcopy(g, g, gsend, sib.at[u], sibling).start()

        @pl.when((t >= 1) & (t < 9))
        def _():
            opposite(t - 1)

        @pl.when(t == 8)
        def _():
            attend(range(NTP), BLOCK, 64)
            send_branch(1, BLOCK, 64)

        @pl.when(t >= 2)
        def _():
            project(t - 2)

        @pl.when(t == 7)
        def _():
            arrived(KR, kvr)
            pcopy.wait()

            def two(i, _):
                attend(range(NTP), pl.multiple_of(i * 64, 64), 64)
                send_branch(1, i * 64, 64)
                return 0

            lax.fori_loop(0, 2, two, 0)
        @pl.when(t == 8)
        def _():
            plane4()

        return 0

    lax.fori_loop(0, 10, step, 0)
    attend(range(NTP), BLOCK + 64, 64)
    send_branch(1, BLOCK + 64, 64)
    plane5()
    rws = jnp.concatenate([G[j, tp] for j in range(NTP)], axis=1)
    logits = lax.dot_general(rws, route[...], (((1,), (1,)), ((), ())), preferred_element_type=F32)
    mix = jax.nn.sigmoid(logits)

    arrived(W.at[:, 1 - k, y], wsown)
    for d in range(4):
        arrived(TWELVE, wsib.at[d])

    order = [(kk, yy) for kk in range(2) for yy in range(4)]

    def put(c):
        return pltpu.make_async_copy(
            OB.at[c], out.at[:, pl.ds(pl.multiple_of(c * WIDE, WIDE), WIDE)], osem
        )

    def outp(c, _):
        acc = []
        for m in range(2):
            lhs = jnp.concatenate([A[m, yy * 2 + kk] for kk, yy in order], axis=1)
            rhs = jnp.concatenate(
                [
                    jnp.concatenate([W[c * (WIDE // 128) + i, kk, yy, m] for kk, yy in order], axis=0)
                    for i in range(WIDE // 128)
                ],
                axis=1,
            )
            acc.append(jnp.dot(lhs, rhs, preferred_element_type=F32))
        OB[c] = (mix[:, 0:1] * acc[0] + mix[:, 1:2] * acc[1]).astype(BF16)
        put(c).start()
        return 0

    arrived(A, arecv)
    lax.fori_loop(0, 2048 // WIDE, outp, 0)

    arrived(OB, osem)
    arrived(OV.at[pl.ds(0, NST - 1)], ixs)
    arrived(KS.at[pl.ds(0, NST - 1)], kvs)
    arrived(G.at[pl.ds(0, 7)], gsend)
    arrived(AS.at[:, pl.ds(0, 7)], asend)
    arrived(W.at[pl.ds(0, 14)], wsend)


def local(
    tokens, store, holder, slot, wq, wk, wval, wo, wi, wv, taps, route, cout, mout
):
    hbm = pl.BlockSpec(memory_space=pltpu.HBM)
    dma = pltpu.SemaphoreType.DMA
    reg = pltpu.SemaphoreType.REGULAR
    V = pltpu.VMEM
    return pl.pallas_call(
        kernel,
        out_shape=jax.ShapeDtypeStruct((SEQ, cout.shape[1]), BF16),
        in_specs=[hbm] * 14,
        out_specs=pl.BlockSpec(memory_space=pl.ANY),
        scratch_shapes=[
            V((SEQ, 128), F32),
            V((2048 // WIDE, SEQ, WIDE), BF16),
            pltpu.SMEM((2, 16), jnp.int32),
            pltpu.SMEM((2, 16), jnp.int32),
            V((3, 128), BF16),
            V((2, 2048), BF16),
            V((8, NTP, SEQ, 256), BF16),
            V((2048, 2048), BF16),
            V((2048, 512), BF16),
            V((2048, 256), BF16),
            V((32, PLEN, 256), BF16),
            V((NST, CAP, PLEN, 256), BF16),
            V((NST * CAP, PLEN, 256), BF16),
            V((NST, 1, 128), jnp.int32),
            V((NST, 1, 128), jnp.int32),
            pltpu.SMEM((NST, 1, 128), jnp.int32),
            V((32, 1, 128), jnp.int32),
            pltpu.SMEM((32, 1, 128), jnp.int32),
            V((NTP, SEQ, 128), BF16),
            V((2, 8, SEQ, 128), BF16),
            V((2, 8, SEQ, 128), BF16),
            V((NST, 2, 4, 2, 128, 128), BF16),
            dma((8,)), dma, dma, dma, dma, dma,
            dma((8, 3)), dma((8,)), dma, dma, dma,
            dma, dma, dma, dma((4,)), dma((4,)), dma, dma, dma,
            reg, reg,
        ],
        compiler_params=pltpu.CompilerParams(
            collective_id=0, has_side_effects=True, vmem_limit_bytes=44 * 1024 * 1024
        ),
    )(
        *(
            pltpu.with_memory_space_constraint(v, pltpu.HBM)
            for v in (
                tokens.reshape(NTP, SEQ, tokens.shape[1]), store.reshape(-1, store.shape[-1]), holder.T, slot.T,
                wq, wo, wi, wv, wk, wval, taps, route.T, cout, mout,
            )
        )
    )


def solution(mesh):
    return jax.shard_map(
        local,
        mesh=mesh,
        in_specs=(
            P("st", "tp"), P("st", None, None), P("st", None), P("st", None),
            P(None, "tp"), P(None, "tp"), P(None, "tp"), P(None, "tp"), P(None, "tp"),
            P(None, "tp"), P(None, "tp"), P(), P("tp", None), P("tp", None),
        ),
        out_specs=P(("st", "tp"), None),
        check_vma=False,
    )
```

```python
import jax
import jax.numpy as jnp
from jax import lax
from jax.experimental import pallas as pl
from jax.experimental.pallas import tpu as pltpu
from jax.sharding import PartitionSpec as P

HEAD_SIZE = 128
SEQ = 256
BLOCK = 128
PLEN = 64
CAP = 4
NY = 4
NXZ = 4
NST = 16
NTP = 8
STEP = 32
WIDE = 1024
MESH = pl.DeviceIdType.MESH
F32 = jnp.float32
BF16 = jnp.bfloat16


def kernel(
    tokens, store, holder_h, slot_h, wq, wo, wi, wv, wk, wval, taps_h, route_h, cout, mout,
    out,
    PM, OB, holder, slot, taps, route, G, ST, WIN, WKV, TB, KS, KR, OV, WV, WS, PV, PS, Q, AS, A, W,
    lsem, stsem, ixr, ixs, kvr, kvs, agr, sib, gsend, arecv, asend,
    wloc, w1, p1, p2, wsib, wsown, wsend, osem, row_sem, all_sem,
):
    st = lax.axis_index("st")
    tp = lax.axis_index("tp")
    y = lax.div(tp, 2)
    k = lax.rem(tp, 2)
    z = lax.div(st, NXZ)
    x = lax.rem(st, NXZ)
    a = (1 - k) * x + k * z
    b = (1 - k) * z + k * x

    def stidx(aa, bb):
        return (1 - k) * (bb * NXZ + aa) + k * (aa * NXZ + bb)

    def ring(v, d):
        return lax.rem(v + d + 4, 4)

    def dev_y(d):
        return (st, ring(y, d) * 2 + k)

    sibling = (st, y * 2 + (1 - k))

    def rcopy(src, dst, ssem, rsem, dev):
        return pltpu.make_async_remote_copy(
            src_ref=src, dst_ref=dst, send_sem=ssem, recv_sem=rsem,
            device_id=dev, device_id_type=MESH,
        )

    def arrived(ref, sem):
        pltpu.make_async_copy(ref, ref, sem).wait()

    def rows(t):
        return pl.ds(pl.multiple_of(t * STEP, STEP), STEP)

    bar = pltpu.get_barrier_semaphore()

    def signal(sem, dev):
        pl.semaphore_signal(sem, inc=1, device_id=dev, device_id_type=MESH)

    def sig_row(d, _):
        p = lax.rem(y + d, NY) * 2 + 1

        @pl.when(p != tp)
        def _():
            signal(bar, (st, p))

        return 0

    def sig_st(d, _):
        signal(bar, (lax.rem(st + d, NST), y * 2))
        return 0

    lax.fori_loop(0, NY, sig_row, 0)
    lax.fori_loop(1, NST, sig_st, 0)

    loads = []
    for j, w in enumerate((wq, wo, wi, wv)):
        loads.append(pltpu.make_async_copy(w, WIN.at[:, pl.ds(j * 128, 128)], lsem.at[0]))
    for j, w in enumerate((wk, wval)):
        loads.append(pltpu.make_async_copy(w, WKV.at[:, pl.ds(j * 128, 128)], lsem.at[1]))
    own = pltpu.make_async_copy(tokens, G.at[tp], lsem.at[2])
    small = [
        pltpu.make_async_copy(p, q, lsem.at[3 + j])
        for j, (p, q) in enumerate(((holder_h, holder), (slot_h, slot), (taps_h, taps), (route_h, route)))
    ]
    for c in small + loads[4:]:
        c.start()

    def store_copy(i):
        r = pl.ds(pl.multiple_of(i * SEQ, SEQ), SEQ)
        return pltpu.make_async_copy(store.at[r, :], ST.at[r, :], stsem)

    def start_store(i, _):
        store_copy(i).start()
        return 0

    lax.fori_loop(0, 8, start_store, 0)
    for c in loads[:4]:
        c.start()
    own.start()

    def wcol(m, cs):
        return (cout, mout)[m].at[:, pl.ds(pl.multiple_of(cs * 128, 128), 128)]

    def start_wl(cs, _):
        for m in range(2):
            pltpu.make_async_copy(wcol(m, cs), W.at[cs, k, y, m], wloc).start()
        return 0

    lax.fori_loop(0, NST, start_wl, 0)
    for c in small[:2]:
        c.wait()

    rowi = lax.broadcasted_iota(jnp.int32, (NST, 128), 0)
    lanei = lax.broadcasted_iota(jnp.int32, (NST, 128), 1)
    count = jnp.zeros((NST, 128), jnp.int32)
    wanted = jnp.zeros((NST, 128), jnp.int32)
    for r in range(32):
        o = holder[r % 2, r // 2]
        v = slot[r % 2, r // 2]
        hit = rowi == o
        PV[r] = jnp.sum(jnp.where(hit, count, 0), axis=0, keepdims=True) + o * CAP
        wanted = jnp.where(hit & (lanei == count), v, wanted)
        count = count + hit.astype(jnp.int32)
    for o in range(NST):
        OV[o] = wanted[o : o + 1]
    pcopy = pltpu.make_async_copy(PV, PS, lsem.at[7])
    pcopy.start()

    @pl.when(k == 1)
    def _():
        pl.semaphore_wait(bar, NTP - 1)
        signal(row_sem, sibling)

    @pl.when(k == 0)
    def _():
        pl.semaphore_wait(row_sem, 1)

    def direct(t):
        src = tokens.at[:, rows(t), :]
        dst = G.at[tp, :, rows(t), :]
        rcopy(src, dst, gsend, agr.at[t, 0], dev_y(1)).start()
        rcopy(src, dst, gsend, agr.at[t, 1], dev_y(-1)).start()
        rcopy(src, dst, gsend, sib.at[t], sibling).start()

    def gblk(d):
        return ring(y, d) * 2 + k


    def w1_start(dy, _):
        for m in range(2):
            rcopy(
                wcol(m, st), W.at[st, k, y, m], wsend, w1,
                (st, lax.rem(y + dy, 4) * 2 + k),
            ).start()
        return 0

    lax.fori_loop(1, 4, w1_start, 0)
    direct(0)
    direct(1)

    @pl.when(k == 0)
    def _():
        pl.semaphore_wait(bar, 2 * (NST - 1))
        signal(all_sem, sibling)

    @pl.when(k == 1)
    def _():
        pl.semaphore_wait(all_sem, 1)

    def ix_copy(d):
        r = lax.rem(st + d, NST)
        return rcopy(OV.at[r], WV.at[st], ixs, ixr, (r, tp))

    def ix_start(d, _):
        ix_copy(d).start()
        return 0

    lax.fori_loop(1, NST, ix_start, 0)
    pltpu.make_async_copy(OV.at[st], WV.at[st], ixr).start()

    arrived(WKV, lsem.at[1])
    arrived(ST, stsem)

    def kv_body(i, _):
        r = pl.ds(pl.multiple_of(i * SEQ, SEQ), SEQ)
        kv = jnp.dot(ST[r, :], WKV[...], preferred_element_type=F32).astype(BF16)
        for j in range(4):
            TB[i * 4 + j] = kv[j * PLEN : (j + 1) * PLEN]
        return 0

    lax.fori_loop(0, 3, kv_body, 0)
    direct(2)
    lax.fori_loop(3, 6, kv_body, 0)

    def send_kv():
        arrived(WV, ixr)
        c = pltpu.make_async_copy(WV, WS, lsem.at[3])
        c.start()
        c.wait()
        lax.fori_loop(1, 4, kv_out, 0)
        for j in range(CAP):
            KS[st, j] = TB[WS[st, 0, j]]
        pltpu.make_async_copy(KS.at[st], KR.at[pl.ds(st * CAP, CAP)], kvr).start()

    def kv_out(d, _):
        r = lax.rem(st + d, NST)
        for j in range(CAP):
            KS[r, j] = TB[WS[r, 0, j]]
        rcopy(KS.at[r], KR.at[pl.ds(st * CAP, CAP)], kvs, kvr, (r, tp)).start()
        return 0

    def dev_a(d):
        return (stidx(ring(a, d), b), tp)

    def dev_b(d):
        return (stidx(a, ring(b, d)), tp)

    def yo(dy):
        return lax.rem(y + dy, 4)

    def plane1():
        arrived(W.at[pl.ds(0, 3), 0, 0], w1)

        def go2(j, _):
            da = lax.div(j, 3) + 1
            dy = lax.rem(j, 3) + 1
            blk = W.at[st, k, yo(dy)]
            rcopy(blk, blk, wsend, p1, (stidx(lax.rem(a + da, 4), b), tp)).start()
            return 0

        lax.fori_loop(0, 9, go2, 0)

    def wblk(j, d):
        return W.at[stidx(lax.div(j, 3), ring(b, d)), k, yo(lax.rem(j, 3) + 1)]

    def wpass(lo, hi, d, sem, dev):
        def go(j, _):
            g = wblk(j, d)
            rcopy(g, g, wsend, sem, dev).start()
            return 0

        lax.fori_loop(lo, hi, go, 0)

    SIX = W.at[pl.ds(0, 6), 0, 0]
    TWELVE = W.at[pl.ds(0, 3), 0]

    def plane2():
        arrived(W.at[pl.ds(0, 9), 0, 0], p1)
        wpass(0, 6, 0, p2.at[0], dev_b(1))
        wpass(6, 12, 0, p2.at[1], dev_b(-1))
        wpass(0, 12, 0, wsib.at[0], sibling)

    def plane3():
        arrived(SIX, p2.at[0])
        arrived(SIX, p2.at[1])
        wpass(0, 6, -1, p2.at[2], dev_b(1))
        wpass(6, 12, 1, p2.at[4], dev_b(-1))
        wpass(0, 6, -1, wsib.at[1], sibling)
        wpass(6, 12, 1, wsib.at[1], sibling)

    def plane4():
        arrived(TWELVE, p2.at[3])
        wpass(6, 12, -1, wsib.at[2], sibling)
        wpass(0, 6, 1, wsib.at[2], sibling)

    def plane5():
        arrived(SIX, p2.at[2])
        wpass(0, 6, 2, wsib.at[3], sibling)
        arrived(SIX, p2.at[4])
        wpass(6, 12, 2, wsib.at[3], sibling)

    plane1()
    lax.fori_loop(6, 8, kv_body, 0)
    send_kv()

    def send_branch(m, lo, n):
        r = pl.ds(pl.multiple_of(lo, STEP), n)

        def go(d, _):
            s = lax.rem(tp + d, NTP)
            rcopy(AS.at[m, s, r, :], A.at[m, tp, r, :], asend, arecv, (st, s)).start()
            return 0

        lax.fori_loop(1, NTP, go, 0)
        pltpu.make_async_copy(AS.at[m, tp, r, :], A.at[m, tp, r, :], arecv).start()

    arrived(WIN, lsem.at[0])
    for c in small[2:]:
        c.wait()
    own.wait()
    arrived(W.at[:, k, y], wloc)
    rcopy(W.at[:, k, y], W.at[:, k, y], wsend, wsown, sibling).start()
    PM[...] = jnp.zeros_like(PM)
    place = lax.rem(lax.broadcasted_iota(jnp.int32, (SEQ, 128), 0), STEP)

    def project(t):
        arrived(G.at[pl.ds(0, 4), :, rows(t), :], sib.at[t])
        rws = jnp.concatenate([G[j, :, rows(t), :].reshape(SEQ, 256) for j in range(NTP)], axis=1)
        p = jnp.dot(rws, WIN[...], preferred_element_type=F32)
        Q[:, rows(t), :] = p[:, 0:128].astype(BF16).reshape(NTP, STEP, 128)
        mixed = p[:, 256:384] * p[:, 384:512]
        prev = PM[...]
        PM[...] = mixed
        tv = taps[...].astype(F32)
        m1 = jnp.where(place >= 1, pltpu.roll(mixed, 1, 0), pltpu.roll(prev, SEQ + 1 - STEP, 0))
        m2 = jnp.where(place >= 2, pltpu.roll(mixed, 2, 0), pltpu.roll(prev, SEQ + 2 - STEP, 0))
        filt = tv[0:1] * m2 + tv[1:2] * m1 + tv[2:3] * mixed
        AS[0, :, rows(t), :] = (p[:, 128:256] * filt).astype(BF16).reshape(NTP, STEP, 128)
        send_branch(0, t * STEP, STEP)

    def attend(seqs, lo, n):
        blk = lo // BLOCK if isinstance(lo, int) else 0
        r = pl.ds(lo, n)
        kvs_, sc = [], []
        for s in seqs:
            i = (s * 2 + blk) * 2
            kv = jnp.concatenate([KR[PS[i, 0, 0]], KR[PS[i + 1, 0, 0]]], axis=0)
            kvs_.append(kv)
            sc.append(
                lax.dot_general(
                    Q[s, r, :], kv[:, :128], (((1,), (1,)), ((), ())), preferred_element_type=F32
                ) * (HEAD_SIZE ** -0.5)
            )
        e = [jnp.exp(v - jnp.max(v, axis=1, keepdims=True)) for v in sc]
        wt = [(v / jnp.sum(v, axis=1, keepdims=True)).astype(BF16) for v in e]
        for s, kv, v in zip(seqs, kvs_, wt):
            o = jnp.dot(v, kv[:, 128:], preferred_element_type=F32)
            AS[1, s, r, :] = o.astype(BF16)

    def step(t, _):
        @pl.when(t < 8)
        def _():
            r = rows(t)
            g = G.at[gblk(-1), :, r, :]
            arrived(g, agr.at[t, 0])
            h = G.at[gblk(-1), pl.ds(0, 4), r, :]
            rcopy(h, h, gsend, agr.at[t, 2], dev_y(1)).start()
            rcopy(g, g, gsend, sib.at[t], sibling).start()
            g2 = G.at[gblk(1), :, r, :]
            arrived(g2, agr.at[t, 1])
            h2 = G.at[gblk(1), pl.ds(4, 4), r, :]
            rcopy(h2, h2, gsend, agr.at[t, 2], dev_y(-1)).start()
            rcopy(g2, g2, gsend, sib.at[t], sibling).start()

        @pl.when((t >= 1) & (t < 6))
        def _():
            direct(t + 2)

        @pl.when(t <= 1)
        def _():
            lax.fori_loop(4 + 6 * t, 10 + 6 * t, kv_out, 0)

        @pl.when(t == 4)
        def _():
            plane2()

        @pl.when(t == 6)
        def _():
            wpass(6, 12, 0, p2.at[3], dev_b(1))
            wpass(0, 6, 0, p2.at[3], dev_b(-1))

        def opposite(u):
            g = G.at[gblk(2), :, rows(u), :]
            arrived(g, agr.at[u, 2])
            rcopy(g, g, gsend, sib.at[u], sibling).start()

        @pl.when((t >= 1) & (t < 9))
        def _():
            opposite(t - 1)

        @pl.when(t == 8)
        def _():
            attend(range(NTP), BLOCK, 64)
            send_branch(1, BLOCK, 64)

        @pl.when(t >= 2)
        def _():
            project(t - 2)

        @pl.when(t == 7)
        def _():
            plane3()
            arrived(KR, kvr)
            pcopy.wait()

            def two(i, _):
                attend(range(NTP), pl.multiple_of(i * 64, 64), 64)
                send_branch(1, i * 64, 64)
                return 0

            lax.fori_loop(0, 2, two, 0)
        @pl.when(t == 8)
        def _():
            plane4()

        return 0

    lax.fori_loop(0, 10, step, 0)
    attend(range(NTP), BLOCK + 64, 64)
    send_branch(1, BLOCK + 64, 64)
    plane5()
    rws = jnp.concatenate([G[j, tp] for j in range(NTP)], axis=1)
    logits = lax.dot_general(rws, route[...], (((1,), (1,)), ((), ())), preferred_element_type=F32)
    mix = jax.nn.sigmoid(logits)

    arrived(W.at[:, 1 - k, y], wsown)
    for d in range(4):
        arrived(TWELVE, wsib.at[d])

    order = [(kk, yy) for kk in range(2) for yy in range(4)]

    def put(c):
        return pltpu.make_async_copy(
            OB.at[c], out.at[:, pl.ds(pl.multiple_of(c * WIDE, WIDE), WIDE)], osem
        )

    def outp(c, _):
        acc = []
        for m in range(2):
            lhs = jnp.concatenate([A[m, yy * 2 + kk] for kk, yy in order], axis=1)
            rhs = jnp.concatenate(
                [
                    jnp.concatenate([W[c * (WIDE // 128) + i, kk, yy, m] for kk, yy in order], axis=0)
                    for i in range(WIDE // 128)
                ],
                axis=1,
            )
            acc.append(jnp.dot(lhs, rhs, preferred_element_type=F32))
        OB[c] = (mix[:, 0:1] * acc[0] + mix[:, 1:2] * acc[1]).astype(BF16)
        put(c).start()
        return 0

    arrived(A, arecv)
    lax.fori_loop(0, 2048 // WIDE, outp, 0)

    arrived(OB, osem)
    arrived(OV.at[pl.ds(0, NST - 1)], ixs)
    arrived(KS.at[pl.ds(0, NST - 1)], kvs)
    arrived(G.at[pl.ds(0, 7)], gsend)
    arrived(AS.at[:, pl.ds(0, 7)], asend)
    arrived(W.at[pl.ds(0, 14)], wsend)


def local(
    tokens, store, holder, slot, wq, wk, wval, wo, wi, wv, taps, route, cout, mout
):
    hbm = pl.BlockSpec(memory_space=pltpu.HBM)
    dma = pltpu.SemaphoreType.DMA
    reg = pltpu.SemaphoreType.REGULAR
    V = pltpu.VMEM
    return pl.pallas_call(
        kernel,
        out_shape=jax.ShapeDtypeStruct((SEQ, cout.shape[1]), BF16),
        in_specs=[hbm] * 14,
        out_specs=pl.BlockSpec(memory_space=pl.ANY),
        scratch_shapes=[
            V((SEQ, 128), F32),
            V((2048 // WIDE, SEQ, WIDE), BF16),
            pltpu.SMEM((2, 16), jnp.int32),
            pltpu.SMEM((2, 16), jnp.int32),
            V((3, 128), BF16),
            V((2, 2048), BF16),
            V((8, NTP, SEQ, 256), BF16),
            V((2048, 2048), BF16),
            V((2048, 512), BF16),
            V((2048, 256), BF16),
            V((32, PLEN, 256), BF16),
            V((NST, CAP, PLEN, 256), BF16),
            V((NST * CAP, PLEN, 256), BF16),
            V((NST, 1, 128), jnp.int32),
            V((NST, 1, 128), jnp.int32),
            pltpu.SMEM((NST, 1, 128), jnp.int32),
            V((32, 1, 128), jnp.int32),
            pltpu.SMEM((32, 1, 128), jnp.int32),
            V((NTP, SEQ, 128), BF16),
            V((2, 8, SEQ, 128), BF16),
            V((2, 8, SEQ, 128), BF16),
            V((NST, 2, 4, 2, 128, 128), BF16),
            dma((8,)), dma, dma, dma, dma, dma,
            dma((8, 3)), dma((8,)), dma, dma, dma,
            dma, dma, dma, dma((5,)), dma((4,)), dma, dma, dma,
            reg, reg,
        ],
        compiler_params=pltpu.CompilerParams(
            collective_id=0, has_side_effects=True, vmem_limit_bytes=44 * 1024 * 1024
        ),
    )(
        *(
            pltpu.with_memory_space_constraint(v, pltpu.HBM)
            for v in (
                tokens.reshape(NTP, SEQ, tokens.shape[1]), store.reshape(-1, store.shape[-1]), holder.T, slot.T,
                wq, wo, wi, wv, wk, wval, taps, route.T, cout, mout,
            )
        )
    )


def solution(mesh):
    return jax.shard_map(
        local,
        mesh=mesh,
        in_specs=(
            P("st", "tp"), P("st", None, None), P("st", None), P("st", None),
            P(None, "tp"), P(None, "tp"), P(None, "tp"), P(None, "tp"), P(None, "tp"),
            P(None, "tp"), P(None, "tp"), P(), P("tp", None), P("tp", None),
        ),
        out_specs=P(("st", "tp"), None),
        check_vma=False,
    )
```

```python
import jax
import jax.numpy as jnp
from jax import lax
from jax.experimental import pallas as pl
from jax.experimental.pallas import tpu as pltpu
from jax.sharding import PartitionSpec as P

HEAD_SIZE = 128
SEQ = 256
BLOCK = 128
PLEN = 64
CAP = 4
NY = 4
NXZ = 4
NST = 16
NTP = 8
STEP = 32
WIDE = 1024
MESH = pl.DeviceIdType.MESH
F32 = jnp.float32
BF16 = jnp.bfloat16


def kernel(
    tokens, store, holder_h, slot_h, wq, wo, wi, wv, wk, wval, taps_h, route_h, cout, mout,
    out,
    PM, OB, holder, slot, taps, route, G, ST, WIN, WKV, TB, KS, KR, OV, WV, WS, PV, PS, Q, AS, A, W,
    lsem, stsem, ixr, ixs, kvr, kvs, agr, sib, gsend, arecv, asend,
    wloc, w1, p1, p2, wsib, wsown, wsend, osem, row_sem, all_sem,
):
    st = lax.axis_index("st")
    tp = lax.axis_index("tp")
    y = lax.div(tp, 2)
    k = lax.rem(tp, 2)
    z = lax.div(st, NXZ)
    x = lax.rem(st, NXZ)
    a = (1 - k) * x + k * z
    b = (1 - k) * z + k * x

    def stidx(aa, bb):
        return (1 - k) * (bb * NXZ + aa) + k * (aa * NXZ + bb)

    def ring(v, d):
        return lax.rem(v + d + 4, 4)

    def dev_y(d):
        return (st, ring(y, d) * 2 + k)

    sibling = (st, y * 2 + (1 - k))

    def rcopy(src, dst, ssem, rsem, dev):
        return pltpu.make_async_remote_copy(
            src_ref=src, dst_ref=dst, send_sem=ssem, recv_sem=rsem,
            device_id=dev, device_id_type=MESH,
        )

    def arrived(ref, sem):
        pltpu.make_async_copy(ref, ref, sem).wait()

    def rows(t):
        return pl.ds(pl.multiple_of(t * STEP, STEP), STEP)

    bar = pltpu.get_barrier_semaphore()

    def signal(sem, dev):
        pl.semaphore_signal(sem, inc=1, device_id=dev, device_id_type=MESH)

    def sig_row(d, _):
        p = lax.rem(y + d, NY) * 2 + 1

        @pl.when(p != tp)
        def _():
            signal(bar, (st, p))

        return 0

    def sig_st(d, _):
        signal(bar, (lax.rem(st + d, NST), y * 2))
        return 0

    lax.fori_loop(0, NY, sig_row, 0)
    lax.fori_loop(1, NST, sig_st, 0)

    loads = []
    for j, w in enumerate((wq, wo, wi, wv)):
        loads.append(pltpu.make_async_copy(w, WIN.at[:, pl.ds(j * 128, 128)], lsem.at[0]))
    for j, w in enumerate((wk, wval)):
        loads.append(pltpu.make_async_copy(w, WKV.at[:, pl.ds(j * 128, 128)], lsem.at[1]))
    own = pltpu.make_async_copy(tokens, G.at[tp], lsem.at[2])
    small = [
        pltpu.make_async_copy(p, q, lsem.at[3 + j])
        for j, (p, q) in enumerate(((holder_h, holder), (slot_h, slot), (taps_h, taps), (route_h, route)))
    ]
    for c in small + loads[4:]:
        c.start()

    def store_copy(i):
        r = pl.ds(pl.multiple_of(i * SEQ, SEQ), SEQ)
        return pltpu.make_async_copy(store.at[r, :], ST.at[r, :], stsem)

    def start_store(i, _):
        store_copy(i).start()
        return 0

    lax.fori_loop(0, 8, start_store, 0)
    for c in loads[:4]:
        c.start()
    own.start()

    def wcol(m, cs):
        return (cout, mout)[m].at[:, pl.ds(pl.multiple_of(cs * 128, 128), 128)]

    def start_wl(cs, _):
        for m in range(2):
            pltpu.make_async_copy(wcol(m, cs), W.at[cs, k, y, m], wloc).start()
        return 0

    lax.fori_loop(0, NST, start_wl, 0)
    for c in small[:2]:
        c.wait()

    rowi = lax.broadcasted_iota(jnp.int32, (NST, 128), 0)
    lanei = lax.broadcasted_iota(jnp.int32, (NST, 128), 1)
    count = jnp.zeros((NST, 128), jnp.int32)
    wanted = jnp.zeros((NST, 128), jnp.int32)
    for r in range(32):
        o = holder[r % 2, r // 2]
        v = slot[r % 2, r // 2]
        hit = rowi == o
        PV[r] = jnp.sum(jnp.where(hit, count, 0), axis=0, keepdims=True) + o * CAP
        wanted = jnp.where(hit & (lanei == count), v, wanted)
        count = count + hit.astype(jnp.int32)
    for o in range(NST):
        OV[o] = wanted[o : o + 1]
    pcopy = pltpu.make_async_copy(PV, PS, lsem.at[7])
    pcopy.start()

    @pl.when(k == 1)
    def _():
        pl.semaphore_wait(bar, NTP - 1)
        signal(row_sem, sibling)

    @pl.when(k == 0)
    def _():
        pl.semaphore_wait(row_sem, 1)

    def direct(t):
        src = tokens.at[:, rows(t), :]
        dst = G.at[tp, :, rows(t), :]
        rcopy(src, dst, gsend, agr.at[t, 0], dev_y(1)).start()
        rcopy(src, dst, gsend, agr.at[t, 1], dev_y(-1)).start()
        rcopy(src, dst, gsend, sib.at[t], sibling).start()

    def gblk(d):
        return ring(y, d) * 2 + k


    def w1_start(dy, _):
        for m in range(2):
            rcopy(
                wcol(m, st), W.at[st, k, y, m], wsend, w1,
                (st, lax.rem(y + dy, 4) * 2 + k),
            ).start()
        return 0

    lax.fori_loop(1, 4, w1_start, 0)
    direct(0)
    direct(1)

    @pl.when(k == 0)
    def _():
        pl.semaphore_wait(bar, 2 * (NST - 1))
        signal(all_sem, sibling)

    @pl.when(k == 1)
    def _():
        pl.semaphore_wait(all_sem, 1)

    def ix_copy(d):
        r = lax.rem(st + d, NST)
        return rcopy(OV.at[r], WV.at[st], ixs, ixr, (r, tp))

    def ix_start(d, _):
        ix_copy(d).start()
        return 0

    lax.fori_loop(1, NST, ix_start, 0)
    pltpu.make_async_copy(OV.at[st], WV.at[st], ixr).start()

    arrived(WKV, lsem.at[1])
    arrived(ST, stsem)

    def kv_body(i, _):
        r = pl.ds(pl.multiple_of(i * SEQ, SEQ), SEQ)
        kv = jnp.dot(ST[r, :], WKV[...], preferred_element_type=F32).astype(BF16)
        for j in range(4):
            TB[i * 4 + j] = kv[j * PLEN : (j + 1) * PLEN]
        return 0

    lax.fori_loop(0, 3, kv_body, 0)
    direct(2)
    lax.fori_loop(3, 6, kv_body, 0)

    def send_kv():
        arrived(WV, ixr)
        c = pltpu.make_async_copy(WV, WS, lsem.at[3])
        c.start()
        c.wait()
        lax.fori_loop(1, 4, kv_out, 0)
        for j in range(CAP):
            KS[st, j] = TB[WS[st, 0, j]]
        pltpu.make_async_copy(KS.at[st], KR.at[pl.ds(st * CAP, CAP)], kvr).start()

    def kv_out(d, _):
        r = lax.rem(st + d, NST)
        for j in range(CAP):
            KS[r, j] = TB[WS[r, 0, j]]
        rcopy(KS.at[r], KR.at[pl.ds(st * CAP, CAP)], kvs, kvr, (r, tp)).start()
        return 0

    def dev_a(d):
        return (stidx(ring(a, d), b), tp)

    def dev_b(d):
        return (stidx(a, ring(b, d)), tp)

    def yo(dy):
        return lax.rem(y + dy, 4)

    def plane1():
        arrived(W.at[pl.ds(0, 3), 0, 0], w1)

        def go2(j, _):
            da = lax.div(j, 3) + 1
            dy = lax.rem(j, 3) + 1
            blk = W.at[st, k, yo(dy)]
            rcopy(blk, blk, wsend, p1, (stidx(lax.rem(a + da, 4), b), tp)).start()
            return 0

        lax.fori_loop(0, 9, go2, 0)

    def wblk(j, d):
        return W.at[stidx(lax.div(j, 3), ring(b, d)), k, yo(lax.rem(j, 3) + 1)]

    def wpass(lo, hi, d, sem, dev):
        def go(j, _):
            g = wblk(j, d)
            rcopy(g, g, wsend, sem, dev).start()
            return 0

        lax.fori_loop(lo, hi, go, 0)

    SIX = W.at[pl.ds(0, 6), 0, 0]
    TWELVE = W.at[pl.ds(0, 3), 0]

    def plane2():
        arrived(W.at[pl.ds(0, 9), 0, 0], p1)
        wpass(0, 6, 0, p2.at[0], dev_b(1))
        wpass(6, 12, 0, p2.at[1], dev_b(-1))
        wpass(0, 12, 0, wsib.at[0], sibling)

    def plane3():
        arrived(SIX, p2.at[0])
        wpass(0, 6, -1, p2.at[2], dev_b(1))
        arrived(SIX, p2.at[1])
        wpass(6, 12, 1, p2.at[4], dev_b(-1))
        wpass(0, 6, -1, wsib.at[1], sibling)
        wpass(6, 12, 1, wsib.at[1], sibling)

    def plane4():
        arrived(TWELVE, p2.at[3])
        wpass(6, 12, -1, wsib.at[2], sibling)
        wpass(0, 6, 1, wsib.at[2], sibling)

    def plane5():
        arrived(SIX, p2.at[2])
        wpass(0, 6, 2, wsib.at[3], sibling)
        arrived(SIX, p2.at[4])
        wpass(6, 12, 2, wsib.at[3], sibling)

    plane1()
    lax.fori_loop(6, 8, kv_body, 0)
    send_kv()

    def send_branch(m, lo, n):
        r = pl.ds(pl.multiple_of(lo, STEP), n)

        def go(d, _):
            s = lax.rem(tp + d, NTP)
            rcopy(AS.at[m, s, r, :], A.at[m, tp, r, :], asend, arecv, (st, s)).start()
            return 0

        lax.fori_loop(1, NTP, go, 0)
        pltpu.make_async_copy(AS.at[m, tp, r, :], A.at[m, tp, r, :], arecv).start()

    arrived(WIN, lsem.at[0])
    for c in small[2:]:
        c.wait()
    own.wait()
    arrived(W.at[:, k, y], wloc)
    rcopy(W.at[:, k, y], W.at[:, k, y], wsend, wsown, sibling).start()
    PM[...] = jnp.zeros_like(PM)
    place = lax.rem(lax.broadcasted_iota(jnp.int32, (SEQ, 128), 0), STEP)

    def project(t):
        arrived(G.at[pl.ds(0, 4), :, rows(t), :], sib.at[t])
        rws = jnp.concatenate([G[j, :, rows(t), :].reshape(SEQ, 256) for j in range(NTP)], axis=1)
        p = jnp.dot(rws, WIN[...], preferred_element_type=F32)
        Q[:, rows(t), :] = p[:, 0:128].astype(BF16).reshape(NTP, STEP, 128)
        mixed = p[:, 256:384] * p[:, 384:512]
        prev = PM[...]
        PM[...] = mixed
        tv = taps[...].astype(F32)
        m1 = jnp.where(place >= 1, pltpu.roll(mixed, 1, 0), pltpu.roll(prev, SEQ + 1 - STEP, 0))
        m2 = jnp.where(place >= 2, pltpu.roll(mixed, 2, 0), pltpu.roll(prev, SEQ + 2 - STEP, 0))
        filt = tv[0:1] * m2 + tv[1:2] * m1 + tv[2:3] * mixed
        AS[0, :, rows(t), :] = (p[:, 128:256] * filt).astype(BF16).reshape(NTP, STEP, 128)
        send_branch(0, t * STEP, STEP)

    def attend(seqs, lo, n):
        blk = lo // BLOCK if isinstance(lo, int) else 0
        r = pl.ds(lo, n)
        kvs_, sc = [], []
        for s in seqs:
            i = (s * 2 + blk) * 2
            kv = jnp.concatenate([KR[PS[i, 0, 0]], KR[PS[i + 1, 0, 0]]], axis=0)
            kvs_.append(kv)
            sc.append(
                lax.dot_general(
                    Q[s, r, :], kv[:, :128], (((1,), (1,)), ((), ())), preferred_element_type=F32
                ) * (HEAD_SIZE ** -0.5)
            )
        e = [jnp.exp(v - jnp.max(v, axis=1, keepdims=True)) for v in sc]
        wt = [(v / jnp.sum(v, axis=1, keepdims=True)).astype(BF16) for v in e]
        for s, kv, v in zip(seqs, kvs_, wt):
            o = jnp.dot(v, kv[:, 128:], preferred_element_type=F32)
            AS[1, s, r, :] = o.astype(BF16)

    def step(t, _):
        @pl.when(t < 8)
        def _():
            r = rows(t)
            g = G.at[gblk(-1), :, r, :]
            arrived(g, agr.at[t, 0])
            h = G.at[gblk(-1), pl.ds(0, 4), r, :]
            rcopy(h, h, gsend, agr.at[t, 2], dev_y(1)).start()
            rcopy(g, g, gsend, sib.at[t], sibling).start()
            g2 = G.at[gblk(1), :, r, :]
            arrived(g2, agr.at[t, 1])
            h2 = G.at[gblk(1), pl.ds(4, 4), r, :]
            rcopy(h2, h2, gsend, agr.at[t, 2], dev_y(-1)).start()
            rcopy(g2, g2, gsend, sib.at[t], sibling).start()

        @pl.when((t >= 1) & (t < 6))
        def _():
            direct(t + 2)

        @pl.when(t <= 1)
        def _():
            lax.fori_loop(4 + 6 * t, 10 + 6 * t, kv_out, 0)

        @pl.when(t == 4)
        def _():
            plane2()

        @pl.when(t == 6)
        def _():
            wpass(6, 12, 0, p2.at[3], dev_b(1))
            wpass(0, 6, 0, p2.at[3], dev_b(-1))

        def opposite(u):
            g = G.at[gblk(2), :, rows(u), :]
            arrived(g, agr.at[u, 2])
            rcopy(g, g, gsend, sib.at[u], sibling).start()

        @pl.when((t >= 1) & (t < 9))
        def _():
            opposite(t - 1)

        @pl.when(t == 8)
        def _():
            attend(range(NTP), BLOCK, 64)
            send_branch(1, BLOCK, 64)

        @pl.when(t >= 2)
        def _():
            project(t - 2)

        @pl.when(t == 7)
        def _():
            plane3()
            arrived(KR, kvr)
            pcopy.wait()

            def two(i, _):
                attend(range(NTP), pl.multiple_of(i * 64, 64), 64)
                send_branch(1, i * 64, 64)
                return 0

            lax.fori_loop(0, 2, two, 0)
        @pl.when(t == 8)
        def _():
            plane4()

        return 0

    lax.fori_loop(0, 10, step, 0)
    attend(range(NTP), BLOCK + 64, 64)
    send_branch(1, BLOCK + 64, 64)
    plane5()
    rws = jnp.concatenate([G[j, tp] for j in range(NTP)], axis=1)
    logits = lax.dot_general(rws, route[...], (((1,), (1,)), ((), ())), preferred_element_type=F32)
    mix = jax.nn.sigmoid(logits)

    arrived(W.at[:, 1 - k, y], wsown)
    for d in range(4):
        arrived(TWELVE, wsib.at[d])

    order = [(kk, yy) for kk in range(2) for yy in range(4)]

    def put(c):
        return pltpu.make_async_copy(
            OB.at[c], out.at[:, pl.ds(pl.multiple_of(c * WIDE, WIDE), WIDE)], osem
        )

    def outp(c, _):
        acc = []
        for m in range(2):
            lhs = jnp.concatenate([A[m, yy * 2 + kk] for kk, yy in order], axis=1)
            rhs = jnp.concatenate(
                [
                    jnp.concatenate([W[c * (WIDE // 128) + i, kk, yy, m] for kk, yy in order], axis=0)
                    for i in range(WIDE // 128)
                ],
                axis=1,
            )
            acc.append(jnp.dot(lhs, rhs, preferred_element_type=F32))
        OB[c] = (mix[:, 0:1] * acc[0] + mix[:, 1:2] * acc[1]).astype(BF16)
        put(c).start()
        return 0

    arrived(A, arecv)
    lax.fori_loop(0, 2048 // WIDE, outp, 0)

    arrived(OB, osem)
    arrived(OV.at[pl.ds(0, NST - 1)], ixs)
    arrived(KS.at[pl.ds(0, NST - 1)], kvs)
    arrived(G.at[pl.ds(0, 7)], gsend)
    arrived(AS.at[:, pl.ds(0, 7)], asend)
    arrived(W.at[pl.ds(0, 14)], wsend)


def local(
    tokens, store, holder, slot, wq, wk, wval, wo, wi, wv, taps, route, cout, mout
):
    hbm = pl.BlockSpec(memory_space=pltpu.HBM)
    dma = pltpu.SemaphoreType.DMA
    reg = pltpu.SemaphoreType.REGULAR
    V = pltpu.VMEM
    return pl.pallas_call(
        kernel,
        out_shape=jax.ShapeDtypeStruct((SEQ, cout.shape[1]), BF16),
        in_specs=[hbm] * 14,
        out_specs=pl.BlockSpec(memory_space=pl.ANY),
        scratch_shapes=[
            V((SEQ, 128), F32),
            V((2048 // WIDE, SEQ, WIDE), BF16),
            pltpu.SMEM((2, 16), jnp.int32),
            pltpu.SMEM((2, 16), jnp.int32),
            V((3, 128), BF16),
            V((2, 2048), BF16),
            V((8, NTP, SEQ, 256), BF16),
            V((2048, 2048), BF16),
            V((2048, 512), BF16),
            V((2048, 256), BF16),
            V((32, PLEN, 256), BF16),
            V((NST, CAP, PLEN, 256), BF16),
            V((NST * CAP, PLEN, 256), BF16),
            V((NST, 1, 128), jnp.int32),
            V((NST, 1, 128), jnp.int32),
            pltpu.SMEM((NST, 1, 128), jnp.int32),
            V((32, 1, 128), jnp.int32),
            pltpu.SMEM((32, 1, 128), jnp.int32),
            V((NTP, SEQ, 128), BF16),
            V((2, 8, SEQ, 128), BF16),
            V((2, 8, SEQ, 128), BF16),
            V((NST, 2, 4, 2, 128, 128), BF16),
            dma((8,)), dma, dma, dma, dma, dma,
            dma((8, 3)), dma((8,)), dma, dma, dma,
            dma, dma, dma, dma((5,)), dma((4,)), dma, dma, dma,
            reg, reg,
        ],
        compiler_params=pltpu.CompilerParams(
            collective_id=0, has_side_effects=True, vmem_limit_bytes=44 * 1024 * 1024
        ),
    )(
        *(
            pltpu.with_memory_space_constraint(v, pltpu.HBM)
            for v in (
                tokens.reshape(NTP, SEQ, tokens.shape[1]), store.reshape(-1, store.shape[-1]), holder.T, slot.T,
                wq, wo, wi, wv, wk, wval, taps, route.T, cout, mout,
            )
        )
    )


def solution(mesh):
    return jax.shard_map(
        local,
        mesh=mesh,
        in_specs=(
            P("st", "tp"), P("st", None, None), P("st", None), P("st", None),
            P(None, "tp"), P(None, "tp"), P(None, "tp"), P(None, "tp"), P(None, "tp"),
            P(None, "tp"), P(None, "tp"), P(), P("tp", None), P("tp", None),
        ),
        out_specs=P(("st", "tp"), None),
        check_vma=False,
    )
```

```python
import jax
import jax.numpy as jnp
from jax import lax
from jax.experimental import pallas as pl
from jax.experimental.pallas import tpu as pltpu
from jax.sharding import PartitionSpec as P

HEAD_SIZE = 128
SEQ = 256
BLOCK = 128
PLEN = 64
CAP = 4
NY = 4
NXZ = 4
NST = 16
NTP = 8
STEP = 32
WIDE = 2048
MESH = pl.DeviceIdType.MESH
F32 = jnp.float32
BF16 = jnp.bfloat16


def kernel(
    tokens, store, holder_h, slot_h, wq, wo, wi, wv, wk, wval, taps_h, route_h, cout, mout,
    out,
    PM, OB, holder, slot, taps, route, G, ST, WIN, WKV, TB, KS, KR, OV, WV, WS, PV, PS, Q, AS, A, W,
    lsem, stsem, ixr, ixs, kvr, kvs, agr, sib, gsend, arecv, asend,
    wloc, w1, p1, p2, wsib, wsown, wsend, osem, row_sem, all_sem,
):
    st = lax.axis_index("st")
    tp = lax.axis_index("tp")
    y = lax.div(tp, 2)
    k = lax.rem(tp, 2)
    z = lax.div(st, NXZ)
    x = lax.rem(st, NXZ)
    a = (1 - k) * x + k * z
    b = (1 - k) * z + k * x

    def stidx(aa, bb):
        return (1 - k) * (bb * NXZ + aa) + k * (aa * NXZ + bb)

    def ring(v, d):
        return lax.rem(v + d + 4, 4)

    def dev_y(d):
        return (st, ring(y, d) * 2 + k)

    sibling = (st, y * 2 + (1 - k))

    def rcopy(src, dst, ssem, rsem, dev):
        return pltpu.make_async_remote_copy(
            src_ref=src, dst_ref=dst, send_sem=ssem, recv_sem=rsem,
            device_id=dev, device_id_type=MESH,
        )

    def arrived(ref, sem):
        pltpu.make_async_copy(ref, ref, sem).wait()

    def rows(t):
        return pl.ds(pl.multiple_of(t * STEP, STEP), STEP)

    bar = pltpu.get_barrier_semaphore()

    def signal(sem, dev):
        pl.semaphore_signal(sem, inc=1, device_id=dev, device_id_type=MESH)

    def sig_row(d, _):
        p = lax.rem(y + d, NY) * 2 + 1

        @pl.when(p != tp)
        def _():
            signal(bar, (st, p))

        return 0

    def sig_st(d, _):
        signal(bar, (lax.rem(st + d, NST), y * 2))
        return 0

    lax.fori_loop(0, NY, sig_row, 0)
    lax.fori_loop(1, NST, sig_st, 0)

    loads = []
    for j, w in enumerate((wq, wo, wi, wv)):
        loads.append(pltpu.make_async_copy(w, WIN.at[:, pl.ds(j * 128, 128)], lsem.at[0]))
    for j, w in enumerate((wk, wval)):
        loads.append(pltpu.make_async_copy(w, WKV.at[:, pl.ds(j * 128, 128)], lsem.at[1]))
    own = pltpu.make_async_copy(tokens, G.at[tp], lsem.at[2])
    small = [
        pltpu.make_async_copy(p, q, lsem.at[3 + j])
        for j, (p, q) in enumerate(((holder_h, holder), (slot_h, slot), (taps_h, taps), (route_h, route)))
    ]
    for c in small + loads[4:]:
        c.start()

    def store_copy(i):
        r = pl.ds(pl.multiple_of(i * SEQ, SEQ), SEQ)
        return pltpu.make_async_copy(store.at[r, :], ST.at[r, :], stsem)

    def start_store(i, _):
        store_copy(i).start()
        return 0

    lax.fori_loop(0, 8, start_store, 0)
    for c in loads[:4]:
        c.start()
    own.start()

    def wcol(m, cs):
        return (cout, mout)[m].at[:, pl.ds(pl.multiple_of(cs * 128, 128), 128)]

    def start_wl(cs, _):
        for m in range(2):
            pltpu.make_async_copy(wcol(m, cs), W.at[cs, k, y, m], wloc).start()
        return 0

    lax.fori_loop(0, NST, start_wl, 0)
    for c in small[:2]:
        c.wait()

    rowi = lax.broadcasted_iota(jnp.int32, (NST, 128), 0)
    lanei = lax.broadcasted_iota(jnp.int32, (NST, 128), 1)
    count = jnp.zeros((NST, 128), jnp.int32)
    wanted = jnp.zeros((NST, 128), jnp.int32)
    for r in range(32):
        o = holder[r % 2, r // 2]
        v = slot[r % 2, r // 2]
        hit = rowi == o
        PV[r] = jnp.sum(jnp.where(hit, count, 0), axis=0, keepdims=True) + o * CAP
        wanted = jnp.where(hit & (lanei == count), v, wanted)
        count = count + hit.astype(jnp.int32)
    for o in range(NST):
        OV[o] = wanted[o : o + 1]
    pcopy = pltpu.make_async_copy(PV, PS, lsem.at[7])
    pcopy.start()

    @pl.when(k == 1)
    def _():
        pl.semaphore_wait(bar, NTP - 1)
        signal(row_sem, sibling)

    @pl.when(k == 0)
    def _():
        pl.semaphore_wait(row_sem, 1)

    def direct(t):
        src = tokens.at[:, rows(t), :]
        dst = G.at[tp, :, rows(t), :]
        rcopy(src, dst, gsend, agr.at[t, 0], dev_y(1)).start()
        rcopy(src, dst, gsend, agr.at[t, 1], dev_y(-1)).start()
        rcopy(src, dst, gsend, sib.at[t], sibling).start()

    def gblk(d):
        return ring(y, d) * 2 + k


    def w1_start(dy, _):
        for m in range(2):
            rcopy(
                wcol(m, st), W.at[st, k, y, m], wsend, w1,
                (st, lax.rem(y + dy, 4) * 2 + k),
            ).start()
        return 0

    lax.fori_loop(1, 4, w1_start, 0)
    direct(0)
    direct(1)

    @pl.when(k == 0)
    def _():
        pl.semaphore_wait(bar, 2 * (NST - 1))
        signal(all_sem, sibling)

    @pl.when(k == 1)
    def _():
        pl.semaphore_wait(all_sem, 1)

    def ix_copy(d):
        r = lax.rem(st + d, NST)
        return rcopy(OV.at[r], WV.at[st], ixs, ixr, (r, tp))

    def ix_start(d, _):
        ix_copy(d).start()
        return 0

    lax.fori_loop(1, NST, ix_start, 0)
    pltpu.make_async_copy(OV.at[st], WV.at[st], ixr).start()

    arrived(WKV, lsem.at[1])
    arrived(ST, stsem)

    def kv_body(i, _):
        r = pl.ds(pl.multiple_of(i * SEQ, SEQ), SEQ)
        kv = jnp.dot(ST[r, :], WKV[...], preferred_element_type=F32).astype(BF16)
        for j in range(4):
            TB[i * 4 + j] = kv[j * PLEN : (j + 1) * PLEN]
        return 0

    lax.fori_loop(0, 3, kv_body, 0)
    direct(2)
    lax.fori_loop(3, 6, kv_body, 0)

    def send_kv():
        arrived(WV, ixr)
        c = pltpu.make_async_copy(WV, WS, lsem.at[3])
        c.start()
        c.wait()
        lax.fori_loop(1, 4, kv_out, 0)
        for j in range(CAP):
            KS[st, j] = TB[WS[st, 0, j]]
        pltpu.make_async_copy(KS.at[st], KR.at[pl.ds(st * CAP, CAP)], kvr).start()

    def kv_out(d, _):
        r = lax.rem(st + d, NST)
        for j in range(CAP):
            KS[r, j] = TB[WS[r, 0, j]]
        rcopy(KS.at[r], KR.at[pl.ds(st * CAP, CAP)], kvs, kvr, (r, tp)).start()
        return 0

    def dev_a(d):
        return (stidx(ring(a, d), b), tp)

    def dev_b(d):
        return (stidx(a, ring(b, d)), tp)

    def yo(dy):
        return lax.rem(y + dy, 4)

    def plane1():
        arrived(W.at[pl.ds(0, 3), 0, 0], w1)

        def go2(j, _):
            da = lax.div(j, 3) + 1
            dy = lax.rem(j, 3) + 1
            blk = W.at[st, k, yo(dy)]
            rcopy(blk, blk, wsend, p1, (stidx(lax.rem(a + da, 4), b), tp)).start()
            return 0

        lax.fori_loop(0, 9, go2, 0)

    def wblk(j, d):
        return W.at[stidx(lax.div(j, 3), ring(b, d)), k, yo(lax.rem(j, 3) + 1)]

    def wpass(lo, hi, d, sem, dev):
        def go(j, _):
            g = wblk(j, d)
            rcopy(g, g, wsend, sem, dev).start()
            return 0

        lax.fori_loop(lo, hi, go, 0)

    SIX = W.at[pl.ds(0, 6), 0, 0]
    TWELVE = W.at[pl.ds(0, 3), 0]

    def plane2():
        arrived(W.at[pl.ds(0, 9), 0, 0], p1)
        wpass(0, 6, 0, p2.at[0], dev_b(1))
        wpass(6, 12, 0, p2.at[1], dev_b(-1))
        wpass(0, 12, 0, wsib.at[0], sibling)

    def plane3():
        arrived(SIX, p2.at[0])
        arrived(SIX, p2.at[1])
        wpass(0, 6, -1, p2.at[2], dev_b(1))
        wpass(6, 12, 1, p2.at[4], dev_b(-1))
        wpass(0, 6, -1, wsib.at[1], sibling)
        wpass(6, 12, 1, wsib.at[1], sibling)

    def plane4():
        arrived(TWELVE, p2.at[3])
        wpass(6, 12, -1, wsib.at[2], sibling)
        wpass(0, 6, 1, wsib.at[2], sibling)

    def plane5():
        arrived(SIX, p2.at[2])
        wpass(0, 6, 2, wsib.at[3], sibling)
        arrived(SIX, p2.at[4])
        wpass(6, 12, 2, wsib.at[3], sibling)

    plane1()
    lax.fori_loop(6, 8, kv_body, 0)
    send_kv()

    def send_branch(m, lo, n):
        r = pl.ds(pl.multiple_of(lo, STEP), n)

        def go(d, _):
            s = lax.rem(tp + d, NTP)
            rcopy(AS.at[m, s, r, :], A.at[m, tp, r, :], asend, arecv, (st, s)).start()
            return 0

        lax.fori_loop(1, NTP, go, 0)
        pltpu.make_async_copy(AS.at[m, tp, r, :], A.at[m, tp, r, :], arecv).start()

    arrived(WIN, lsem.at[0])
    for c in small[2:]:
        c.wait()
    own.wait()
    arrived(W.at[:, k, y], wloc)
    rcopy(W.at[:, k, y], W.at[:, k, y], wsend, wsown, sibling).start()
    PM[...] = jnp.zeros_like(PM)
    place = lax.rem(lax.broadcasted_iota(jnp.int32, (SEQ, 128), 0), STEP)

    def project(t):
        arrived(G.at[pl.ds(0, 4), :, rows(t), :], sib.at[t])
        rws = jnp.concatenate([G[j, :, rows(t), :].reshape(SEQ, 256) for j in range(NTP)], axis=1)
        p = jnp.dot(rws, WIN[...], preferred_element_type=F32)
        Q[:, rows(t), :] = p[:, 0:128].astype(BF16).reshape(NTP, STEP, 128)
        mixed = p[:, 256:384] * p[:, 384:512]
        prev = PM[...]
        PM[...] = mixed
        tv = taps[...].astype(F32)
        m1 = jnp.where(place >= 1, pltpu.roll(mixed, 1, 0), pltpu.roll(prev, SEQ + 1 - STEP, 0))
        m2 = jnp.where(place >= 2, pltpu.roll(mixed, 2, 0), pltpu.roll(prev, SEQ + 2 - STEP, 0))
        filt = tv[0:1] * m2 + tv[1:2] * m1 + tv[2:3] * mixed
        AS[0, :, rows(t), :] = (p[:, 128:256] * filt).astype(BF16).reshape(NTP, STEP, 128)
        send_branch(0, t * STEP, STEP)

    def attend(seqs, lo, n):
        blk = lo // BLOCK if isinstance(lo, int) else 0
        r = pl.ds(lo, n)
        kvs_, sc = [], []
        for s in seqs:
            i = (s * 2 + blk) * 2
            kv = jnp.concatenate([KR[PS[i, 0, 0]], KR[PS[i + 1, 0, 0]]], axis=0)
            kvs_.append(kv)
            sc.append(
                lax.dot_general(
                    Q[s, r, :], kv[:, :128], (((1,), (1,)), ((), ())), preferred_element_type=F32
                ) * (HEAD_SIZE ** -0.5)
            )
        e = [jnp.exp(v - jnp.max(v, axis=1, keepdims=True)) for v in sc]
        wt = [(v / jnp.sum(v, axis=1, keepdims=True)).astype(BF16) for v in e]
        for s, kv, v in zip(seqs, kvs_, wt):
            o = jnp.dot(v, kv[:, 128:], preferred_element_type=F32)
            AS[1, s, r, :] = o.astype(BF16)

    def step(t, _):
        @pl.when(t < 8)
        def _():
            r = rows(t)
            g = G.at[gblk(-1), :, r, :]
            arrived(g, agr.at[t, 0])
            h = G.at[gblk(-1), pl.ds(0, 4), r, :]
            rcopy(h, h, gsend, agr.at[t, 2], dev_y(1)).start()
            rcopy(g, g, gsend, sib.at[t], sibling).start()
            g2 = G.at[gblk(1), :, r, :]
            arrived(g2, agr.at[t, 1])
            h2 = G.at[gblk(1), pl.ds(4, 4), r, :]
            rcopy(h2, h2, gsend, agr.at[t, 2], dev_y(-1)).start()
            rcopy(g2, g2, gsend, sib.at[t], sibling).start()

        @pl.when((t >= 1) & (t < 6))
        def _():
            direct(t + 2)

        @pl.when(t <= 1)
        def _():
            lax.fori_loop(4 + 6 * t, 10 + 6 * t, kv_out, 0)

        @pl.when(t == 4)
        def _():
            plane2()

        @pl.when(t == 6)
        def _():
            wpass(6, 12, 0, p2.at[3], dev_b(1))
            wpass(0, 6, 0, p2.at[3], dev_b(-1))

        def opposite(u):
            g = G.at[gblk(2), :, rows(u), :]
            arrived(g, agr.at[u, 2])
            rcopy(g, g, gsend, sib.at[u], sibling).start()

        @pl.when((t >= 1) & (t < 9))
        def _():
            opposite(t - 1)

        @pl.when(t == 8)
        def _():
            attend(range(NTP), BLOCK, 64)
            send_branch(1, BLOCK, 64)

        @pl.when(t >= 2)
        def _():
            project(t - 2)

        @pl.when(t == 7)
        def _():
            plane3()
            arrived(KR, kvr)
            pcopy.wait()

            def two(i, _):
                attend(range(NTP), pl.multiple_of(i * 64, 64), 64)
                send_branch(1, i * 64, 64)
                return 0

            lax.fori_loop(0, 2, two, 0)
        @pl.when(t == 8)
        def _():
            plane4()

        return 0

    lax.fori_loop(0, 10, step, 0)
    attend(range(NTP), BLOCK + 64, 64)
    send_branch(1, BLOCK + 64, 64)
    plane5()
    rws = jnp.concatenate([G[j, tp] for j in range(NTP)], axis=1)
    logits = lax.dot_general(rws, route[...], (((1,), (1,)), ((), ())), preferred_element_type=F32)
    mix = jax.nn.sigmoid(logits)

    arrived(W.at[:, 1 - k, y], wsown)
    for d in range(4):
        arrived(TWELVE, wsib.at[d])

    order = [(kk, yy) for kk in range(2) for yy in range(4)]

    def put(c):
        return pltpu.make_async_copy(
            OB.at[c], out.at[:, pl.ds(pl.multiple_of(c * WIDE, WIDE), WIDE)], osem
        )

    def outp(c, _):
        acc = []
        for m in range(2):
            lhs = jnp.concatenate([A[m, yy * 2 + kk] for kk, yy in order], axis=1)
            rhs = jnp.concatenate(
                [
                    jnp.concatenate([W[c * (WIDE // 128) + i, kk, yy, m] for kk, yy in order], axis=0)
                    for i in range(WIDE // 128)
                ],
                axis=1,
            )
            acc.append(jnp.dot(lhs, rhs, preferred_element_type=F32))
        OB[c] = (mix[:, 0:1] * acc[0] + mix[:, 1:2] * acc[1]).astype(BF16)
        put(c).start()
        return 0

    arrived(A, arecv)
    lax.fori_loop(0, 2048 // WIDE, outp, 0)

    arrived(OB, osem)
    arrived(OV.at[pl.ds(0, NST - 1)], ixs)
    arrived(KS.at[pl.ds(0, NST - 1)], kvs)
    arrived(G.at[pl.ds(0, 7)], gsend)
    arrived(AS.at[:, pl.ds(0, 7)], asend)
    arrived(W.at[pl.ds(0, 14)], wsend)


def local(
    tokens, store, holder, slot, wq, wk, wval, wo, wi, wv, taps, route, cout, mout
):
    hbm = pl.BlockSpec(memory_space=pltpu.HBM)
    dma = pltpu.SemaphoreType.DMA
    reg = pltpu.SemaphoreType.REGULAR
    V = pltpu.VMEM
    return pl.pallas_call(
        kernel,
        out_shape=jax.ShapeDtypeStruct((SEQ, cout.shape[1]), BF16),
        in_specs=[hbm] * 14,
        out_specs=pl.BlockSpec(memory_space=pl.ANY),
        scratch_shapes=[
            V((SEQ, 128), F32),
            V((2048 // WIDE, SEQ, WIDE), BF16),
            pltpu.SMEM((2, 16), jnp.int32),
            pltpu.SMEM((2, 16), jnp.int32),
            V((3, 128), BF16),
            V((2, 2048), BF16),
            V((8, NTP, SEQ, 256), BF16),
            V((2048, 2048), BF16),
            V((2048, 512), BF16),
            V((2048, 256), BF16),
            V((32, PLEN, 256), BF16),
            V((NST, CAP, PLEN, 256), BF16),
            V((NST * CAP, PLEN, 256), BF16),
            V((NST, 1, 128), jnp.int32),
            V((NST, 1, 128), jnp.int32),
            pltpu.SMEM((NST, 1, 128), jnp.int32),
            V((32, 1, 128), jnp.int32),
            pltpu.SMEM((32, 1, 128), jnp.int32),
            V((NTP, SEQ, 128), BF16),
            V((2, 8, SEQ, 128), BF16),
            V((2, 8, SEQ, 128), BF16),
            V((NST, 2, 4, 2, 128, 128), BF16),
            dma((8,)), dma, dma, dma, dma, dma,
            dma((8, 3)), dma((8,)), dma, dma, dma,
            dma, dma, dma, dma((5,)), dma((4,)), dma, dma, dma,
            reg, reg,
        ],
        compiler_params=pltpu.CompilerParams(
            collective_id=0, has_side_effects=True, vmem_limit_bytes=44 * 1024 * 1024
        ),
    )(
        *(
            pltpu.with_memory_space_constraint(v, pltpu.HBM)
            for v in (
                tokens.reshape(NTP, SEQ, tokens.shape[1]), store.reshape(-1, store.shape[-1]), holder.T, slot.T,
                wq, wo, wi, wv, wk, wval, taps, route.T, cout, mout,
            )
        )
    )


def solution(mesh):
    return jax.shard_map(
        local,
        mesh=mesh,
        in_specs=(
            P("st", "tp"), P("st", None, None), P("st", None), P("st", None),
            P(None, "tp"), P(None, "tp"), P(None, "tp"), P(None, "tp"), P(None, "tp"),
            P(None, "tp"), P(None, "tp"), P(), P("tp", None), P("tp", None),
        ),
        out_specs=P(("st", "tp"), None),
        check_vma=False,
    )
```
